256 devices in a mesh: sp: 64 (over z, x, core), tp: 4 (over y).
Axes of the slice: x: 4, y: 4, z: 8, core: 2. Of those that a mesh axis runs over, the one named last changes fastest.
Arguments:
- conv_out: bfloat16 [12288, 2048], P('sp', 'tp'), may hold values from -6 to 6
- gate_in: bfloat16 [12288, 2048], P('sp', 'tp'), may hold values from -6 to 6
- block_states: float32 [64, 2048], P('sp', 'tp'), may hold values from -4 to 4
- decay_param: float32 [2048], P('tp'), may hold values from 4 to 20
- decay_shift: float32 [12288], P('sp'), may hold values from -2 to 0, as said below
- w_reset: bfloat16 [16, 128, 128], P('tp'), may hold values from -0.5 to 0.5
- w_input: bfloat16 [16, 128, 128], P('tp'), may hold values from -0.5 to 0.5
- w_out: bfloat16 [2048, 2048], P('tp'), may hold values from -0.125 to 0.125
- mixed: bfloat16 [12288, 2048], P('sp', 'tp'), may hold values from -6 to 6
- d_out: bfloat16 [12288, 2048], P('sp', 'tp'), may hold values from -16 to 16
- expert_ids: int32 [12288, 2], P('sp'), may hold values from 0 to 63, all different within a row; in each aligned block of 192 rows (0 to 191, 192 to 383, ...) at most 12 rows name the same one
- route_weights: float32 [12288, 2], P('sp'), may hold values from 0.2 to 1.4
- w_gate: bfloat16 [64, 2048, 1024], P('sp', None, 'tp'), may hold values from -0.125 to 0.125
- w_up: bfloat16 [64, 2048, 1024], P('sp', None, 'tp'), may hold values from -0.125 to 0.125
- w_down: bfloat16 [64, 1024, 2048], P('sp', 'tp'), may hold values from -0.1875 to 0.1875
Outputs:
- grad_w_gate: float32 [64, 2048, 1024], P('sp', None, 'tp')
- grad_w_up: float32 [64, 2048, 1024], P('sp', None, 'tp')
- grad_w_down: float32 [64, 1024, 2048], P('sp', 'tp')
- grad_out_proj_t: float32 [2048, 2048], P('sp', 'tp')
- recurrence_input_gradient: bfloat16 [12288, 2048], P('sp', 'tp')
- grad_gate: bfloat16 [12288, 2048], P('sp', 'tp')
The draws below stay inside these ranges and needn't reach their ends.
Inputs may be any that keep to these rules, and one draw needn't show every extreme that they name: `expert_ids`: each row names 2 different experts; among the 192 tokens of one index of sp no expert is named more than 12 times, and in some index of sp one expert is named exactly 12 times. decay_shift is at most -0.05 / 12288 at every position.
All inputs are finite; a program needn't handle non-finite values.
Results may differ from the reference program's by a relative error of at most 0.013.
Values may be sent and summed in bfloat16 or wider, within the bound.
A program may use at most 128 MiB of HBM per device.

```python
import math
import jax
import jax.numpy as jnp
import numpy as np
from jax import lax

D = 2048
HEADS = 16
HEAD_DIM = 128
DR = 2048
FE = 1024
TOP = 2
TOK_DEV = 192
SEQUENCE_TOKENS = 12288
EXPERTS = 64
CAP = 12
N_SP = 64
N_TP = 4


def draw_decay_param(key, part):
    chooser, slow_key, fast_key = jax.random.split(jax.random.fold_in(key, 11), 3)
    portion = 0.5
    is_slow = jax.random.uniform(chooser, (DR,), jnp.float32) < portion
    slow_rate = jax.random.uniform(slow_key, (DR,), jnp.float32, minval=0.1, maxval=0.4) / (4.0 * SEQUENCE_TOKENS)
    fast_rate = 1.0 / (4.0 * jax.random.uniform(fast_key, (DR,), jnp.float32, minval=30.0, maxval=100.0))
    rates = jnp.where(is_slow, slow_rate, fast_rate)
    return (-jnp.log(jnp.expm1(rates))).astype(jnp.float32)


def draw_decay_shift(key, part):
    level_key, location_key, depth_key = jax.random.split(jax.random.fold_in(key, 23), 3)
    blocks = SEQUENCE_TOKENS // TOK_DEV
    levels = jnp.exp(jax.random.uniform(level_key, (blocks,), jnp.float32, minval=math.log(0.05), maxval=math.log(0.4)))
    reference_value = -jnp.repeat(levels, TOK_DEV) / SEQUENCE_TOKENS
    spike_locations = jax.random.randint(location_key, (2,), 0, SEQUENCE_TOKENS)
    nesting_levels = jax.random.uniform(depth_key, (2,), jnp.float32, minval=math.log(0.6), maxval=math.log(0.8))
    return reference_value.at[spike_locations].add(nesting_levels).astype(jnp.float32)


def raised(entries, key, source, target, blocks, factor):
    owner, partner = [(jnp.arange(entries.shape[position]) // (entries.shape[position] // blocks)).reshape([-1 if axis == position else 1 for axis in range(entries.ndim)]) for position in (source, target)]
    chosen = jax.random.permutation(key, blocks)[partner]
    strong = (owner == chosen) | (owner == (partner + blocks // 2) % blocks)
    return jnp.where(strong, factor * entries, entries)


def shard_levels(key, extent, cuts, smallest, high):
    def one(axis_at, parts):
        draws = jax.random.uniform(jax.random.fold_in(jax.random.fold_in(key, 6), axis_at), (parts,), jnp.float32, smallest / len(cuts), high / len(cuts))
        return jnp.repeat(jnp.exp(draws), extent[axis_at] // parts).reshape((-1,) + (1,) * (len(extent) - axis_at - 1))

    gain = one(*cuts[0])
    for cut in cuts[1:]:
        gain = gain * one(*cut)
    return gain


def assign_block(own_key, own, number, rows, count, top, limit, lean):
    ranking = jax.random.permutation(own_key, count)
    packed, ordinary = portions_of(count, rows * top, limit, lean, True), portions_of(count, rows * top, limit, lean, False)
    places = jnp.arange(count)

    def named(lengths, offset_by):
        used = int((lengths > 0).sum())
        fixed = max(1, used // 4)
        passed = fixed + (places - fixed + offset_by * (used - fixed)) % max(1, count - fixed)
        return jnp.zeros((count,), jnp.int32).at[ranking[jnp.where(places < fixed, places, passed)]].set(jnp.asarray(lengths, jnp.int32))

    lengths = jnp.where(number % 4 == 0, named(packed, number // 4), named(ordinary, number - number // 4 - 1))
    mixed = jax.random.permutation(jax.random.fold_in(own, 3), count)
    giver, sink = mixed[0:count // 2 * 2:2], mixed[1:count // 2 * 2:2]
    margin = jnp.minimum(lengths[giver] - 1, limit - lengths[sink]) // 2
    margin = jnp.where((giver == ranking[0]) | (sink == ranking[0]) | (lengths[sink] == 0), 0, jnp.maximum(margin, 0))
    passed = jax.random.randint(jax.random.fold_in(own, 4), (count // 2,), 0, 1 << 20) % (margin + 1)
    lengths = lengths.at[giver].add(-passed).at[sink].add(passed)
    items = jnp.searchsorted(jnp.cumsum(lengths), jnp.arange(rows * top), side="right").astype(jnp.int32)
    listing = items.reshape(top, rows).T
    listing = listing[jax.random.permutation(jax.random.fold_in(own, 1), rows)]
    offset_by = jax.random.randint(jax.random.fold_in(own, 2), (rows, 1), 0, top)
    return jnp.take_along_axis(listing, (jnp.arange(top)[None, :] + offset_by) % top, axis=1)


def portions_of(count, total, limit, lean, full):
    weights = [(1 << 20) // math.isqrt(grade ** lean) + 1 for grade in range(1, count + 1)]
    largest = limit if full else min(limit, max(-(-total // count), total * weights[0] // sum(weights)))
    least = 1 if total - largest >= count - 1 else 0
    given, rest = [largest] + [least] * (count - 1), total - largest - least * (count - 1)
    while rest > 0:
        candidates = [i for i in range(1, count) if given[i] < largest] or [i for i in range(1, count) if given[i] < limit]
        whole, left = sum([weights[i] for i in candidates]), rest
        for i in candidates:
            more = min(limit - given[i], max(1, left * weights[i] // whole), rest)
            given[i] = given[i] + more
            rest = rest - more
    return np.array(given)


def bell_draw(own_key, shape, width, bound, cuts=(), kind=jnp.bfloat16):
    drawn = jax.random.normal(own_key, shape, jnp.float32) * width
    if len(cuts) > 0:
        drawn = shard_levels(own_key, shape, cuts, -0.22, 0.18) * drawn
    return jnp.clip(drawn, min=-bound, max=bound).astype(kind)


def noise_with(own_key, extent, width, most, shards, heavy, kind=jnp.bfloat16):
    result = width * jax.random.normal(own_key, extent, jnp.float32)
    if shards:
        result = result * shard_levels(own_key, extent, shards, -0.22, 0.18)
    return jnp.clip(raised(result, jax.random.fold_in(own_key, 3), *heavy), -most, most).astype(kind)


def setup_inputs(seed: int = 0) -> dict:
    key_list = jax.random.split(jax.random.key(seed), 16)
    conv_out = bell_draw(key_list[0], (SEQUENCE_TOKENS, DR), 1.0, 6.0, ((0, 64), (1, 4)))
    gate_in = bell_draw(key_list[1], (SEQUENCE_TOKENS, DR), 1.0, 6.0, ((0, 64), (1, 4)))
    block_states = bell_draw(key_list[2], (N_SP, DR), 0.5, 4.0, ((0, 64), (1, 4)), jnp.float32)
    decay_param = draw_decay_param(jax.random.fold_in(key_list[15], 71), 0)
    decay_shift = draw_decay_shift(jax.random.fold_in(key_list[15], 71), 0)
    w_reset = bell_draw(key_list[5], (HEADS, HEAD_DIM, HEAD_DIM), HEAD_DIM ** -0.5, 0.5, ((0, 4),))
    w_input = bell_draw(key_list[6], (HEADS, HEAD_DIM, HEAD_DIM), HEAD_DIM ** -0.5, 0.5, ((0, 4),))
    w_out = bell_draw(key_list[7], (DR, D), DR ** -0.5, 0.125, ((0, 4),))
    mixed = bell_draw(key_list[8], (SEQUENCE_TOKENS, D), 1.0, 6.0, ((0, 64), (1, 4)))
    d_out = noise_with(key_list[9], (SEQUENCE_TOKENS, D), 1.0, 16.0, ((0, 64), (1, 4)), (0, 1, 64, 4.0))
    expert_ids_keys = jax.random.split(jax.random.fold_in(key_list[10], 1), SEQUENCE_TOKENS // TOK_DEV)
    expert_ids_turns = jax.random.permutation(jax.random.fold_in(key_list[10], 3), SEQUENCE_TOKENS // TOK_DEV)
    expert_ids = jax.vmap(lambda own, number: assign_block(jax.random.fold_in(key_list[10], 2), own, number, TOK_DEV, EXPERTS, TOP, CAP, 1))(expert_ids_keys, expert_ids_turns).reshape((SEQUENCE_TOKENS, TOP))
    route_weights = jnp.clip(0.2 + 1.19999997 * jax.random.uniform(key_list[11], (SEQUENCE_TOKENS, TOP), jnp.float32) ** shard_levels(key_list[11], (SEQUENCE_TOKENS, TOP), ((0, 64),), -0.2, 0.2), 0.2, 1.4)
    w_gate = bell_draw(key_list[12], (EXPERTS, D, FE), D ** -0.5, 0.125, ((0, 64), (2, 4)))
    w_up = bell_draw(key_list[13], (EXPERTS, D, FE), D ** -0.5, 0.125, ((0, 64), (2, 4)))
    w_down = bell_draw(key_list[14], (EXPERTS, FE, D), FE ** -0.5, 0.1875, ((0, 64), (1, 4)))
    return dict(conv_out=conv_out, gate_in=gate_in, block_states=block_states, decay_param=decay_param, decay_shift=decay_shift, w_reset=w_reset, w_input=w_input, w_out=w_out, mixed=mixed, d_out=d_out, expert_ids=expert_ids, route_weights=route_weights, w_gate=w_gate, w_up=w_up, w_down=w_down)


def decay_combine(first_pair, second_pair):
    return (first_pair[0] * second_pair[0], second_pair[0] * first_pair[1] + second_pair[1])

def gelu_slope(values):
    outcome, pullback = jax.vjp(jax.nn.gelu, values)
    return (outcome, pullback(jnp.ones_like(values))[0])

def head_maps(values, weights):
    count = values.shape[0]
    split = values.astype(jnp.float32).reshape(count, weights.shape[0], weights.shape[1])
    mapped = jnp.einsum('thi,hij->thj', split, weights.astype(jnp.float32))
    return mapped.reshape(count, -1)

def head_back(grads, weights):
    count = grads.shape[0]
    split = grads.astype(jnp.float32).reshape(count, weights.shape[0], weights.shape[2])
    mapped = jnp.einsum('thj,hij->thi', split, weights.astype(jnp.float32))
    return mapped.reshape(count, -1)

def over_rows(left_matrix, right_matrix):
    return lax.dot_general(left_matrix, right_matrix, (((0,), (0,)), ((), ())), preferred_element_type=jnp.float32)

def against_rows(left_matrix, right_matrix):
    return lax.dot_general(left_matrix, right_matrix, (((1,), (1,)), ((), ())), preferred_element_type=jnp.float32)

def reference(conv_out, gate_in, block_states, decay_param, decay_shift, w_reset, w_input, w_out, mixed, d_out, expert_ids, route_weights, w_gate, w_up, w_down):
    conv_full = conv_out.astype(jnp.float32)
    reset = jax.nn.sigmoid(head_maps(conv_out, w_reset))
    input_gate = jax.nn.sigmoid(head_maps(conv_out, w_input))
    slow_rate = jax.nn.softplus(-decay_param)
    log_decay = -8.0 * reset * slow_rate[None, :] + decay_shift[:, None]
    decays = jnp.exp(log_decay)
    norm_in = jnp.sqrt(-jnp.expm1(2.0 * log_decay))
    drives = norm_in * input_gate * conv_full
    blocked = (N_SP, TOK_DEV, DR)
    cum_decay, cum_drive = lax.associative_scan(decay_combine, (decays.reshape(blocked), drives.reshape(blocked)), axis=1)
    states = cum_decay * block_states[:, None, :] + cum_drive
    prev_states = jnp.concatenate([block_states[:, None, :], states[:, :-1]], axis=1).reshape(SEQUENCE_TOKENS, DR)
    states = states.reshape(SEQUENCE_TOKENS, DR)
    gate_act, gate_deriv = gelu_slope(gate_in.astype(jnp.float32))
    merged_in = (gate_act * states).astype(jnp.bfloat16)
    flat_ids = expert_ids.reshape(N_SP, TOK_DEV * TOP)
    onehot = (flat_ids[:, :, None] == jnp.arange(EXPERTS, dtype=jnp.int32)[None, None, :]).astype(jnp.int32)
    slot_rank = lax.optimization_barrier(jnp.sum((jnp.cumsum(onehot, axis=1) - 1) * onehot, axis=2))
    source_index = jnp.arange(N_SP, dtype=jnp.int32)[:, None]
    slot_flat = (source_index * CAP + slot_rank).reshape(-1).astype(jnp.int32)
    expert_flat = expert_ids.reshape(-1).astype(jnp.int32)
    assign_ids = jnp.arange(SEQUENCE_TOKENS * TOP, dtype=jnp.int32)
    slot_table = jnp.full((EXPERTS, N_SP * CAP), SEQUENCE_TOKENS * TOP, jnp.int32).at[expert_flat, slot_flat].set(assign_ids)
    scaled_cot = (route_weights[:, :, None] * d_out.astype(jnp.float32)[:, None, :]).astype(jnp.bfloat16).reshape(SEQUENCE_TOKENS * TOP, D)
    cot_padded = jnp.concatenate([scaled_cot, jnp.zeros((1, D), jnp.bfloat16)], axis=0)
    mixed_padded = jnp.concatenate([mixed, jnp.zeros((1, D), jnp.bfloat16)], axis=0)
    block_width = FE // N_TP

    def one_expert(operands):
        slot_ids, gate_matrix, up_matrix, down_matrix = operands
        token_ids = jnp.where(slot_ids < SEQUENCE_TOKENS * TOP, slot_ids // TOP, SEQUENCE_TOKENS)
        expert_in = mixed_padded[token_ids]
        expert_cot = cot_padded[slot_ids]
        up_pre = jnp.dot(expert_in, gate_matrix, preferred_element_type=jnp.float32)
        linear = jnp.dot(expert_in, up_matrix, preferred_element_type=jnp.float32)
        sigmoid_up = jax.nn.sigmoid(up_pre)
        silu_up = up_pre * sigmoid_up
        hidden_state = (silu_up * linear).astype(jnp.bfloat16)
        d_hidden = against_rows(expert_cot, down_matrix)
        d_linear = (d_hidden * silu_up).astype(jnp.bfloat16)
        d_up = (d_hidden * linear * sigmoid_up * (1.0 + up_pre * (1.0 - sigmoid_up))).astype(jnp.bfloat16)
        grad_gate_e = over_rows(expert_in, d_up)
        grad_up_e = over_rows(expert_in, d_linear)
        grad_down_e = over_rows(hidden_state, expert_cot)
        row_count = expert_in.shape[0]
        up_blocks = d_up.astype(jnp.float32).reshape(row_count, N_TP, block_width)
        lin_blocks = d_linear.astype(jnp.float32).reshape(row_count, N_TP, block_width)
        gate_blocks = gate_matrix.astype(jnp.float32).reshape(D, N_TP, block_width)
        upw_blocks = up_matrix.astype(jnp.float32).reshape(D, N_TP, block_width)
        pieces = jnp.einsum('rqf,dqf->qrd', up_blocks, gate_blocks) + jnp.einsum('rqf,dqf->qrd', lin_blocks, upw_blocks)
        rounded = lax.optimization_barrier(pieces.astype(jnp.bfloat16))
        row_grad = lax.optimization_barrier(jnp.sum(rounded.astype(jnp.float32), axis=0)).astype(jnp.bfloat16)
        return (grad_gate_e, grad_up_e, grad_down_e, row_grad)
    grad_w_gate, grad_w_up, grad_w_down, row_grads = lax.map(one_expert, (slot_table, w_gate, w_up, w_down))
    returned = row_grads[expert_flat, slot_flat].astype(jnp.float32).reshape(SEQUENCE_TOKENS, TOP, D)
    d_mixed = (d_out.astype(jnp.float32) + lax.optimization_barrier(jnp.sum(returned, axis=1))).astype(jnp.bfloat16)
    grad_out_proj_t = over_rows(d_mixed, merged_in)
    d_merged = against_rows(d_mixed, w_out)
    grad_gate = (d_merged * states * gate_deriv).astype(jnp.bfloat16)
    d_states = d_merged * gate_act
    next_decay = jnp.concatenate([decays[1:], jnp.zeros((1, DR), jnp.float32)], axis=0)
    _, state_flipped = lax.associative_scan(decay_combine, (next_decay[::-1], d_states[::-1]), axis=0)
    state_grad = state_flipped[::-1]
    d_log_decay = state_grad * decays * prev_states - state_grad * input_gate * conv_full * decays * decays / norm_in
    d_pre_reset = (d_log_decay * (-8.0 * slow_rate[None, :]) * reset * (1.0 - reset)).astype(jnp.bfloat16)
    d_pre_input = (state_grad * norm_in * conv_full * input_gate * (1.0 - input_gate)).astype(jnp.bfloat16)
    recurrence_input_gradient = (state_grad * norm_in * input_gate + head_back(d_pre_reset, w_reset) + head_back(d_pre_input, w_input)).astype(jnp.bfloat16)
    return (grad_w_gate, grad_w_up, grad_w_down, grad_out_proj_t, recurrence_input_gradient, grad_gate)
```

```python
import functools

import jax
import jax.numpy as jnp
from jax import lax
from jax.experimental import pallas as pl
from jax.experimental.pallas import tpu as pltpu
from jax.sharding import PartitionSpec as P

F32 = jnp.float32
BF16 = jnp.bfloat16
MESH = pl.DeviceIdType.MESH
Z_ORDER = (0, 1, 7, 2, 6, 3, 5, 4)
VM = pl.BlockSpec(memory_space=pltpu.VMEM)
ANY = pl.BlockSpec(memory_space=pl.ANY)


def dot(a, b, dims=((1,), (0,))):
    return lax.dot_general(a, b, (dims, ((), ())), preferred_element_type=F32)


def swap4(value):
    return pltpu.roll(value, 4, axis=1)


def low_half(shape):
    return lax.broadcasted_iota(jnp.int32, shape, 1) < 4


def forward_kernel(
    conv_ref, gate_ref, first_ref, slow_ref, shift_ref, wr_ref, wi_ref,
    saved_ref, merged_ref, drive_ref, prev_ref, state_ref, reset_ref, norm_ref, inp_ref,
):
    rows, width = conv_ref.shape
    heads, hd = wr_ref.shape[0], wr_ref.shape[1]
    for h in range(heads):
        cols = slice(h * hd, (h + 1) * hd)
        conv = conv_ref[:, cols]
        reset = jax.nn.sigmoid(dot(conv, wr_ref[h]))
        inp = jax.nn.sigmoid(dot(conv, wi_ref[h]))
        log_decay = -8.0 * reset * slow_ref[:, cols] + shift_ref[...]
        decay = jnp.exp(log_decay)
        twice = 2.0 * log_decay
        small = jnp.maximum(twice, -0.5)
        series = 1.0 + small * (1.0 / 10.0)
        for n in (9, 8, 7, 6, 5, 4, 3, 2):
            series = 1.0 + small * (1.0 / n) * series
        less = jnp.where(twice > -0.5, small * series, jnp.exp(twice) - 1.0)
        norm = jnp.sqrt(-less)
        saved_ref[0, :, cols] = decay
        reset_ref[:, cols] = reset
        norm_ref[:, cols] = norm
        inp_ref[:, cols] = inp
        drive_ref[:, cols] = norm * inp * conv.astype(F32)

    def step(group, state):
        for i in range(8):
            t = pl.ds(group * 8 + i, 1)
            prev_ref[t, :] = state
            state = saved_ref[0, t, :] * state + drive_ref[t, :]
            state_ref[t, :] = state
        return state

    lax.fori_loop(0, rows // 8, step, first_ref[...])

    def back(group, prod):
        for i in range(8):
            t = rows - 1 - (group * 8 + i)
            saved_ref[1, pl.ds(t, 1), :] = prod
            prod = prod * saved_ref[0, pl.ds(t, 1), :]
        return prod

    lax.fori_loop(0, rows // 8, back, jnp.ones((1, width), F32))

    for h in range(heads):
        cols = slice(h * hd, (h + 1) * hd)
        conv = conv_ref[:, cols].astype(F32)
        decay, reset, norm, inp = saved_ref[0, :, cols], reset_ref[:, cols], norm_ref[:, cols], inp_ref[:, cols]
        by_log = decay * prev_ref[:, cols] - inp * conv * decay * decay / norm
        saved_ref[2, :, cols] = by_log * (-8.0 * slow_ref[:, cols]) * reset * (1.0 - reset)
        saved_ref[3, :, cols] = norm * conv * inp * (1.0 - inp)
        saved_ref[4, :, cols] = norm * inp
        state = state_ref[:, cols]
        value = gate_ref[:, cols].astype(F32)
        k = 0.7978845608028654
        square = value * value
        bent = jnp.tanh(k * (value + 0.044715 * value * square))
        act = 0.5 * value * (1.0 + bent)
        slope = 0.5 * (1.0 + bent) + 0.5 * value * (1.0 - bent * bent) * k * (1.0 + 3.0 * 0.044715 * square)
        saved_ref[5, :, cols] = state * slope
        saved_ref[6, :, cols] = act
        merged_ref[:, cols] = (act * state).astype(BF16)


def forward(conv, gate_in, first, slow, shift, w_reset, w_input):
    rows, width = conv.shape
    return pl.pallas_call(
        forward_kernel,
        out_shape=(
            jax.ShapeDtypeStruct((7, rows, width), F32),
            jax.ShapeDtypeStruct((rows, width), BF16),
        ),
        in_specs=[VM] * 7,
        out_specs=(VM, VM),
        scratch_shapes=[pltpu.VMEM((rows, width), F32)] * 6,
        name="forward_recurrence",
    )(conv, gate_in, first, slow, shift, w_reset, w_input)


def slot_tests(codes, experts):
    tokens = codes.shape[1]
    row = lax.broadcasted_iota(jnp.int32, (experts * 8, tokens), 0)
    base = (row // 8) * 16
    main = base + row % 8
    tail = base + 8 + row % 4
    return [[codes[k : k + 1, :] == want for k in (0, 1)] for want in (main, tail)], row % 8 < 4


def pack_kernel(ids_ref, wts_ref, d_out_ref, mixed_ref, send_ref, code_ref):
    experts = send_ref.shape[0]
    tokens, width = d_out_ref.shape
    half = width // 2
    each = lax.broadcasted_iota(jnp.int32, (experts, tokens), 0)
    named = [ids_ref[k : k + 1, :] == each for k in (0, 1)]
    both = jnp.where(named[0] | named[1], 1.0, 0.0).astype(BF16)
    earlier = (
        lax.broadcasted_iota(jnp.int32, (tokens, tokens), 0)
        < lax.broadcasted_iota(jnp.int32, (tokens, tokens), 1)
    )
    count = dot(both, jnp.where(earlier, 1.0, 0.0).astype(BF16))
    codes = []
    for k in (0, 1):
        rank = jnp.sum(jnp.where(named[k], count, 0.0), axis=0, keepdims=True)
        codes.append(ids_ref[k : k + 1, :] * 16 + rank.astype(jnp.int32))
        code_ref[k : k + 1, :] = codes[k]
    codes = jnp.concatenate(codes, axis=0)
    (main, tail), low = slot_tests(codes, experts)

    def weight(tests):
        return jnp.sum(
            jnp.where(tests[0], wts_ref[0:1, :], 0.0) + jnp.where(tests[1], wts_ref[1:2, :], 0.0),
            axis=1,
            keepdims=True,
        )

    main_pick = jnp.where(main[0] | main[1], 1.0, 0.0).astype(BF16)
    in_tail = tail[0] | tail[1]
    low_pick = jnp.where(in_tail & low, 1.0, 0.0).astype(BF16)
    high_pick = jnp.where(in_tail & ~low, 1.0, 0.0).astype(BF16)

    for at, (ref, w_main, w_tail) in enumerate(
        ((d_out_ref, weight(main), weight(tail)), (mixed_ref, None, None))
    ):
        first = dot(main_pick, ref[...])
        second = dot(low_pick, ref[:, :half]) + dot(high_pick, ref[:, half:])
        if w_main is not None:
            first, second = first * w_main, second * w_tail
        rows = slice(at * 8, at * 8 + 8)
        send_ref[:, rows, :width] = first.reshape(experts, 8, width).astype(BF16)
        send_ref[:, rows, width:] = second.reshape(experts, 8, half).astype(BF16)


def pack(ids, wts, d_out, mixed, experts):
    tokens, width = d_out.shape
    return pl.pallas_call(
        pack_kernel,
        out_shape=(
            jax.ShapeDtypeStruct((experts, 16, width + width // 2), BF16),
            jax.ShapeDtypeStruct((2, tokens), jnp.int32),
        ),
        in_specs=[VM] * 4,
        out_specs=(VM, VM),
        name="pack_slots",
    )(ids, wts, d_out, mixed)


def place():
    sp, tp = lax.axis_index("sp"), lax.axis_index("tp")
    return sp, tp, sp // 8, (sp // 2) % 4, sp % 2


def offset_device(z, x, c, dz, j):
    return ((z + dz) % 8) * 8 + ((x + j // 2) % 4) * 2 + (c + j % 2) % 2


def greet(sp, tp, n_sp, n_tp):
    barrier = pltpu.get_barrier_semaphore()

    def to_sp(k, _):
        pl.semaphore_signal(barrier, inc=1, device_id=((sp + k) % n_sp, tp), device_id_type=MESH)
        return 0

    lax.fori_loop(1, n_sp, to_sp, 0)
    for k in range(1, n_tp):
        pl.semaphore_signal(barrier, inc=1, device_id=(sp, (tp + k) % n_tp), device_id_type=MESH)
    pl.semaphore_wait(barrier, n_sp - 1 + n_tp - 1)


def remote(src, dst, send_sem, recv_sem, sp, tp):
    return pltpu.make_async_remote_copy(
        src_ref=src, dst_ref=dst, send_sem=send_sem, recv_sem=recv_sem,
        device_id=(sp, tp), device_id_type=MESH,
    )


def wait_bytes(ref, sem):
    pltpu.make_async_copy(ref, ref, sem).wait()


def dispatch_kernel(n_tp, send_ref, got_ref, own_sem, send_sem, recv_sem, y_send, y_recv, f_send, f_recv):
    sp, tp, z, x, c = place()
    n_sp = send_ref.shape[0]
    right, left, far = (tp + 1) % n_tp, (tp + n_tp - 1) % n_tp, (tp + 2) % n_tp
    greet(sp, tp, n_sp, n_tp)
    own = pltpu.make_async_copy(send_ref.at[sp], got_ref.at[tp, sp], own_sem)
    own.start()
    for i, dz in enumerate(Z_ORDER):

        def send(j, _):
            to = offset_device(z, x, c, dz, j)
            remote(send_ref.at[to], got_ref.at[tp, sp], send_sem, recv_sem.at[i], to, tp).start()
            return 0

        lax.fori_loop(1 if dz == 0 else 0, 8, send, 0)

    def group(i):
        return ((z + 8 - Z_ORDER[i]) % 8) * 8

    def forward_on(i):
        at = group(i)
        wait_bytes(got_ref.at[left, pl.ds(at, 8)], y_recv.at[0, i])
        part = got_ref.at[left, pl.ds(at, 4)]
        remote(part, part, f_send.at[0], f_recv.at[0, i], sp, right).start()
        wait_bytes(got_ref.at[right, pl.ds(at, 8)], y_recv.at[1, i])
        part = got_ref.at[right, pl.ds(at + 4, 4)]
        remote(part, part, f_send.at[1], f_recv.at[1, i], sp, left).start()

    for i in range(8):
        at = group(i)
        if i == 0:
            own.wait()
            wait_bytes(got_ref.at[tp, pl.ds(at, 7)], recv_sem.at[i])
        else:
            wait_bytes(got_ref.at[tp, pl.ds(at, 8)], recv_sem.at[i])
        part = got_ref.at[tp, pl.ds(at, 8)]
        remote(part, part, y_send.at[0], y_recv.at[0, i], sp, right).start()
        remote(part, part, y_send.at[1], y_recv.at[1, i], sp, left).start()
        if i > 0:
            forward_on(i - 1)
    forward_on(7)
    for i in range(8):
        at = group(i)
        wait_bytes(got_ref.at[far, pl.ds(at, 4)], f_recv.at[0, i])
        wait_bytes(got_ref.at[far, pl.ds(at + 4, 4)], f_recv.at[1, i])
    wait_bytes(send_ref.at[pl.ds(0, n_sp - 1)], send_sem)
    for side in (0, 1):
        wait_bytes(got_ref.at[tp], y_send.at[side])
        wait_bytes(got_ref.at[tp, pl.ds(0, n_sp // 2)], f_send.at[side])


def dispatch(send, n_tp):
    dma = pltpu.SemaphoreType.DMA
    return pl.pallas_call(
        functools.partial(dispatch_kernel, n_tp),
        out_shape=jax.ShapeDtypeStruct((n_tp, *send.shape), BF16),
        in_specs=[VM],
        out_specs=ANY,
        scratch_shapes=[dma, dma, dma((8,)), dma((2,)), dma((2, 8)), dma((2,)), dma((2, 8))],
        compiler_params=pltpu.CompilerParams(collective_id=0, has_side_effects=True),
        name="dispatch",
    )(send)


def expert_kernel(
    got_ref, wg_ref, wu_ref, wd_ref, gg_ref, gu_ref, gd_ref, part_ref,
    rows_ref, cot_ref, grad_ref, hidden_ref,
):
    n_tp, n_src = got_ref.shape[0], got_ref.shape[1]
    width = got_ref.shape[3] * 2 // 3
    half = width // 2
    fe = wg_ref.shape[1]
    main_rows = n_src * 8

    for q in range(n_tp):
        cols = slice(q * width, (q + 1) * width)

        def unpack(g, _):
            src = pl.ds(g * 16, 16)
            for at, ref in ((0, cot_ref), (8, rows_ref)):
                ref[pl.ds(g * 128, 128), cols] = (
                    got_ref[q, src, at : at + 8, :width].astype(F32).reshape(128, width).astype(BF16)
                )
                tails = got_ref[q, src, at : at + 8, width:].astype(F32)
                turned = swap4(tails)
                tails, turned = tails.reshape(8, 2, 8, half), turned.reshape(8, 2, 8, half)
                low = low_half((8, 8, half))
                left = jnp.where(low, tails[:, 0], turned[:, 1])
                right = jnp.where(low, turned[:, 0], tails[:, 1])
                both = jnp.concatenate([left, right], axis=2).reshape(64, width).astype(BF16)
                ref[pl.ds(main_rows + g * 64, 64), cols] = both
            return 0

        lax.fori_loop(0, n_src // 16, unpack, 0)

    def terms(r, _):
        rows = pl.ds(r * 256, 256)
        value = rows_ref[rows, :]
        up_pre = dot(value, wg_ref[...])
        linear = dot(value, wu_ref[...])
        d_hidden = dot(cot_ref[rows, :], wd_ref[...], ((1,), (1,)))
        gate = jax.nn.sigmoid(up_pre)
        silu = up_pre * gate
        hidden_ref[rows, :] = (silu * linear).astype(BF16)
        grad_ref[rows, fe:] = (d_hidden * silu).astype(BF16)
        grad_ref[rows, :fe] = (d_hidden * linear * gate * (1.0 + up_pre * (1.0 - gate))).astype(BF16)
        return 0

    lax.fori_loop(0, rows_ref.shape[0] // 256, terms, 0)

    for q in range(n_tp):
        cols = slice(q * width, (q + 1) * width)

        def part_of(rows):
            return dot(grad_ref[rows, :fe], wg_ref[cols, :], ((1,), (1,))) + dot(
                grad_ref[rows, fe:], wu_ref[cols, :], ((1,), (1,))
            )

        def first(r, _):
            part = part_of(pl.ds(r * 256, 256)).reshape(32, 8, width)
            part_ref[q, pl.ds(r * 32, 32), :, :width] = part.astype(BF16)
            return 0

        lax.fori_loop(0, main_rows // 256, first, 0)

        def second(r, _):
            part = part_of(pl.ds(main_rows + r * 128, 128)).reshape(16, 8, width)
            left, right = part[:, :, :half], part[:, :, half:]
            low = low_half((16, 8, half))
            one = jnp.where(low, left, swap4(right))
            two = jnp.where(low, swap4(left), right)
            both = jnp.stack([one, two], axis=1).reshape(32, 8, half)
            part_ref[q, pl.ds(r * 32, 32), :, width:] = both.astype(BF16)
            return 0

        lax.fori_loop(0, n_src // 32, second, 0)

    def weight_grads(k, _):
        cols = pl.ds(pl.multiple_of(k * 512, 512), 512)
        both = dot(rows_ref[:, cols], grad_ref[...], ((0,), (0,)))
        gg_ref[cols, :] = both[:, :fe]
        gu_ref[cols, :] = both[:, fe:]
        gd_ref[:, cols] = dot(hidden_ref[...], cot_ref[:, cols], ((0,), (0,)))
        return 0

    lax.fori_loop(0, rows_ref.shape[1] // 512, weight_grads, 0)


def experts_back(got, w_gate, w_up, w_down):
    n_tp, n_src, _, packed = got.shape
    model, fe = w_gate.shape
    rows = n_src * 12
    return pl.pallas_call(
        expert_kernel,
        out_shape=(
            jax.ShapeDtypeStruct((model, fe), F32),
            jax.ShapeDtypeStruct((model, fe), F32),
            jax.ShapeDtypeStruct((fe, model), F32),
            jax.ShapeDtypeStruct((n_tp, n_src, 8, packed), BF16),
        ),
        in_specs=[VM] * 4,
        out_specs=(VM,) * 4,
        scratch_shapes=[
            pltpu.VMEM((rows, model), BF16),
            pltpu.VMEM((rows, model), BF16),
            pltpu.VMEM((rows, 2 * fe), BF16),
            pltpu.VMEM((rows, fe), BF16),
        ],
        compiler_params=pltpu.CompilerParams(vmem_limit_bytes=56 * 2**20),
        name="experts",
    )(got, w_gate, w_up, w_down)


def tail_kernel(
    part_ref, code_ref, d_out_ref, saved_ref, merged_ref, w_out_ref, wr_ref, wi_ref,
    proj_ref, rec_ref, gate_ref,
    term_ref, back_ref, ret_ref, mix_ref, acc_ref, local_ref, keep_ref, pair_ref, pair_got,
    x_ref, x_got, z_ref, z_got, own_ref, lead_ref, lead_got,
    term_send, term_recv, ret_send, ret_recv, mix_send, mix_recv, pair_send, pair_recv,
    x_send, x_recv, z_send, z_recv, lead_send, lead_recv,
):
    sp, tp, z, x, c = place()
    n_tp, n_sp = part_ref.shape[0], part_ref.shape[1]
    tokens, width = d_out_ref.shape
    half = width // 2
    greet(sp, tp, n_sp, n_tp)

    for i, dz in enumerate(Z_ORDER):
        at = ((z + dz) % 8) * 8
        for k in (1, 3, 2):
            to = (tp + k) % n_tp
            remote(
                part_ref.at[to, pl.ds(at, 8)], term_ref.at[k - 1, i],
                term_send.at[k - 1], term_recv.at[k - 1, i], sp, to,
            ).start()
    for i, dz in enumerate(Z_ORDER):
        at = ((z + dz) % 8) * 8
        total = part_ref[tp, pl.ds(at, 8)].astype(F32)
        for k in range(1, n_tp):
            wait_bytes(term_ref.at[k - 1, i], term_recv.at[k - 1, i])
            total = total + term_ref[k - 1, i].astype(F32)
        back_ref[pl.ds(at, 8)] = total.astype(BF16)

        def send(j, _):
            to = offset_device(z, x, c, dz, j)
            remote(back_ref.at[to], ret_ref.at[sp], ret_send, ret_recv, to, tp).start()
            return 0

        lax.fori_loop(1 if dz == 0 else 0, 8, send, 0)
    ret_ref[sp] = back_ref[sp]
    wait_bytes(ret_ref.at[pl.ds(0, n_sp - 1)], ret_recv)

    (main, tail), low = slot_tests(code_ref[...], n_sp)
    main_pick = jnp.where(main[0] | main[1], 1.0, 0.0).astype(BF16)
    in_tail = tail[0] | tail[1]
    low_pick = jnp.where(in_tail & low, 1.0, 0.0).astype(BF16)
    high_pick = jnp.where(in_tail & ~low, 1.0, 0.0).astype(BF16)
    first = ret_ref[:, :, :width].astype(F32).reshape(n_sp * 8, width).astype(BF16)
    second = ret_ref[:, :, width:].astype(F32).reshape(n_sp * 8, half).astype(BF16)
    rows = ((0,), (0,))
    summed = dot(main_pick, first, rows) + jnp.concatenate(
        [dot(low_pick, second, rows), dot(high_pick, second, rows)], axis=1
    )
    mix_ref[tp] = (d_out_ref[...].astype(F32) + summed).astype(BF16)
    for k in (1, 3, 2):
        to = (tp + k) % n_tp
        remote(mix_ref.at[tp], mix_ref.at[tp], mix_send.at[k - 1], mix_recv.at[k - 1], sp, to).start()

    def number(k, h):
        return 2 * ((tp + n_tp - k) % n_tp) + h

    slot_of = (0, 1, 3, 2)
    for n, k in enumerate(slot_of):
        q = (tp + n_tp - k) % n_tp
        if k:
            wait_bytes(mix_ref.at[q], mix_recv.at[k - 1])
        mixed = mix_ref[q]
        block = dot(mixed, w_out_ref[:, pl.ds(pl.multiple_of(q * width, width), width)], ((1,), (1,)))
        if n == 0:
            acc_ref[...] = block
        else:
            acc_ref[...] += block
        for h in (0, 1):
            slot = 2 * n + h
            grad = dot(mixed[:, h * half : (h + 1) * half], merged_ref[...], rows)
            grad = grad.reshape(4, 2, half // 8, width)
            keep_ref[slot] = jnp.where(c == 0, grad[:, 0], grad[:, 1])
            pair_ref[slot] = jnp.where(c == 0, grad[:, 1], grad[:, 0]).astype(BF16)
            remote(
                pair_ref.at[slot], pair_got.at[slot], pair_send, pair_recv.at[slot], sp + 1 - 2 * c, tp
            ).start()

    d_merged = acc_ref[...]
    gate_ref[...] = (d_merged * saved_ref[5]).astype(BF16)
    acc_ref[...] = d_merged * saved_ref[6]

    def back(group, carry):
        for i in range(8):
            t = pl.ds(tokens - 1 - (group * 8 + i), 1)
            grad = acc_ref[t, :] + carry
            local_ref[t, :] = grad
            carry = grad * saved_ref[0, t, :]
        return carry

    lead = lax.fori_loop(0, tokens // 8, back, jnp.zeros((1, width), F32))
    lead_ref[0, 0:1, :] = saved_ref[1, 0:1, :] * saved_ref[0, 0:1, :]
    lead_ref[0, 1:2, :] = lead
    lead_got[sp] = lead_ref[0]

    def tell(k, _):
        remote(lead_ref.at[0], lead_got.at[sp], lead_send, lead_recv, (sp + k) % n_sp, tp).start()
        return 0

    lax.fori_loop(1, n_sp, tell, 0)

    for slot in range(8):
        wait_bytes(pair_got.at[slot], pair_recv.at[slot])
        total = keep_ref[slot] + pair_got[slot].astype(F32)
        keep_ref[slot] = total
        x_ref[slot] = total.astype(BF16)
        for dx in (1, 3, 2):
            to = (x + dx) % 4
            remote(
                x_ref.at[slot, to], x_got.at[slot, dx - 1], x_send, x_recv.at[slot],
                z * 8 + to * 2 + c, tp,
            ).start()

    for slot in range(8):
        wait_bytes(x_got.at[slot], x_recv.at[slot])
        total = keep_ref[slot, x] + x_got[slot, 0].astype(F32) + x_got[slot, 1].astype(F32) + x_got[slot, 2].astype(F32)
        z_ref[slot] = total.astype(BF16)
        to = number(slot_of[slot // 2], slot % 2)

        @pl.when(to == z)
        def _():
            own_ref[...] = total

        @pl.when(to != z)
        def _():
            remote(z_ref.at[slot], z_got.at[z], z_send, z_recv, to * 8 + x * 2 + c, tp).start()

    wait_bytes(lead_got.at[pl.ds(0, n_sp - 1)], lead_recv)

    def later(k, carry):
        i = n_sp - 1 - k
        pair = lead_got[i]
        return jnp.where(i > sp, pair[1:2, :] + pair[0:1, :] * carry, carry)

    incoming = lax.fori_loop(0, n_sp, later, jnp.zeros((1, width), F32))
    heads, hd = wr_ref.shape[0], wr_ref.shape[1]
    for h in range(heads):
        cols = slice(h * hd, (h + 1) * hd)
        grad = local_ref[:, cols] + saved_ref[1, :, cols] * incoming[:, cols]
        by_reset = (grad * saved_ref[2, :, cols]).astype(BF16)
        by_input = (grad * saved_ref[3, :, cols]).astype(BF16)
        rec_ref[:, cols] = (
            grad * saved_ref[4, :, cols]
            + dot(by_reset, wr_ref[h], ((1,), (1,)))
            + dot(by_input, wi_ref[h], ((1,), (1,)))
        ).astype(BF16)

    wait_bytes(z_got.at[pl.ds(0, 7)], z_recv)
    total = own_ref[...]
    for d in range(1, 8):
        total = total + z_got[(z + d) % 8].astype(F32)
    proj_ref[...] = total

    for k in range(n_tp - 1):
        wait_bytes(part_ref.at[tp], term_send.at[k])
        wait_bytes(mix_ref.at[tp], mix_send.at[k])
    wait_bytes(back_ref.at[pl.ds(0, n_sp - 1)], ret_send)
    wait_bytes(pair_ref, pair_send)
    wait_bytes(x_ref.at[:, pl.ds(0, 3)], x_send)
    wait_bytes(z_ref.at[pl.ds(0, 7)], z_send)
    wait_bytes(lead_got.at[pl.ds(0, n_sp - 1)], lead_send)


def tail(part, codes, d_out, saved, merged, w_out, w_reset, w_input):
    n_tp, n_sp, _, packed = part.shape
    tokens, width = d_out.shape
    own_rows = n_tp * width // n_sp
    dma = pltpu.SemaphoreType.DMA
    block = (own_rows, width)
    return pl.pallas_call(
        tail_kernel,
        out_shape=(
            jax.ShapeDtypeStruct(block, F32),
            jax.ShapeDtypeStruct((tokens, width), BF16),
            jax.ShapeDtypeStruct((tokens, width), BF16),
        ),
        in_specs=[VM] * 8,
        out_specs=(VM,) * 3,
        scratch_shapes=[
            pltpu.VMEM((3, 8, 8, 8, packed), BF16),
            pltpu.VMEM((n_sp, 8, packed), BF16),
            pltpu.VMEM((n_sp, 8, packed), BF16),
            pltpu.VMEM((n_tp, tokens, width), BF16),
            pltpu.VMEM((tokens, width), F32),
            pltpu.VMEM((tokens, width), F32),
            pltpu.VMEM((8, 4, *block), F32),
            pltpu.VMEM((8, 4, *block), BF16),
            pltpu.VMEM((8, 4, *block), BF16),
            pltpu.VMEM((8, 4, *block), BF16),
            pltpu.VMEM((8, 3, *block), BF16),
            pltpu.VMEM((8, *block), BF16),
            pltpu.VMEM((8, *block), BF16),
            pltpu.VMEM(block, F32),
            pltpu.VMEM((1, 2, width), F32),
            pltpu.VMEM((n_sp, 2, width), F32),
            dma((3,)), dma((3, 8)), dma, dma, dma((3,)), dma((3,)), dma, dma((8,)),
            dma, dma((8,)), dma, dma, dma, dma,
        ],
        compiler_params=pltpu.CompilerParams(
            collective_id=1, has_side_effects=True, vmem_limit_bytes=56 * 2**20
        ),
        name="return_and_tail",
    )(part, codes, d_out, saved, merged, w_out, w_reset, w_input)


def body(
    n_sp, n_tp, conv_out, gate_in, block_states, decay_param, decay_shift, w_reset, w_input, w_out,
    mixed, d_out, expert_ids, route_weights, w_gate, w_up, w_down,
):
    slow = jax.nn.softplus(-decay_param)[None, :]
    send, codes = pack(expert_ids.T, route_weights.T, d_out, mixed, n_sp)
    got = dispatch(send, n_tp)
    saved, merged = forward(conv_out, gate_in, block_states, slow, decay_shift[:, None], w_reset, w_input)
    grad_gate_e, grad_up_e, grad_down_e, part = experts_back(got, w_gate[0], w_up[0], w_down[0])
    proj, rec, grad_gate = tail(part, codes, d_out, saved, merged, w_out, w_reset, w_input)
    return grad_gate_e[None], grad_up_e[None], grad_down_e[None], proj, rec, grad_gate


def solution(mesh):
    in_specs = (
        P("sp", "tp"), P("sp", "tp"), P("sp", "tp"), P("tp"), P("sp"),
        P("tp", None, None), P("tp", None, None), P("tp", None),
        P("sp", "tp"), P("sp", "tp"), P("sp", None), P("sp", None),
        P("sp", None, "tp"), P("sp", None, "tp"), P("sp", "tp", None),
    )
    out_specs = (
        P("sp", None, "tp"), P("sp", None, "tp"), P("sp", "tp", None),
        P("sp", "tp"), P("sp", "tp"), P("sp", "tp"),
    )
    run = functools.partial(body, mesh.shape["sp"], mesh.shape["tp"])
    return jax.shard_map(run, mesh=mesh, in_specs=in_specs, out_specs=out_specs, check_vma=False)
```

```python
import functools

import jax
import jax.numpy as jnp
from jax import lax
from jax.experimental import pallas as pl
from jax.experimental.pallas import tpu as pltpu
from jax.sharding import PartitionSpec as P

F32 = jnp.float32
BF16 = jnp.bfloat16
MESH = pl.DeviceIdType.MESH
VM = pl.BlockSpec(memory_space=pltpu.VMEM)
ANY = pl.BlockSpec(memory_space=pl.ANY)


def dot(a, b, dims=((1,), (0,))):
    return lax.dot_general(a, b, (dims, ((), ())), preferred_element_type=F32)


def swap4(value):
    return pltpu.roll(value, 4, axis=1)


def low_half(shape):
    return lax.broadcasted_iota(jnp.int32, shape, 1) < 4


def gates(conv_ref, slow_ref, shift_ref, wr_ref, wi_ref, saved_ref, drive_ref, reset_ref, norm_ref, inp_ref):
    hd = wr_ref.shape[1]
    rows = conv_ref.shape[0]
    shift = jnp.transpose(jnp.broadcast_to(shift_ref[...], (8, rows)))[:, 0:1]
    for h in range(wr_ref.shape[0]):
        cols = slice(h * hd, (h + 1) * hd)
        conv = conv_ref[:, cols]
        reset = jax.nn.sigmoid(dot(conv, wr_ref[h]))
        inp = jax.nn.sigmoid(dot(conv, wi_ref[h]))
        log_decay = -8.0 * reset * slow_ref[:, cols] + shift
        decay = jnp.exp(log_decay)
        twice = 2.0 * log_decay
        small = jnp.maximum(twice, -0.5)
        series = 1.0 + small * (1.0 / 10.0)
        for n in (9, 8, 7, 6, 5, 4, 3, 2):
            series = 1.0 + small * (1.0 / n) * series
        less = jnp.where(twice > -0.5, small * series, jnp.exp(twice) - 1.0)
        norm = jnp.sqrt(-less)
        saved_ref[0, :, cols] = decay
        reset_ref[:, cols] = reset
        norm_ref[:, cols] = norm
        inp_ref[:, cols] = inp
        drive_ref[:, cols] = norm * inp * conv.astype(F32)


def run_forward(first_ref, saved_ref, drive_ref, prev_ref, state_ref):
    rows, width = drive_ref.shape

    def step(group, state):
        for i in range(8):
            t = pl.ds(group * 8 + i, 1)
            prev_ref[t, :] = state
            state = saved_ref[0, t, :] * state + drive_ref[t, :]
            state_ref[t, :] = state
        return state

    lax.fori_loop(0, rows // 8, step, first_ref[...])

    def back(group, prod):
        for i in range(8):
            t = rows - 1 - (group * 8 + i)
            saved_ref[1, pl.ds(t, 1), :] = prod
            prod = prod * saved_ref[0, pl.ds(t, 1), :]
        return prod

    lax.fori_loop(0, rows // 8, back, jnp.ones((1, width), F32))


def factors(
    conv_ref, gate_ref, slow_ref, saved_ref, merged_ref, prev_ref, state_ref, reset_ref, norm_ref, inp_ref
):
    hd = 128
    for h in range(conv_ref.shape[1] // hd):
        cols = slice(h * hd, (h + 1) * hd)
        conv = conv_ref[:, cols].astype(F32)
        decay, reset, norm, inp = saved_ref[0, :, cols], reset_ref[:, cols], norm_ref[:, cols], inp_ref[:, cols]
        by_log = decay * prev_ref[:, cols] - inp * conv * decay * decay / norm
        saved_ref[2, :, cols] = by_log * (-8.0 * slow_ref[:, cols]) * reset * (1.0 - reset)
        saved_ref[3, :, cols] = norm * conv * inp * (1.0 - inp)
        saved_ref[4, :, cols] = norm * inp
        state = state_ref[:, cols]
        value = gate_ref[:, cols].astype(F32)
        k = 0.7978845608028654
        square = value * value
        bent = jnp.tanh(k * (value + 0.044715 * value * square))
        act = 0.5 * value * (1.0 + bent)
        slope = 0.5 * (1.0 + bent) + 0.5 * value * (1.0 - bent * bent) * k * (1.0 + 3.0 * 0.044715 * square)
        saved_ref[5, :, cols] = state * slope
        saved_ref[6, :, cols] = act
        merged_ref[:, cols] = (act * state).astype(BF16)


def slot_tests(codes, experts):
    tokens = codes.shape[1]
    row = lax.broadcasted_iota(jnp.int32, (experts * 8, tokens), 0)
    base = (row // 8) * 16
    main = base + row % 8
    tail = base + 8 + row % 4
    return [[codes[k : k + 1, :] == want for k in (0, 1)] for want in (main, tail)], row % 8 < 4


def pack(ids_ref, wts_ref, d_out_ref, mixed_ref, send_ref, code_ref):
    experts = send_ref.shape[0]
    tokens, width = d_out_ref.shape
    half = width // 2
    each = lax.broadcasted_iota(jnp.int32, (experts, tokens), 0)
    named = [ids_ref[k : k + 1, :] == each for k in (0, 1)]
    both = jnp.where(named[0] | named[1], 1.0, 0.0).astype(BF16)
    earlier = (
        lax.broadcasted_iota(jnp.int32, (tokens, tokens), 0)
        < lax.broadcasted_iota(jnp.int32, (tokens, tokens), 1)
    )
    count = dot(both, jnp.where(earlier, 1.0, 0.0).astype(BF16))
    codes = []
    for k in (0, 1):
        rank = jnp.sum(jnp.where(named[k], count, 0.0), axis=0, keepdims=True)
        codes.append(ids_ref[k : k + 1, :] * 16 + rank.astype(jnp.int32))
        code_ref[k : k + 1, :] = codes[k]
    codes = jnp.concatenate(codes, axis=0)
    (main, tail), low = slot_tests(codes, experts)

    def weight(tests):
        return jnp.sum(
            jnp.where(tests[0], wts_ref[0:1, :], 0.0) + jnp.where(tests[1], wts_ref[1:2, :], 0.0),
            axis=1,
            keepdims=True,
        )

    main_pick = jnp.where(main[0] | main[1], 1.0, 0.0).astype(BF16)
    in_tail = tail[0] | tail[1]
    low_pick = jnp.where(in_tail & low, 1.0, 0.0).astype(BF16)
    high_pick = jnp.where(in_tail & ~low, 1.0, 0.0).astype(BF16)

    for at, (ref, w_main, w_tail) in enumerate(
        ((d_out_ref, weight(main), weight(tail)), (mixed_ref, None, None))
    ):
        first = dot(main_pick, ref[...])
        second = dot(low_pick, ref[:, :half]) + dot(high_pick, ref[:, half:])
        if w_main is not None:
            first, second = first * w_main, second * w_tail
        rows = slice(at * 8, at * 8 + 8)
        send_ref[:, rows, :width] = first.reshape(experts, 8, width).astype(BF16)
        send_ref[:, rows, width:] = second.reshape(experts, 8, half).astype(BF16)


def place():
    sp, tp = lax.axis_index("sp"), lax.axis_index("tp")
    return sp, tp, sp // 8, (sp // 2) % 4, sp % 2


def z_offset(i):
    return ((i % 2) * ((i + 1) // 2) + (1 - i % 2) * (8 - i // 2)) % 8


def offset_device(z, x, c, dz, j):
    return ((z + dz) % 8) * 8 + ((x + j // 2) % 4) * 2 + (c + j % 2) % 2


def greet(sp, tp, n_sp, n_tp):
    barrier = pltpu.get_barrier_semaphore()

    def to_sp(k, _):
        pl.semaphore_signal(barrier, inc=1, device_id=((sp + k) % n_sp, tp), device_id_type=MESH)
        return 0

    lax.fori_loop(1, n_sp, to_sp, 0)
    for k in range(1, n_tp):
        pl.semaphore_signal(barrier, inc=1, device_id=(sp, (tp + k) % n_tp), device_id_type=MESH)


def all_here(n_sp, n_tp):
    pl.semaphore_wait(pltpu.get_barrier_semaphore(), n_sp - 1 + n_tp - 1)


def remote(src, dst, send_sem, recv_sem, sp, tp):
    return pltpu.make_async_remote_copy(
        src_ref=src, dst_ref=dst, send_sem=send_sem, recv_sem=recv_sem,
        device_id=(sp, tp), device_id_type=MESH,
    )


def wait_bytes(ref, sem):
    pltpu.make_async_copy(ref, ref, sem).wait()


def unpack(got_ref, q, at, row, rows_ref, cot_ref):
    packed = got_ref.shape[3]
    width, half = packed * 2 // 3, packed // 3
    cols = slice(q * width, (q + 1) * width)
    for first, ref in ((0, cot_ref), (8, rows_ref)):
        block = got_ref[q, pl.ds(at, 8), first : first + 8, :].astype(F32)
        ref[pl.ds(row, 64), cols] = block[:, :, :width].reshape(64, width).astype(BF16)
        tails = block[:, :, width:]
        turned = swap4(tails)
        tails, turned = tails.reshape(4, 2, 8, half), turned.reshape(4, 2, 8, half)
        low = low_half((4, 8, half))
        left = jnp.where(low, tails[:, 0], turned[:, 1])
        right = jnp.where(low, turned[:, 0], tails[:, 1])
        both = jnp.concatenate([left, right], axis=2).reshape(32, width)
        ref[pl.ds(row + 64, 32), cols] = both.astype(BF16)


def expert_terms(row, rows_ref, cot_ref, grad_ref, hidden_ref, wboth_ref, wd_ref):
    fe = wd_ref.shape[0]
    rows = pl.ds(row, 96)
    both = dot(rows_ref[rows, :], wboth_ref[...])
    up_pre, linear = both[:, :fe], both[:, fe:]
    d_hidden = dot(cot_ref[rows, :], wd_ref[...], ((1,), (1,)))
    gate = jax.nn.sigmoid(up_pre)
    silu = up_pre * gate
    hidden_ref[rows, :] = (silu * linear).astype(BF16)
    d_linear = (d_hidden * silu).astype(BF16)
    d_up = (d_hidden * linear * gate * (1.0 + up_pre * (1.0 - gate))).astype(BF16)
    grad_ref[rows, :fe] = d_up
    grad_ref[rows, fe:] = d_linear


def row_part(q, at, row, grad_ref, wboth_ref, part_ref):
    packed = part_ref.shape[3]
    width, half = packed * 2 // 3, packed // 3
    part = dot(grad_ref[pl.ds(row, 96), :], wboth_ref[q * width : (q + 1) * width, :], ((1,), (1,)))
    part_ref[q, pl.ds(at, 8), :, :width] = part[:64].reshape(8, 8, width).astype(BF16)
    tails = part[64:].reshape(4, 8, width)
    left, right = tails[:, :, :half], tails[:, :, half:]
    low = low_half((4, 8, half))
    one = jnp.where(low, left, swap4(right))
    two = jnp.where(low, swap4(left), right)
    part_ref[q, pl.ds(at, 8), :, width:] = jnp.stack([one, two], axis=1).reshape(8, 8, half).astype(BF16)


STAGES = (0, 2, 3, 4, 5)
GROUPS = 8


def step_kernel(
    conv_ref, gate_in_ref, first_ref, slow_ref, shift_ref, wr_ref, wi_ref, wo_hbm, mixed_ref, d_out_ref,
    ids_ref, wts_ref, wg_hbm, wu_hbm, wd_hbm,
    both_hbm, down_hbm, proj_ref, rec_ref, gate_ref,
    send_ref, code_ref, got_ref, rows_ref, cot_ref, grad_ref, hidden_ref, part_ref, far_ref, comb_ref,
    near_ref, back_ref, ret_ref, saved_ref, merged_ref, temp_ref, wboth_ref, wd_ref, wo_ref, both_ref,
    down_ref, mix_ref, acc_ref, local_ref, keep_ref, pair_ref, pair_got, x_ref, x_got, z_ref, z_got,
    own_ref, lead_ref, lead_got,
    load_sem, store_sem, send_sem, recv_sem, y_send, y_recv, f_send, f_recv, far_send, far_recv,
    near_send, near_recv, ret_send, ret_recv, mix_send, mix_recv, pair_send, pair_recv,
    x_send, x_recv, z_send, z_recv, lead_send, lead_recv,
):
    sp, tp, z, x, c = place()
    n_tp, n_sp = part_ref.shape[0], part_ref.shape[1]
    tokens, width = d_out_ref.shape
    half = width // 2
    fe = wd_ref.shape[0]
    right, left, far = (tp + 1) % n_tp, (tp + n_tp - 1) % n_tp, (tp + 2) % n_tp
    drive_ref, prev_ref, state_ref, reset_ref, norm_ref, inp_ref = [temp_ref.at[k] for k in range(6)]

    greet(sp, tp, n_sp, n_tp)
    loads = [
        pltpu.make_async_copy(src, dst, load_sem.at[k])
        for k, (src, dst) in enumerate((
            (wg_hbm, wboth_ref.at[:, pl.ds(0, fe)]), (wu_hbm, wboth_ref.at[:, pl.ds(fe, fe)]),
            (wd_hbm, wd_ref), (wo_hbm, wo_ref),
        ))
    ]
    for load in loads:
        load.start()
    pack(ids_ref, wts_ref, d_out_ref, mixed_ref, send_ref, code_ref)
    got_ref[tp, sp] = send_ref[sp]
    all_here(n_sp, n_tp)

    def send_group(i, _):
        def send(j, _):
            to = offset_device(z, x, c, z_offset(i), j)
            remote(send_ref.at[to], got_ref.at[tp, sp], send_sem, recv_sem.at[i], to, tp).start()
            return 0

        lax.fori_loop(jnp.where(i == 0, 1, 0), 8, send, 0)
        return 0

    lax.fori_loop(0, GROUPS, send_group, 0)

    def source_group(i):
        return (z + 8 - z_offset(i)) % 8

    def gather(i):
        at = source_group(i) * 8

        @pl.when(i == 0)
        def _():
            wait_bytes(got_ref.at[tp, pl.ds(at, 7)], recv_sem.at[i])

        @pl.when(i > 0)
        def _():
            wait_bytes(got_ref.at[tp, pl.ds(at, 8)], recv_sem.at[i])

        block = got_ref.at[tp, pl.ds(at, 8)]
        remote(block, block, y_send.at[0], y_recv.at[0, i], sp, right).start()
        remote(block, block, y_send.at[1], y_recv.at[1, i], sp, left).start()

    def relay(i):
        at = source_group(i) * 8
        wait_bytes(got_ref.at[left, pl.ds(at, 8)], y_recv.at[0, i])
        block = got_ref.at[left, pl.ds(at, 4)]
        remote(block, block, f_send.at[0], f_recv.at[0, i], sp, right).start()
        wait_bytes(got_ref.at[right, pl.ds(at, 8)], y_recv.at[1, i])
        block = got_ref.at[right, pl.ds(at + 4, 4)]
        remote(block, block, f_send.at[1], f_recv.at[1, i], sp, left).start()

    def compute(i):
        group = source_group(i)
        at, row = group * 8, pl.multiple_of(group * 96, 32)
        wait_bytes(got_ref.at[far, pl.ds(at, 4)], f_recv.at[0, i])
        wait_bytes(got_ref.at[far, pl.ds(at + 4, 4)], f_recv.at[1, i])
        for q in range(n_tp):
            unpack(got_ref, q, at, row, rows_ref, cot_ref)
        expert_terms(row, rows_ref, cot_ref, grad_ref, hidden_ref, wboth_ref, wd_ref)
        for q in range(n_tp):
            row_part(q, at, row, grad_ref, wboth_ref, part_ref)
        lower, upper = pl.ds(at, 4), pl.ds(at + 4, 4)
        remote(part_ref.at[far, lower], far_ref.at[0, i], far_send.at[0], far_recv.at[0, i], sp, left).start()
        remote(part_ref.at[far, upper], far_ref.at[1, i], far_send.at[1], far_recv.at[1, i], sp, right).start()
        remote(
            part_ref.at[left, upper], near_ref.at[0, i, pl.ds(4, 4)], near_send.at[0], near_recv.at[0, i], sp, left
        ).start()
        remote(
            part_ref.at[right, lower], near_ref.at[1, i, pl.ds(0, 4)], near_send.at[1], near_recv.at[1, i], sp, right
        ).start()

    def add_far(i):
        at = source_group(i) * 8
        for side, (to, first) in enumerate(((left, 0), (right, 4))):
            wait_bytes(far_ref.at[side, i], far_recv.at[side, i])
            own = part_ref[to, pl.ds(at + first, 4)].astype(F32)
            comb_ref[side, i] = (own + far_ref[side, i].astype(F32)).astype(BF16)
            remote(
                comb_ref.at[side, i], near_ref.at[side, i, pl.ds(first, 4)],
                near_send.at[side], near_recv.at[side, i], sp, to,
            ).start()

    def give_back(i):
        group = source_group(i)
        at = group * 8
        wait_bytes(near_ref.at[0, i], near_recv.at[0, i])
        wait_bytes(near_ref.at[1, i], near_recv.at[1, i])
        total = part_ref[tp, pl.ds(at, 8)].astype(F32) + near_ref[0, i].astype(F32) + near_ref[1, i].astype(F32)
        back_ref[pl.ds(at, 8)] = total.astype(BF16)

        def send(j, _):
            to = group * 8 + ((x + j // 2) % 4) * 2 + (c + j % 2) % 2
            remote(back_ref.at[to], ret_ref.at[sp], ret_send, ret_recv, to, tp).start()
            return 0

        lax.fori_loop(jnp.where(i == 0, 1, 0), 8, send, 0)

    def step(s, _):
        for lag, stage in zip(STAGES, (gather, relay, compute, add_far, give_back)):
            if stage is compute:

                @pl.when(s == lag)
                def _():
                    for load in loads[:3]:
                        load.wait()

            @pl.when(jnp.logical_and(s >= lag, s < lag + GROUPS))
            def _():
                stage(s - lag)

        @pl.when(s == 0)
        def _():
            gates(conv_ref, slow_ref, shift_ref, wr_ref, wi_ref, saved_ref, drive_ref, reset_ref, norm_ref, inp_ref)

        @pl.when(s == 1)
        def _():
            run_forward(first_ref, saved_ref, drive_ref, prev_ref, state_ref)

        @pl.when(s == 2)
        def _():
            factors(
                conv_ref, gate_in_ref, slow_ref, saved_ref, merged_ref, prev_ref, state_ref, reset_ref,
                norm_ref, inp_ref,
            )

        return 0

    lax.fori_loop(0, GROUPS + STAGES[-1], step, 0)

    over_rows = ((0,), (0,))

    def weight_grads(k, _):
        cols = pl.ds(pl.multiple_of(k * 512, 512), 512)
        both_ref[cols, :] = dot(rows_ref[:, cols], grad_ref[...], over_rows).astype(BF16)
        down_ref[:, cols] = dot(hidden_ref[...], cot_ref[:, cols], over_rows).astype(BF16)
        return 0

    lax.fori_loop(0, rows_ref.shape[1] // 512, weight_grads, 0)
    stores = [
        pltpu.make_async_copy(both_ref, both_hbm, store_sem.at[0]),
        pltpu.make_async_copy(down_ref, down_hbm, store_sem.at[1]),
    ]
    for store in stores:
        store.start()

    (main, tail), low = slot_tests(code_ref[...], n_sp)
    main_pick = jnp.where(main[0] | main[1], 1.0, 0.0).astype(BF16)
    in_tail = tail[0] | tail[1]
    low_pick = jnp.where(in_tail & low, 1.0, 0.0).astype(BF16)
    high_pick = jnp.where(in_tail & ~low, 1.0, 0.0).astype(BF16)
    ret_ref[sp] = back_ref[sp]
    wait_bytes(ret_ref.at[pl.ds(0, n_sp - 1)], ret_recv)
    main_rows = ret_ref[:, :, :width].astype(F32).reshape(n_sp * 8, width).astype(BF16)
    tail_rows = ret_ref[:, :, width:].astype(F32).reshape(n_sp * 8, half).astype(BF16)
    summed = dot(main_pick, main_rows, over_rows) + jnp.concatenate(
        [dot(low_pick, tail_rows, over_rows), dot(high_pick, tail_rows, over_rows)], axis=1
    )
    mix_ref[tp] = (d_out_ref[...].astype(F32) + summed).astype(BF16)
    for k in (1, 3, 2):
        to = (tp + k) % n_tp
        remote(mix_ref.at[tp], mix_ref.at[tp], mix_send.at[k - 1], mix_recv.at[k - 1], sp, to).start()
    loads[3].wait()

    slot_of = (0, 1, 3, 2)
    for n, k in enumerate(slot_of):
        q = (tp + n_tp - k) % n_tp
        if k:
            wait_bytes(mix_ref.at[q], mix_recv.at[k - 1])
        whole = mix_ref[q]
        block = dot(whole, wo_ref[:, pl.ds(pl.multiple_of(q * width, width), width)], ((1,), (1,)))
        if n == 0:
            acc_ref[...] = block
        else:
            acc_ref[...] += block
        for h in (0, 1):
            slot = 2 * n + h
            grad = dot(whole[:, h * half : (h + 1) * half], merged_ref[...], over_rows)
            grad = grad.reshape(4, 2, half // 8, width)
            keep_ref[slot] = jnp.where(c == 0, grad[:, 0], grad[:, 1])
            pair_ref[slot] = jnp.where(c == 0, grad[:, 1], grad[:, 0]).astype(BF16)
            remote(
                pair_ref.at[slot], pair_got.at[slot], pair_send, pair_recv.at[slot], sp + 1 - 2 * c, tp
            ).start()

    d_merged = acc_ref[...]
    gate_ref[...] = (d_merged * saved_ref[5]).astype(BF16)
    acc_ref[...] = d_merged * saved_ref[6]

    def back(group, carry):
        for i in range(8):
            t = pl.ds(tokens - 1 - (group * 8 + i), 1)
            grad = acc_ref[t, :] + carry
            local_ref[t, :] = grad
            carry = grad * saved_ref[0, t, :]
        return carry

    lead = lax.fori_loop(0, tokens // 8, back, jnp.zeros((1, width), F32))
    lead_ref[0, 0:1, :] = saved_ref[1, 0:1, :] * saved_ref[0, 0:1, :]
    lead_ref[0, 1:2, :] = lead
    lead_got[sp] = lead_ref[0]

    def tell(k, _):
        remote(lead_ref.at[0], lead_got.at[sp], lead_send, lead_recv, (sp + k) % n_sp, tp).start()
        return 0

    lax.fori_loop(1, n_sp, tell, 0)

    for slot in range(8):
        wait_bytes(pair_got.at[slot], pair_recv.at[slot])
        total = keep_ref[slot] + pair_got[slot].astype(F32)
        keep_ref[slot] = total
        x_ref[slot] = total.astype(BF16)
        for dx in (1, 3, 2):
            to = (x + dx) % 4
            remote(
                x_ref.at[slot, to], x_got.at[slot, dx - 1], x_send, x_recv.at[slot],
                z * 8 + to * 2 + c, tp,
            ).start()

    for slot in range(8):
        wait_bytes(x_got.at[slot], x_recv.at[slot])
        total = keep_ref[slot, x] + x_got[slot, 0].astype(F32) + x_got[slot, 1].astype(F32) + x_got[slot, 2].astype(F32)
        z_ref[slot] = total.astype(BF16)
        to = 2 * ((tp + n_tp - slot_of[slot // 2]) % n_tp) + slot % 2

        @pl.when(to == z)
        def _():
            own_ref[...] = total

        @pl.when(to != z)
        def _():
            remote(z_ref.at[slot], z_got.at[z], z_send, z_recv, to * 8 + x * 2 + c, tp).start()

    wait_bytes(lead_got.at[pl.ds(0, n_sp - 1)], lead_recv)

    def later(k, carry):
        i = n_sp - 1 - k
        pair = lead_got[i]
        return jnp.where(i > sp, pair[1:2, :] + pair[0:1, :] * carry, carry)

    incoming = lax.fori_loop(0, n_sp, later, jnp.zeros((1, width), F32))
    heads, hd = wr_ref.shape[0], wr_ref.shape[1]
    for h in range(heads):
        cols = slice(h * hd, (h + 1) * hd)
        grad = local_ref[:, cols] + saved_ref[1, :, cols] * incoming[:, cols]
        by_reset = (grad * saved_ref[2, :, cols]).astype(BF16)
        by_input = (grad * saved_ref[3, :, cols]).astype(BF16)
        rec_ref[:, cols] = (
            grad * saved_ref[4, :, cols]
            + dot(by_reset, wr_ref[h], ((1,), (1,)))
            + dot(by_input, wi_ref[h], ((1,), (1,)))
        ).astype(BF16)

    wait_bytes(z_got.at[pl.ds(0, 7)], z_recv)
    total = own_ref[...]
    for d in range(1, 8):
        total = total + z_got[(z + d) % 8].astype(F32)
    proj_ref[...] = total

    wait_bytes(send_ref.at[pl.ds(0, n_sp - 1)], send_sem)
    for side in (0, 1):
        wait_bytes(got_ref.at[tp], y_send.at[side])
        wait_bytes(got_ref.at[tp, pl.ds(0, n_sp // 2)], f_send.at[side])
        wait_bytes(part_ref.at[tp, pl.ds(0, n_sp // 2)], far_send.at[side])
        wait_bytes(part_ref.at[tp], near_send.at[side])
    for k in range(n_tp - 1):
        wait_bytes(mix_ref.at[tp], mix_send.at[k])
    wait_bytes(back_ref.at[pl.ds(0, n_sp - 1)], ret_send)
    wait_bytes(pair_ref, pair_send)
    wait_bytes(x_ref.at[:, pl.ds(0, 3)], x_send)
    wait_bytes(z_ref.at[pl.ds(0, 7)], z_send)
    wait_bytes(lead_got.at[pl.ds(0, n_sp - 1)], lead_send)
    for store in stores:
        store.wait()


def whole_step(n_sp, n_tp, *args):
    conv, w_gate = args[0], args[12]
    tokens, width = conv.shape
    model, fe = w_gate.shape
    packed = width + width // 2
    rows = n_sp * 12
    block = (model // n_sp, width)
    dma = pltpu.SemaphoreType.DMA
    specs = [VM] * 15
    for k in (7, 12, 13, 14):
        specs[k] = ANY
    return pl.pallas_call(
        step_kernel,
        out_shape=(
            jax.ShapeDtypeStruct((model, 2 * fe), BF16),
            jax.ShapeDtypeStruct((fe, model), BF16),
            jax.ShapeDtypeStruct(block, F32),
            jax.ShapeDtypeStruct((tokens, width), BF16),
            jax.ShapeDtypeStruct((tokens, width), BF16),
        ),
        in_specs=specs,
        out_specs=(ANY, ANY, VM, VM, VM),
        scratch_shapes=[
            pltpu.VMEM((n_sp, 16, packed), BF16),
            pltpu.VMEM((2, tokens), jnp.int32),
            pltpu.VMEM((n_tp, n_sp, 16, packed), BF16),
            pltpu.VMEM((rows, model), BF16),
            pltpu.VMEM((rows, model), BF16),
            pltpu.VMEM((rows, 2 * fe), BF16),
            pltpu.VMEM((rows, fe), BF16),
            pltpu.VMEM((n_tp, n_sp, 8, packed), BF16),
            pltpu.VMEM((2, GROUPS, 4, 8, packed), BF16),
            pltpu.VMEM((2, GROUPS, 4, 8, packed), BF16),
            pltpu.VMEM((2, GROUPS, 8, 8, packed), BF16),
            pltpu.VMEM((n_sp, 8, packed), BF16),
            pltpu.VMEM((n_sp, 8, packed), BF16),
            pltpu.VMEM((7, tokens, width), F32),
            pltpu.VMEM((tokens, width), BF16),
            pltpu.VMEM((6, tokens, width), F32),
            pltpu.VMEM((model, 2 * fe), BF16),
            pltpu.VMEM((fe, model), BF16),
            pltpu.VMEM((width, model), BF16),
            pltpu.VMEM((model, 2 * fe), BF16),
            pltpu.VMEM((fe, model), BF16),
            pltpu.VMEM((n_tp, tokens, width), BF16),
            pltpu.VMEM((tokens, width), F32),
            pltpu.VMEM((tokens, width), F32),
            pltpu.VMEM((8, 4, *block), F32),
            pltpu.VMEM((8, 4, *block), BF16),
            pltpu.VMEM((8, 4, *block), BF16),
            pltpu.VMEM((8, 4, *block), BF16),
            pltpu.VMEM((8, 3, *block), BF16),
            pltpu.VMEM((8, *block), BF16),
            pltpu.VMEM((8, *block), BF16),
            pltpu.VMEM(block, F32),
            pltpu.VMEM((1, 2, width), F32),
            pltpu.VMEM((n_sp, 2, width), F32),
            dma((4,)), dma((2,)), dma, dma((8,)), dma((2,)), dma((2, 8)), dma((2,)), dma((2, 8)),
            dma((2,)), dma((2, 8)), dma((2,)), dma((2, 8)), dma, dma, dma((3,)), dma((3,)),
            dma, dma((8,)), dma, dma((8,)), dma, dma, dma, dma,
        ],
        compiler_params=pltpu.CompilerParams(
            collective_id=0, has_side_effects=True, vmem_limit_bytes=63 * 2**20
        ),
        name="whole_step",
    )(*args)


def write_kernel(both_ref, down_ref, proj_ref, rec_ref, gate_ref, gg_ref, gu_ref, gd_ref, p_ref, r_ref, g_ref):
    fe = gg_ref.shape[1]
    gg_ref[...] = both_ref[:, :fe].astype(F32)
    gu_ref[...] = both_ref[:, fe:].astype(F32)
    gd_ref[...] = down_ref[...].astype(F32)
    p_ref[...] = proj_ref[...]
    r_ref[...] = rec_ref[...]
    g_ref[...] = gate_ref[...]


def write_out(both, down, proj, rec, gate, parts=4):
    model, fe = both.shape[0], both.shape[1] // 2

    def cut(array):
        return pl.BlockSpec((array.shape[0] // parts, array.shape[1]), lambda i: (i, 0))

    outs = (
        jax.ShapeDtypeStruct((model, fe), F32),
        jax.ShapeDtypeStruct((model, fe), F32),
        jax.ShapeDtypeStruct((fe, model), F32),
        jax.ShapeDtypeStruct(proj.shape, proj.dtype),
        jax.ShapeDtypeStruct(rec.shape, rec.dtype),
        jax.ShapeDtypeStruct(gate.shape, gate.dtype),
    )
    ins = (both, down, proj, rec, gate)
    return pl.pallas_call(
        write_kernel,
        grid=(parts,),
        out_shape=outs,
        in_specs=[cut(a) for a in ins],
        out_specs=tuple(cut(a) for a in outs),
        name="write_out",
    )(*ins)


def body(
    n_sp, n_tp, conv_out, gate_in, block_states, decay_param, decay_shift, w_reset, w_input, w_out,
    mixed, d_out, expert_ids, route_weights, w_gate, w_up, w_down,
):
    slow = jax.nn.softplus(-decay_param)[None, :]
    both, down, proj, rec, gate = whole_step(
        n_sp, n_tp, conv_out, gate_in, block_states, slow, decay_shift[None, :], w_reset, w_input, w_out,
        mixed, d_out, expert_ids.T, route_weights.T, w_gate[0], w_up[0], w_down[0],
    )
    gg, gu, gd, proj, rec, gate = write_out(both, down, proj, rec, gate)
    return gg[None], gu[None], gd[None], proj, rec, gate


def solution(mesh):
    in_specs = (
        P("sp", "tp"), P("sp", "tp"), P("sp", "tp"), P("tp"), P("sp"),
        P("tp", None, None), P("tp", None, None), P("tp", None),
        P("sp", "tp"), P("sp", "tp"), P("sp", None), P("sp", None),
        P("sp", None, "tp"), P("sp", None, "tp"), P("sp", "tp", None),
    )
    out_specs = (
        P("sp", None, "tp"), P("sp", None, "tp"), P("sp", "tp", None),
        P("sp", "tp"), P("sp", "tp"), P("sp", "tp"),
    )
    run = functools.partial(body, mesh.shape["sp"], mesh.shape["tp"])
    return jax.shard_map(run, mesh=mesh, in_specs=in_specs, out_specs=out_specs, check_vma=False)
```

```python
import functools

import jax
import jax.numpy as jnp
from jax import lax
from jax.experimental import pallas as pl
from jax.experimental.pallas import tpu as pltpu
from jax.sharding import PartitionSpec as P

F32 = jnp.float32
BF16 = jnp.bfloat16
MESH = pl.DeviceIdType.MESH
VM = pl.BlockSpec(memory_space=pltpu.VMEM)
ANY = pl.BlockSpec(memory_space=pl.ANY)


def dot(a, b, dims=((1,), (0,))):
    return lax.dot_general(a, b, (dims, ((), ())), preferred_element_type=F32)


def swap4(value):
    return pltpu.roll(value, 4, axis=1)


def low_half(shape):
    return lax.broadcasted_iota(jnp.int32, shape, 1) < 4


def gates(conv_ref, param_ref, slow_ref, shift_ref, wr_ref, wi_ref, saved_ref, drive_ref, reset_ref, norm_ref, inp_ref):
    hd = wr_ref.shape[1]
    rows = conv_ref.shape[0]
    shift = jnp.transpose(jnp.broadcast_to(shift_ref[...], (8, rows)))[:, 0:1]
    param = param_ref[...]
    slow_ref[...] = jnp.maximum(-param, 0.0) + jnp.log1p(jnp.exp(-jnp.abs(param)))
    for h in range(wr_ref.shape[0]):
        cols = slice(h * hd, (h + 1) * hd)
        conv = conv_ref[:, cols]
        reset = jax.nn.sigmoid(dot(conv, wr_ref[h]))
        inp = jax.nn.sigmoid(dot(conv, wi_ref[h]))
        log_decay = -8.0 * reset * slow_ref[:, cols] + shift
        decay = jnp.exp(log_decay)
        twice = 2.0 * log_decay
        small = jnp.maximum(twice, -0.5)
        series = 1.0 + small * (1.0 / 10.0)
        for n in (9, 8, 7, 6, 5, 4, 3, 2):
            series = 1.0 + small * (1.0 / n) * series
        less = jnp.where(twice > -0.5, small * series, jnp.exp(twice) - 1.0)
        norm = jnp.sqrt(-less)
        saved_ref[0, :, cols] = decay
        reset_ref[:, cols] = reset
        norm_ref[:, cols] = norm
        inp_ref[:, cols] = inp
        drive_ref[:, cols] = norm * inp * conv.astype(F32)


def run_forward(first_ref, saved_ref, drive_ref, prev_ref, state_ref):
    rows, width = drive_ref.shape

    def step(group, state):
        for i in range(8):
            t = pl.ds(group * 8 + i, 1)
            prev_ref[t, :] = state
            state = saved_ref[0, t, :] * state + drive_ref[t, :]
            state_ref[t, :] = state
        return state

    lax.fori_loop(0, rows // 8, step, first_ref[...])

    def back(group, prod):
        for i in range(8):
            t = rows - 1 - (group * 8 + i)
            saved_ref[1, pl.ds(t, 1), :] = prod
            prod = prod * saved_ref[0, pl.ds(t, 1), :]
        return prod

    lax.fori_loop(0, rows // 8, back, jnp.ones((1, width), F32))


def factors(
    conv_ref, gate_ref, slow_ref, saved_ref, merged_ref, prev_ref, state_ref, reset_ref, norm_ref, inp_ref
):
    hd = 128
    for h in range(conv_ref.shape[1] // hd):
        cols = slice(h * hd, (h + 1) * hd)
        conv = conv_ref[:, cols].astype(F32)
        decay, reset, norm, inp = saved_ref[0, :, cols], reset_ref[:, cols], norm_ref[:, cols], inp_ref[:, cols]
        by_log = decay * prev_ref[:, cols] - inp * conv * decay * decay / norm
        saved_ref[2, :, cols] = by_log * (-8.0 * slow_ref[:, cols]) * reset * (1.0 - reset)
        saved_ref[3, :, cols] = norm * conv * inp * (1.0 - inp)
        saved_ref[4, :, cols] = norm * inp
        state = state_ref[:, cols]
        value = gate_ref[:, cols].astype(F32)
        k = 0.7978845608028654
        square = value * value
        bent = jnp.tanh(k * (value + 0.044715 * value * square))
        act = 0.5 * value * (1.0 + bent)
        slope = 0.5 * (1.0 + bent) + 0.5 * value * (1.0 - bent * bent) * k * (1.0 + 3.0 * 0.044715 * square)
        saved_ref[5, :, cols] = state * slope
        saved_ref[6, :, cols] = act
        merged_ref[:, cols] = (act * state).astype(BF16)


def slot_tests(codes, experts):
    tokens = codes.shape[1]
    row = lax.broadcasted_iota(jnp.int32, (experts * 8, tokens), 0)
    base = (row // 8) * 16
    main = base + row % 8
    tail = base + 8 + row % 4
    return [[codes[k : k + 1, :] == want for k in (0, 1)] for want in (main, tail)], row % 8 < 4


def pack(ids_ref, wts_ref, d_out_ref, mixed_ref, send_ref, code_ref):
    experts = send_ref.shape[0]
    tokens, width = d_out_ref.shape
    half = width // 2
    each = lax.broadcasted_iota(jnp.int32, (experts, tokens), 0)
    named = [ids_ref[k : k + 1, :] == each for k in (0, 1)]
    both = jnp.where(named[0] | named[1], 1.0, 0.0).astype(BF16)
    earlier = (
        lax.broadcasted_iota(jnp.int32, (tokens, tokens), 0)
        < lax.broadcasted_iota(jnp.int32, (tokens, tokens), 1)
    )
    count = dot(both, jnp.where(earlier, 1.0, 0.0).astype(BF16))
    codes = []
    for k in (0, 1):
        rank = jnp.sum(jnp.where(named[k], count, 0.0), axis=0, keepdims=True)
        codes.append(ids_ref[k : k + 1, :] * 16 + rank.astype(jnp.int32))
        code_ref[k : k + 1, :] = codes[k]
    codes = jnp.concatenate(codes, axis=0)
    (main, tail), low = slot_tests(codes, experts)

    def weight(tests):
        return jnp.sum(
            jnp.where(tests[0], wts_ref[0:1, :], 0.0) + jnp.where(tests[1], wts_ref[1:2, :], 0.0),
            axis=1,
            keepdims=True,
        )

    main_pick = jnp.where(main[0] | main[1], 1.0, 0.0).astype(BF16)
    in_tail = tail[0] | tail[1]
    low_pick = jnp.where(in_tail & low, 1.0, 0.0).astype(BF16)
    high_pick = jnp.where(in_tail & ~low, 1.0, 0.0).astype(BF16)

    for at, (ref, w_main, w_tail) in enumerate(
        ((d_out_ref, weight(main), weight(tail)), (mixed_ref, None, None))
    ):
        first = dot(main_pick, ref[...])
        second = dot(low_pick, ref[:, :half]) + dot(high_pick, ref[:, half:])
        if w_main is not None:
            first, second = first * w_main, second * w_tail
        rows = slice(at * 8, at * 8 + 8)
        send_ref[:, rows, :width] = first.reshape(experts, 8, width).astype(BF16)
        send_ref[:, rows, width:] = second.reshape(experts, 8, half).astype(BF16)


def place():
    sp, tp = lax.axis_index("sp"), lax.axis_index("tp")
    return sp, tp, sp // 8, (sp // 2) % 4, sp % 2


Z_ORDER = (0, 1, 6, 2, 5, 4, 3, 7)


def z_offset(i):
    return sum(jnp.where(i == k, dz, 0) for k, dz in enumerate(Z_ORDER))


def offset_device(z, x, c, dz, j):
    return ((z + dz) % 8) * 8 + ((x + j // 2) % 4) * 2 + (c + j % 2) % 2


def greet(sp, tp, n_sp, n_tp):
    barrier = pltpu.get_barrier_semaphore()

    def to_sp(k, _):
        pl.semaphore_signal(barrier, inc=1, device_id=((sp + k) % n_sp, tp), device_id_type=MESH)
        return 0

    lax.fori_loop(1, n_sp, to_sp, 0)
    for k in range(1, n_tp):
        pl.semaphore_signal(barrier, inc=1, device_id=(sp, (tp + k) % n_tp), device_id_type=MESH)


def all_here(n_sp, n_tp):
    pl.semaphore_wait(pltpu.get_barrier_semaphore(), n_sp - 1 + n_tp - 1)


def remote(src, dst, send_sem, recv_sem, sp, tp):
    return pltpu.make_async_remote_copy(
        src_ref=src, dst_ref=dst, send_sem=send_sem, recv_sem=recv_sem,
        device_id=(sp, tp), device_id_type=MESH,
    )


def wait_bytes(ref, sem):
    pltpu.make_async_copy(ref, ref, sem).wait()


def unpack(got_ref, q, at, row, rows_ref, cot_ref):
    packed = got_ref.shape[3]
    width, half = packed * 2 // 3, packed // 3
    cols = slice(q * width, (q + 1) * width)
    for first, ref in ((0, cot_ref), (8, rows_ref)):
        block = got_ref[q, pl.ds(at, 8), first : first + 8, :].astype(F32)
        ref[pl.ds(row, 64), cols] = block[:, :, :width].reshape(64, width).astype(BF16)
        tails = block[:, :, width:]
        turned = swap4(tails)
        tails, turned = tails.reshape(4, 2, 8, half), turned.reshape(4, 2, 8, half)
        low = low_half((4, 8, half))
        left = jnp.where(low, tails[:, 0], turned[:, 1])
        right = jnp.where(low, turned[:, 0], tails[:, 1])
        both = jnp.concatenate([left, right], axis=2).reshape(32, width)
        ref[pl.ds(row + 64, 32), cols] = both.astype(BF16)


def expert_terms(row, rows_ref, cot_ref, grad_ref, hidden_ref, wboth_ref, wd_ref):
    fe = wd_ref.shape[0]
    rows = pl.ds(row, 96)
    both = dot(rows_ref[rows, :], wboth_ref[...])
    up_pre, linear = both[:, :fe], both[:, fe:]
    d_hidden = dot(cot_ref[rows, :], wd_ref[...], ((1,), (1,)))
    gate = jax.nn.sigmoid(up_pre)
    silu = up_pre * gate
    hidden_ref[rows, :] = (silu * linear).astype(BF16)
    d_linear = (d_hidden * silu).astype(BF16)
    d_up = (d_hidden * linear * gate * (1.0 + up_pre * (1.0 - gate))).astype(BF16)
    grad_ref[rows, :fe] = d_up
    grad_ref[rows, fe:] = d_linear


def row_part(q, at, row, grad_ref, wboth_ref, part_ref):
    packed = part_ref.shape[3]
    width, half = packed * 2 // 3, packed // 3
    part = dot(grad_ref[pl.ds(row, 96), :], wboth_ref[pl.ds(pl.multiple_of(q * width, width), width), :], ((1,), (1,)))
    part_ref[q, pl.ds(at, 8), :, :width] = part[:64].reshape(8, 8, width).astype(BF16)
    tails = part[64:].reshape(4, 8, width)
    left, right = tails[:, :, :half], tails[:, :, half:]
    low = low_half((4, 8, half))
    one = jnp.where(low, left, swap4(right))
    two = jnp.where(low, swap4(left), right)
    part_ref[q, pl.ds(at, 8), :, width:] = jnp.stack([one, two], axis=1).reshape(8, 8, half).astype(BF16)


STAGES = (0, 2, 3, 4, 5)
GROUPS = 8


def step_kernel(
    conv_ref, gate_in_ref, first_ref, param_ref, shift_ref, wr_ref, wi_ref, wo_hbm, mixed_ref, d_out_ref,
    ids_ref, wts_ref, wg_hbm, wu_hbm, wd_hbm,
    both_hbm, down_hbm, proj_ref, rec_ref, gate_ref,
    send_ref, code_ref, got_ref, rows_ref, cot_ref, grad_ref, hidden_ref, part_ref, far_ref, comb_ref,
    near_ref, back_ref, ret_ref, saved_ref, merged_ref, temp_ref, slow_ref, wboth_ref, wd_ref, wo_ref, both_ref,
    down_ref, mix_ref, acc_ref, local_ref, keep_ref, pair_ref, pair_got, x_ref, x_far_ref, x_comb_ref, x_near_ref, z_ref, z_got,
    own_ref, lead_ref, lead_got,
    load_sem, store_sem, send_sem, near_x_recv, recv_sem, y_send, y_recv, f_send, f_recv, far_send, far_recv,
    near_send, near_recv, ret_send, ret_recv, mix_send, mix_recv, pair_send, pair_recv,
    x_send, x_recv, z_send, z_recv, lead_send, lead_recv,
):
    sp, tp, z, x, c = place()
    n_tp, n_sp = part_ref.shape[0], part_ref.shape[1]
    tokens, width = d_out_ref.shape
    half = width // 2
    fe = wd_ref.shape[0]
    right, left, far = (tp + 1) % n_tp, (tp + n_tp - 1) % n_tp, (tp + 2) % n_tp
    drive_ref, prev_ref, state_ref, reset_ref, norm_ref, inp_ref = [temp_ref.at[k] for k in range(6)]

    greet(sp, tp, n_sp, n_tp)
    loads = [
        pltpu.make_async_copy(src, dst, load_sem.at[k])
        for k, (src, dst) in enumerate((
            (wg_hbm, wboth_ref.at[:, pl.ds(0, fe)]), (wu_hbm, wboth_ref.at[:, pl.ds(fe, fe)]),
            (wd_hbm, wd_ref), (wo_hbm, wo_ref),
        ))
    ]
    for load in loads:
        load.start()
    pack(ids_ref, wts_ref, d_out_ref, mixed_ref, send_ref, code_ref)
    got_ref[tp, sp] = send_ref[sp]
    gates(
        conv_ref, param_ref, slow_ref, shift_ref, wr_ref, wi_ref, saved_ref, drive_ref, reset_ref, norm_ref, inp_ref
    )
    run_forward(first_ref, saved_ref, drive_ref, prev_ref, state_ref)
    factors(
        conv_ref, gate_in_ref, slow_ref, saved_ref, merged_ref, prev_ref, state_ref, reset_ref, norm_ref, inp_ref
    )
    all_here(n_sp, n_tp)

    for dx in (0, 1, 3, 2):
        for dc in (0, 1):
            if dx or dc:
                to = z * 8 + ((x + dx) % 4) * 2 + (c + dc) % 2
                remote(send_ref.at[to], got_ref.at[tp, sp], send_sem, near_x_recv.at[dx], to, tp).start()

    def gather_block(i, at, count):
        block = got_ref.at[tp, pl.ds(at, count)]
        remote(block, block, y_send.at[0], y_recv.at[0, i], sp, right).start()
        remote(block, block, y_send.at[1], y_recv.at[1, i], sp, left).start()

    for dx in (0, 1, 3, 2):
        at = z * 8 + ((x + 4 - dx) % 4) * 2
        wait_bytes(got_ref.at[tp, pl.ds(at, 2 if dx else 1)], near_x_recv.at[dx])
        gather_block(0, at, 2)
        if dx == 0:

            def send_group(i, _):
                def send(j, _):
                    to = offset_device(z, x, c, z_offset(i), j)
                    remote(send_ref.at[to], got_ref.at[tp, sp], send_sem, recv_sem.at[i], to, tp).start()
                    return 0

                lax.fori_loop(0, 8, send, 0)
                return 0

            lax.fori_loop(1, GROUPS, send_group, 0)

    def source_group(i):
        return (z + 8 - z_offset(i)) % 8

    def gather(i):
        @pl.when(i > 0)
        def _():
            at = source_group(i) * 8
            wait_bytes(got_ref.at[tp, pl.ds(at, 8)], recv_sem.at[i])
            gather_block(i, at, 8)

    def relay(i):
        at = source_group(i) * 8
        wait_bytes(got_ref.at[left, pl.ds(at, 8)], y_recv.at[0, i])
        block = got_ref.at[left, pl.ds(at, 4)]
        remote(block, block, f_send.at[0], f_recv.at[0, i], sp, right).start()
        wait_bytes(got_ref.at[right, pl.ds(at, 8)], y_recv.at[1, i])
        block = got_ref.at[right, pl.ds(at + 4, 4)]
        remote(block, block, f_send.at[1], f_recv.at[1, i], sp, left).start()

    def compute(i):
        group = source_group(i)
        at, row = group * 8, pl.multiple_of(group * 96, 32)
        wait_bytes(got_ref.at[far, pl.ds(at, 4)], f_recv.at[0, i])
        wait_bytes(got_ref.at[far, pl.ds(at + 4, 4)], f_recv.at[1, i])
        for q in range(n_tp):
            unpack(got_ref, q, at, row, rows_ref, cot_ref)
        expert_terms(row, rows_ref, cot_ref, grad_ref, hidden_ref, wboth_ref, wd_ref)
        lower, upper = pl.ds(at, 4), pl.ds(at + 4, 4)
        row_part(far, at, row, grad_ref, wboth_ref, part_ref)
        remote(part_ref.at[far, lower], far_ref.at[0, i], far_send.at[0], far_recv.at[0, i], sp, left).start()
        remote(part_ref.at[far, upper], far_ref.at[1, i], far_send.at[1], far_recv.at[1, i], sp, right).start()
        row_part(left, at, row, grad_ref, wboth_ref, part_ref)
        remote(
            part_ref.at[left, upper], near_ref.at[0, i, pl.ds(4, 4)], near_send.at[0], near_recv.at[0, i], sp, left
        ).start()
        row_part(right, at, row, grad_ref, wboth_ref, part_ref)
        remote(
            part_ref.at[right, lower], near_ref.at[1, i, pl.ds(0, 4)], near_send.at[1], near_recv.at[1, i], sp, right
        ).start()
        row_part(tp, at, row, grad_ref, wboth_ref, part_ref)

    def add_far(i):
        at = source_group(i) * 8
        for side, (to, first) in enumerate(((left, 0), (right, 4))):
            wait_bytes(far_ref.at[side, i], far_recv.at[side, i])
            own = part_ref[to, pl.ds(at + first, 4)].astype(F32)
            comb_ref[side, i] = (own + far_ref[side, i].astype(F32)).astype(BF16)
            remote(
                comb_ref.at[side, i], near_ref.at[side, i, pl.ds(first, 4)],
                near_send.at[side], near_recv.at[side, i], sp, to,
            ).start()

    def give_back(i):
        group = source_group(i)
        at = group * 8
        wait_bytes(near_ref.at[0, i], near_recv.at[0, i])
        wait_bytes(near_ref.at[1, i], near_recv.at[1, i])
        total = part_ref[tp, pl.ds(at, 8)].astype(F32) + near_ref[0, i].astype(F32) + near_ref[1, i].astype(F32)
        back_ref[pl.ds(at, 8)] = total.astype(BF16)

        def send(j, _):
            to = group * 8 + ((x + j // 2) % 4) * 2 + (c + j % 2) % 2
            remote(back_ref.at[to], ret_ref.at[sp], ret_send, ret_recv, to, tp).start()
            return 0

        lax.fori_loop(jnp.where(i == 0, 1, 0), 8, send, 0)

    def step(s, _):
        for lag, stage in zip(STAGES, (gather, relay, compute, add_far, give_back)):
            if stage is compute:

                @pl.when(s == lag)
                def _():
                    for load in loads[:3]:
                        load.wait()

            @pl.when(jnp.logical_and(s >= lag, s < lag + GROUPS))
            def _():
                stage(s - lag)

        return 0

    lax.fori_loop(0, GROUPS + STAGES[-1], step, 0)

    over_rows = ((0,), (0,))

    def weight_grads(k, _):
        cols = pl.ds(pl.multiple_of(k * 512, 512), 512)
        both_ref[cols, :] = dot(rows_ref[:, cols], grad_ref[...], over_rows).astype(BF16)
        down_ref[:, cols] = dot(hidden_ref[...], cot_ref[:, cols], over_rows).astype(BF16)
        return 0

    lax.fori_loop(0, rows_ref.shape[1] // 512, weight_grads, 0)
    stores = [
        pltpu.make_async_copy(both_ref, both_hbm, store_sem.at[0]),
        pltpu.make_async_copy(down_ref, down_hbm, store_sem.at[1]),
    ]
    for store in stores:
        store.start()

    (main, tail), low = slot_tests(code_ref[...], n_sp)
    main_pick = jnp.where(main[0] | main[1], 1.0, 0.0).astype(BF16)
    in_tail = tail[0] | tail[1]
    low_pick = jnp.where(in_tail & low, 1.0, 0.0).astype(BF16)
    high_pick = jnp.where(in_tail & ~low, 1.0, 0.0).astype(BF16)
    ret_ref[sp] = back_ref[sp]
    wait_bytes(ret_ref.at[pl.ds(0, n_sp - 1)], ret_recv)
    main_rows = ret_ref[:, :, :width].astype(F32).reshape(n_sp * 8, width).astype(BF16)
    tail_rows = ret_ref[:, :, width:].astype(F32).reshape(n_sp * 8, half).astype(BF16)
    summed = dot(main_pick, main_rows, over_rows) + jnp.concatenate(
        [dot(low_pick, tail_rows, over_rows), dot(high_pick, tail_rows, over_rows)], axis=1
    )
    mix_ref[tp] = (d_out_ref[...].astype(F32) + summed).astype(BF16)
    for side, to in enumerate((right, left)):
        remote(mix_ref.at[tp], mix_ref.at[tp], mix_send.at[side], mix_recv.at[side], sp, to).start()
    loads[3].wait()

    blocks = (tp, left, right, far)
    x_right, x_left, x_far = (x + 1) % 4, (x + 3) % 4, (x + 2) % 4
    part_rows = half // 8
    cut = part_rows // 2

    def along(x_to, z_to=z):
        return z_to * 8 + x_to * 2 + c

    def products(n):
        q = blocks[n]
        whole = mix_ref[q]
        block = dot(whole, wo_ref[:, pl.ds(pl.multiple_of(q * width, width), width)], ((1,), (1,)))
        if n == 0:
            acc_ref[...] = block
        else:
            acc_ref[...] += block
        for h in (0, 1):
            slot = 2 * n + h
            grad = dot(whole[:, h * half : (h + 1) * half], merged_ref[...], over_rows)
            grad = grad.reshape(4, 2, part_rows, width)
            keep_ref[slot] = jnp.where(c == 0, grad[:, 0], grad[:, 1])
            pair_ref[slot] = jnp.where(c == 0, grad[:, 1], grad[:, 0]).astype(BF16)
            remote(
                pair_ref.at[slot], pair_got.at[slot], pair_send, pair_recv.at[slot], sp + 1 - 2 * c, tp
            ).start()

    def x_start(n):
        for slot in (2 * n, 2 * n + 1):
            wait_bytes(pair_got.at[slot], pair_recv.at[slot])
            total = keep_ref[slot] + pair_got[slot].astype(F32)
            keep_ref[slot] = total
            x_ref[slot] = total.astype(BF16)
            lower, upper = pl.ds(0, cut), pl.ds(cut, cut)
            for block, rows, ref, side, at, to in (
                (x_far, lower, x_far_ref, 0, None, x_left),
                (x_far, upper, x_far_ref, 1, None, x_right),
                (x_left, upper, x_near_ref, 0, upper, x_left),
                (x_right, lower, x_near_ref, 1, lower, x_right),
            ):
                goal = ref.at[slot, side] if at is None else ref.at[slot, side, at]
                send, recv = (x_send.at[0], x_recv.at[0, slot, side]) if at is None else (x_send.at[1], x_recv.at[1, slot, side])
                remote(x_ref.at[slot, block, rows], goal, send, recv, along(to), tp).start()

    def x_relay(n):
        for slot in (2 * n, 2 * n + 1):
            for side, to, first in ((0, x_left, 0), (1, x_right, cut)):
                wait_bytes(x_far_ref.at[slot, side], x_recv.at[0, slot, side])
                own = keep_ref[slot, to, first : first + cut]
                x_comb_ref[slot, side] = (own + x_far_ref[slot, side].astype(F32)).astype(BF16)
                remote(
                    x_comb_ref.at[slot, side], x_near_ref.at[slot, side, pl.ds(first, cut)],
                    x_send.at[1], x_recv.at[1, slot, side], along(to), tp,
                ).start()

    def z_start(n):
        for h in (0, 1):
            slot = 2 * n + h
            total = keep_ref[slot, x]
            for side in (0, 1):
                wait_bytes(x_near_ref.at[slot, side], x_recv.at[1, slot, side])
                total = total + x_near_ref[slot, side].astype(F32)
            z_ref[slot] = total.astype(BF16)
            to = 2 * blocks[n] + h

            @pl.when(to == z)
            def _():
                own_ref[...] = total

            @pl.when(to != z)
            def _():
                remote(z_ref.at[slot], z_got.at[z], z_send, z_recv, along(x, to), tp).start()

    upper_half = tokens // 2
    products(0)
    wait_bytes(mix_ref.at[left], mix_recv.at[0])
    piece = mix_ref.at[left, pl.ds(0, upper_half)]
    remote(piece, piece, mix_send.at[2], mix_recv.at[2], sp, right).start()
    wait_bytes(mix_ref.at[right], mix_recv.at[1])
    piece = mix_ref.at[right, pl.ds(upper_half, upper_half)]
    remote(piece, piece, mix_send.at[3], mix_recv.at[3], sp, left).start()
    x_start(0)
    products(1)
    products(2)
    x_start(1)
    x_relay(0)
    x_start(2)
    wait_bytes(mix_ref.at[far, pl.ds(0, upper_half)], mix_recv.at[2])
    wait_bytes(mix_ref.at[far, pl.ds(upper_half, upper_half)], mix_recv.at[3])
    products(3)

    d_merged = acc_ref[...]
    gate_ref[...] = (d_merged * saved_ref[5]).astype(BF16)
    acc_ref[...] = d_merged * saved_ref[6]

    def back(group, carry):
        for i in range(8):
            t = pl.ds(tokens - 1 - (group * 8 + i), 1)
            grad = acc_ref[t, :] + carry
            local_ref[t, :] = grad
            carry = grad * saved_ref[0, t, :]
        return carry

    lead = lax.fori_loop(0, tokens // 8, back, jnp.zeros((1, width), F32))
    lead_ref[0, 0:1, :] = saved_ref[1, 0:1, :] * saved_ref[0, 0:1, :]
    lead_ref[0, 1:2, :] = lead
    lead_got[sp] = lead_ref[0]
    x_start(3)

    def tell(k, _):
        remote(lead_ref.at[0], lead_got.at[sp], lead_send, lead_recv, (sp + k) % n_sp, tp).start()
        return 0

    lax.fori_loop(1, n_sp, tell, 0)
    x_relay(1)
    x_relay(2)
    z_start(0)
    x_relay(3)
    for n in (1, 2, 3):
        z_start(n)

    wait_bytes(lead_got.at[pl.ds(0, n_sp - 1)], lead_recv)

    def later(k, carry):
        i = n_sp - 1 - k
        pair = lead_got[i]
        return jnp.where(i > sp, pair[1:2, :] + pair[0:1, :] * carry, carry)

    incoming = lax.fori_loop(0, n_sp, later, jnp.zeros((1, width), F32))
    heads, hd = wr_ref.shape[0], wr_ref.shape[1]
    for h in range(heads):
        cols = slice(h * hd, (h + 1) * hd)
        grad = local_ref[:, cols] + saved_ref[1, :, cols] * incoming[:, cols]
        by_reset = (grad * saved_ref[2, :, cols]).astype(BF16)
        by_input = (grad * saved_ref[3, :, cols]).astype(BF16)
        rec_ref[:, cols] = (
            grad * saved_ref[4, :, cols]
            + dot(by_reset, wr_ref[h], ((1,), (1,)))
            + dot(by_input, wi_ref[h], ((1,), (1,)))
        ).astype(BF16)

    wait_bytes(z_got.at[pl.ds(0, 7)], z_recv)
    total = own_ref[...]
    for d in range(1, 8):
        total = total + z_got[(z + d) % 8].astype(F32)
    proj_ref[...] = total

    wait_bytes(send_ref.at[pl.ds(0, n_sp - 1)], send_sem)
    for side in (0, 1):
        wait_bytes(got_ref.at[tp], y_send.at[side])
        wait_bytes(got_ref.at[tp, pl.ds(0, n_sp // 2)], f_send.at[side])
        wait_bytes(part_ref.at[tp, pl.ds(0, n_sp // 2)], far_send.at[side])
        wait_bytes(part_ref.at[tp], near_send.at[side])
        wait_bytes(mix_ref.at[tp], mix_send.at[side])
        wait_bytes(mix_ref.at[tp, pl.ds(0, upper_half)], mix_send.at[2 + side])
    wait_bytes(back_ref.at[pl.ds(0, n_sp - 1)], ret_send)
    wait_bytes(pair_ref, pair_send)
    wait_bytes(x_far_ref, x_send.at[0])
    wait_bytes(x_near_ref, x_send.at[1])
    wait_bytes(z_ref.at[pl.ds(0, 7)], z_send)
    wait_bytes(lead_got.at[pl.ds(0, n_sp - 1)], lead_send)
    for store in stores:
        store.wait()


def whole_step(n_sp, n_tp, *args):
    conv, w_gate = args[0], args[12]
    tokens, width = conv.shape
    model, fe = w_gate.shape
    packed = width + width // 2
    rows = n_sp * 12
    block = (model // n_sp, width)
    dma = pltpu.SemaphoreType.DMA
    specs = [VM] * 15
    for k in (7, 12, 13, 14):
        specs[k] = ANY
    return pl.pallas_call(
        step_kernel,
        out_shape=(
            jax.ShapeDtypeStruct((model, 2 * fe), BF16),
            jax.ShapeDtypeStruct((fe, model), BF16),
            jax.ShapeDtypeStruct(block, F32),
            jax.ShapeDtypeStruct((tokens, width), BF16),
            jax.ShapeDtypeStruct((tokens, width), BF16),
        ),
        in_specs=specs,
        out_specs=(ANY, ANY, VM, VM, VM),
        scratch_shapes=[
            pltpu.VMEM((n_sp, 16, packed), BF16),
            pltpu.VMEM((2, tokens), jnp.int32),
            pltpu.VMEM((n_tp, n_sp, 16, packed), BF16),
            pltpu.VMEM((rows, model), BF16),
            pltpu.VMEM((rows, model), BF16),
            pltpu.VMEM((rows, 2 * fe), BF16),
            pltpu.VMEM((rows, fe), BF16),
            pltpu.VMEM((n_tp, n_sp, 8, packed), BF16),
            pltpu.VMEM((2, GROUPS, 4, 8, packed), BF16),
            pltpu.VMEM((2, GROUPS, 4, 8, packed), BF16),
            pltpu.VMEM((2, GROUPS, 8, 8, packed), BF16),
            pltpu.VMEM((n_sp, 8, packed), BF16),
            pltpu.VMEM((n_sp, 8, packed), BF16),
            pltpu.VMEM((7, tokens, width), F32),
            pltpu.VMEM((tokens, width), BF16),
            pltpu.VMEM((6, tokens, width), F32),
            pltpu.VMEM((1, width), F32),
            pltpu.VMEM((model, 2 * fe), BF16),
            pltpu.VMEM((fe, model), BF16),
            pltpu.VMEM((width, model), BF16),
            pltpu.VMEM((model, 2 * fe), BF16),
            pltpu.VMEM((fe, model), BF16),
            pltpu.VMEM((n_tp, tokens, width), BF16),
            pltpu.VMEM((tokens, width), F32),
            pltpu.VMEM((tokens, width), F32),
            pltpu.VMEM((8, 4, *block), F32),
            pltpu.VMEM((8, 4, *block), BF16),
            pltpu.VMEM((8, 4, *block), BF16),
            pltpu.VMEM((8, 4, *block), BF16),
            pltpu.VMEM((8, 2, block[0] // 2, width), BF16),
            pltpu.VMEM((8, 2, block[0] // 2, width), BF16),
            pltpu.VMEM((8, 2, *block), BF16),
            pltpu.VMEM((8, *block), BF16),
            pltpu.VMEM((8, *block), BF16),
            pltpu.VMEM(block, F32),
            pltpu.VMEM((1, 2, width), F32),
            pltpu.VMEM((n_sp, 2, width), F32),
            dma((4,)), dma((2,)), dma, dma((4,)), dma((8,)), dma((2,)), dma((2, 8)), dma((2,)), dma((2, 8)),
            dma((2,)), dma((2, 8)), dma((2,)), dma((2, 8)), dma, dma, dma((4,)), dma((4,)),
            dma, dma((8,)), dma((2,)), dma((2, 8, 2)), dma, dma, dma, dma,
        ],
        compiler_params=pltpu.CompilerParams(
            collective_id=0, has_side_effects=True, vmem_limit_bytes=63 * 2**20
        ),
        name="whole_step",
    )(*args)


def write_kernel(both_ref, down_ref, proj_ref, rec_ref, gate_ref, gg_ref, gu_ref, gd_ref, p_ref, r_ref, g_ref):
    fe = gg_ref.shape[1]
    gg_ref[...] = both_ref[:, :fe].astype(F32)
    gu_ref[...] = both_ref[:, fe:].astype(F32)
    gd_ref[...] = down_ref[...].astype(F32)
    p_ref[...] = proj_ref[...]
    r_ref[...] = rec_ref[...]
    g_ref[...] = gate_ref[...]


def write_out(both, down, proj, rec, gate, parts=4):
    model, fe = both.shape[0], both.shape[1] // 2

    def cut(array):
        return pl.BlockSpec((array.shape[0] // parts, array.shape[1]), lambda i: (i, 0))

    outs = (
        jax.ShapeDtypeStruct((model, fe), F32),
        jax.ShapeDtypeStruct((model, fe), F32),
        jax.ShapeDtypeStruct((fe, model), F32),
        jax.ShapeDtypeStruct(proj.shape, proj.dtype),
        jax.ShapeDtypeStruct(rec.shape, rec.dtype),
        jax.ShapeDtypeStruct(gate.shape, gate.dtype),
    )
    ins = (both, down, proj, rec, gate)
    return pl.pallas_call(
        write_kernel,
        grid=(parts,),
        out_shape=outs,
        in_specs=[cut(a) for a in ins],
        out_specs=tuple(cut(a) for a in outs),
        name="write_out",
    )(*ins)


def body(
    n_sp, n_tp, conv_out, gate_in, block_states, decay_param, decay_shift, w_reset, w_input, w_out,
    mixed, d_out, expert_ids, route_weights, w_gate, w_up, w_down,
):
    both, down, proj, rec, gate = whole_step(
        n_sp, n_tp, conv_out, gate_in, block_states, decay_param[None, :], decay_shift[None, :], w_reset, w_input, w_out,
        mixed, d_out, expert_ids.T, route_weights.T, w_gate[0], w_up[0], w_down[0],
    )
    gg, gu, gd, proj, rec, gate = write_out(both, down, proj, rec, gate)
    return gg[None], gu[None], gd[None], proj, rec, gate


def solution(mesh):
    in_specs = (
        P("sp", "tp"), P("sp", "tp"), P("sp", "tp"), P("tp"), P("sp"),
        P("tp", None, None), P("tp", None, None), P("tp", None),
        P("sp", "tp"), P("sp", "tp"), P("sp", None), P("sp", None),
        P("sp", None, "tp"), P("sp", None, "tp"), P("sp", "tp", None),
    )
    out_specs = (
        P("sp", None, "tp"), P("sp", None, "tp"), P("sp", "tp", None),
        P("sp", "tp"), P("sp", "tp"), P("sp", "tp"),
    )
    run = functools.partial(body, mesh.shape["sp"], mesh.shape["tp"])
    return jax.shard_map(run, mesh=mesh, in_specs=in_specs, out_specs=out_specs, check_vma=False)
```

```python
import functools

import jax
import jax.numpy as jnp
from jax import lax
from jax.experimental import pallas as pl
from jax.experimental.pallas import tpu as pltpu
from jax.sharding import PartitionSpec as P

F32 = jnp.float32
BF16 = jnp.bfloat16
MESH = pl.DeviceIdType.MESH
VM = pl.BlockSpec(memory_space=pltpu.VMEM)
ANY = pl.BlockSpec(memory_space=pl.ANY)


def dot(a, b, dims=((1,), (0,))):
    return lax.dot_general(a, b, (dims, ((), ())), preferred_element_type=F32)


def swap4(value):
    return pltpu.roll(value, 4, axis=1)


def low_half(shape):
    return lax.broadcasted_iota(jnp.int32, shape, 1) < 4


def gates(conv_ref, param_ref, slow_ref, shift_ref, wr_ref, wi_ref, saved_ref, drive_ref, reset_ref, norm_ref, inp_ref):
    hd = wr_ref.shape[1]
    rows = conv_ref.shape[0]
    shift = jnp.transpose(jnp.broadcast_to(shift_ref[...], (8, rows)))[:, 0:1]
    param = param_ref[...]
    slow_ref[...] = jnp.maximum(-param, 0.0) + jnp.log1p(jnp.exp(-jnp.abs(param)))
    for h in range(wr_ref.shape[0]):
        cols = slice(h * hd, (h + 1) * hd)
        conv = conv_ref[:, cols]
        reset = jax.nn.sigmoid(dot(conv, wr_ref[h]))
        inp = jax.nn.sigmoid(dot(conv, wi_ref[h]))
        log_decay = -8.0 * reset * slow_ref[:, cols] + shift
        decay = jnp.exp(log_decay)
        twice = 2.0 * log_decay
        small = jnp.maximum(twice, -0.5)
        series = 1.0 + small * (1.0 / 10.0)
        for n in (9, 8, 7, 6, 5, 4, 3, 2):
            series = 1.0 + small * (1.0 / n) * series
        less = jnp.where(twice > -0.5, small * series, jnp.exp(twice) - 1.0)
        norm = jnp.sqrt(-less)
        saved_ref[0, :, cols] = decay
        reset_ref[:, cols] = reset
        norm_ref[:, cols] = norm
        inp_ref[:, cols] = inp
        drive_ref[:, cols] = norm * inp * conv.astype(F32)


def run_forward(first_ref, saved_ref, drive_ref, prev_ref, state_ref):
    rows, width = drive_ref.shape

    def step(group, state):
        for i in range(8):
            t = pl.ds(group * 8 + i, 1)
            prev_ref[t, :] = state
            state = saved_ref[0, t, :] * state + drive_ref[t, :]
            state_ref[t, :] = state
        return state

    lax.fori_loop(0, rows // 8, step, first_ref[...])

    def back(group, prod):
        for i in range(8):
            t = rows - 1 - (group * 8 + i)
            saved_ref[1, pl.ds(t, 1), :] = prod
            prod = prod * saved_ref[0, pl.ds(t, 1), :]
        return prod

    lax.fori_loop(0, rows // 8, back, jnp.ones((1, width), F32))


def factors(
    conv_ref, gate_ref, slow_ref, saved_ref, merged_ref, prev_ref, state_ref, reset_ref, norm_ref, inp_ref
):
    hd = 128
    for h in range(conv_ref.shape[1] // hd):
        cols = slice(h * hd, (h + 1) * hd)
        conv = conv_ref[:, cols].astype(F32)
        decay, reset, norm, inp = saved_ref[0, :, cols], reset_ref[:, cols], norm_ref[:, cols], inp_ref[:, cols]
        by_log = decay * prev_ref[:, cols] - inp * conv * decay * decay / norm
        saved_ref[2, :, cols] = by_log * (-8.0 * slow_ref[:, cols]) * reset * (1.0 - reset)
        saved_ref[3, :, cols] = norm * conv * inp * (1.0 - inp)
        saved_ref[4, :, cols] = norm * inp
        state = state_ref[:, cols]
        value = gate_ref[:, cols].astype(F32)
        k = 0.7978845608028654
        square = value * value
        bent = jnp.tanh(k * (value + 0.044715 * value * square))
        act = 0.5 * value * (1.0 + bent)
        slope = 0.5 * (1.0 + bent) + 0.5 * value * (1.0 - bent * bent) * k * (1.0 + 3.0 * 0.044715 * square)
        saved_ref[5, :, cols] = state * slope
        saved_ref[6, :, cols] = act
        merged_ref[:, cols] = (act * state).astype(BF16)


def slot_tests(codes, experts):
    tokens = codes.shape[1]
    row = lax.broadcasted_iota(jnp.int32, (experts * 8, tokens), 0)
    base = (row // 8) * 16
    main = base + row % 8
    tail = base + 8 + row % 4
    return [[codes[k : k + 1, :] == want for k in (0, 1)] for want in (main, tail)], row % 8 < 4


def pack(ids_ref, wts_ref, d_out_ref, mixed_ref, send_ref, code_ref):
    experts = send_ref.shape[0]
    tokens, width = d_out_ref.shape
    half = width // 2
    each = lax.broadcasted_iota(jnp.int32, (experts, tokens), 0)
    named = [ids_ref[k : k + 1, :] == each for k in (0, 1)]
    both = jnp.where(named[0] | named[1], 1.0, 0.0).astype(BF16)
    earlier = (
        lax.broadcasted_iota(jnp.int32, (tokens, tokens), 0)
        < lax.broadcasted_iota(jnp.int32, (tokens, tokens), 1)
    )
    count = dot(both, jnp.where(earlier, 1.0, 0.0).astype(BF16))
    codes = []
    for k in (0, 1):
        rank = jnp.sum(jnp.where(named[k], count, 0.0), axis=0, keepdims=True)
        codes.append(ids_ref[k : k + 1, :] * 16 + rank.astype(jnp.int32))
        code_ref[k : k + 1, :] = codes[k]
    codes = jnp.concatenate(codes, axis=0)
    (main, tail), low = slot_tests(codes, experts)

    def weight(tests):
        return jnp.sum(
            jnp.where(tests[0], wts_ref[0:1, :], 0.0) + jnp.where(tests[1], wts_ref[1:2, :], 0.0),
            axis=1,
            keepdims=True,
        )

    main_pick = jnp.where(main[0] | main[1], 1.0, 0.0).astype(BF16)
    in_tail = tail[0] | tail[1]
    low_pick = jnp.where(in_tail & low, 1.0, 0.0).astype(BF16)
    high_pick = jnp.where(in_tail & ~low, 1.0, 0.0).astype(BF16)

    for at, (ref, w_main, w_tail) in enumerate(
        ((d_out_ref, weight(main), weight(tail)), (mixed_ref, None, None))
    ):
        first = dot(main_pick, ref[...])
        second = dot(low_pick, ref[:, :half]) + dot(high_pick, ref[:, half:])
        if w_main is not None:
            first, second = first * w_main, second * w_tail
        rows = slice(at * 8, at * 8 + 8)
        send_ref[:, rows, :width] = first.reshape(experts, 8, width).astype(BF16)
        send_ref[:, rows, width:] = second.reshape(experts, 8, half).astype(BF16)


def place():
    sp, tp = lax.axis_index("sp"), lax.axis_index("tp")
    return sp, tp, sp // 8, (sp // 2) % 4, sp % 2


Z_ORDER = (0, 1, 6, 2, 5, 4, 3, 7)


def z_offset(i):
    return sum(jnp.where(i == k, dz, 0) for k, dz in enumerate(Z_ORDER))


def offset_device(z, x, c, dz, j):
    return ((z + dz) % 8) * 8 + ((x + j // 2) % 4) * 2 + (c + j % 2) % 2


def greet(sp, tp, n_sp, n_tp):
    barrier = pltpu.get_barrier_semaphore()

    def to_sp(k, _):
        to = (sp + n_sp // 2 + k) % n_sp
        pl.semaphore_signal(barrier, inc=1, device_id=(to, tp), device_id_type=MESH)
        return 0

    lax.fori_loop(0, n_sp // 2, to_sp, 0)
    lax.fori_loop(1 - n_sp // 2, 0, to_sp, 0)
    for k in range(1, n_tp):
        pl.semaphore_signal(barrier, inc=1, device_id=(sp, (tp + k) % n_tp), device_id_type=MESH)


def all_here(n_sp, n_tp):
    pl.semaphore_wait(pltpu.get_barrier_semaphore(), n_sp - 1 + n_tp - 1)


def remote(src, dst, send_sem, recv_sem, sp, tp):
    return pltpu.make_async_remote_copy(
        src_ref=src, dst_ref=dst, send_sem=send_sem, recv_sem=recv_sem,
        device_id=(sp, tp), device_id_type=MESH,
    )


def wait_bytes(ref, sem):
    pltpu.make_async_copy(ref, ref, sem).wait()


def unpack(got_ref, q, at, row, rows_ref, cot_ref):
    packed = got_ref.shape[3]
    width, half = packed * 2 // 3, packed // 3
    cols = slice(q * width, (q + 1) * width)
    for first, ref in ((0, cot_ref), (8, rows_ref)):
        block = got_ref[q, pl.ds(at, 8), first : first + 8, :].astype(F32)
        ref[pl.ds(row, 64), cols] = block[:, :, :width].reshape(64, width).astype(BF16)
        tails = block[:, :, width:]
        turned = swap4(tails)
        tails, turned = tails.reshape(4, 2, 8, half), turned.reshape(4, 2, 8, half)
        low = low_half((4, 8, half))
        left = jnp.where(low, tails[:, 0], turned[:, 1])
        right = jnp.where(low, turned[:, 0], tails[:, 1])
        both = jnp.concatenate([left, right], axis=2).reshape(32, width)
        ref[pl.ds(row + 64, 32), cols] = both.astype(BF16)


def expert_terms(row, rows_ref, cot_ref, grad_ref, hidden_ref, wboth_ref, wd_ref):
    fe = wd_ref.shape[0]
    rows = pl.ds(row, 96)
    both = dot(rows_ref[rows, :], wboth_ref[...])
    up_pre, linear = both[:, :fe], both[:, fe:]
    d_hidden = dot(cot_ref[rows, :], wd_ref[...], ((1,), (1,)))
    gate = jax.nn.sigmoid(up_pre)
    silu = up_pre * gate
    hidden_ref[rows, :] = (silu * linear).astype(BF16)
    d_linear = (d_hidden * silu).astype(BF16)
    d_up = (d_hidden * linear * gate * (1.0 + up_pre * (1.0 - gate))).astype(BF16)
    grad_ref[rows, :fe] = d_up
    grad_ref[rows, fe:] = d_linear


def row_part(q, at, row, grad_ref, wboth_ref, part_ref):
    packed = part_ref.shape[3]
    width, half = packed * 2 // 3, packed // 3
    part = dot(grad_ref[pl.ds(row, 96), :], wboth_ref[pl.ds(pl.multiple_of(q * width, width), width), :], ((1,), (1,)))
    part_ref[q, pl.ds(at, 8), :, :width] = part[:64].reshape(8, 8, width).astype(BF16)
    tails = part[64:].reshape(4, 8, width)
    left, right = tails[:, :, :half], tails[:, :, half:]
    low = low_half((4, 8, half))
    one = jnp.where(low, left, swap4(right))
    two = jnp.where(low, swap4(left), right)
    part_ref[q, pl.ds(at, 8), :, width:] = jnp.stack([one, two], axis=1).reshape(8, 8, half).astype(BF16)


GROUPS = 8


def step_kernel(
    conv_hbm, gate_in_hbm, first_hbm, param_hbm, shift_hbm, wr_hbm, wi_hbm, wo_hbm, mixed_hbm, d_out_hbm,
    ids_hbm, wts_hbm, wg_hbm, wu_hbm, wd_hbm,
    both_hbm, down_hbm, proj_ref, rec_ref, gate_ref,
    conv_ref, gate_in_ref, first_ref, param_ref, shift_ref, wr_ref, wi_ref, mixed_ref, d_out_ref, ids_ref, wts_ref,
    send_ref, code_ref, got_ref, rows_ref, cot_ref, grad_ref, hidden_ref, part_ref, far_ref, comb_ref,
    near_ref, back_ref, ret_ref, saved_ref, merged_ref, temp_ref, slow_ref, wboth_ref, wd_ref, wo_ref, both_ref,
    down_ref, mix_ref, acc_ref, local_ref, keep_ref, pair_ref, pair_got, x_ref, x_far_ref, x_comb_ref, x_near_ref, z_ref, z_got,
    own_ref, lead_ref, plane_ref, plane_got, line_got,
    load_sem, store_sem, send_sem, recv_sem, y_send, y_recv, f_send, f_recv, far_send, far_recv,
    near_send, near_recv, ret_send, ret_recv, mix_send, mix_recv, pair_send, pair_recv,
    x_send, x_recv, z_send, z_recv, plane_send, plane_recv, line_send, line_recv,
):
    sp, tp, z, x, c = place()
    n_tp, n_sp = part_ref.shape[0], part_ref.shape[1]
    tokens, width = d_out_ref.shape
    half = width // 2
    fe = wd_ref.shape[0]
    right, left, far = (tp + 1) % n_tp, (tp + n_tp - 1) % n_tp, (tp + 2) % n_tp
    drive_ref, prev_ref, state_ref, reset_ref, norm_ref, inp_ref = [temp_ref.at[k] for k in range(6)]

    greet(sp, tp, n_sp, n_tp)
    loads = [
        pltpu.make_async_copy(src, dst, load_sem.at[k])
        for k, (src, dst) in enumerate((
            (ids_hbm, ids_ref), (wts_hbm, wts_ref), (d_out_hbm, d_out_ref), (mixed_hbm, mixed_ref),
            (conv_hbm, conv_ref), (param_hbm, param_ref), (shift_hbm, shift_ref), (wr_hbm, wr_ref), (wi_hbm, wi_ref),
            (first_hbm, first_ref), (gate_in_hbm, gate_in_ref),
            (wg_hbm, wboth_ref.at[:, pl.ds(0, fe)]), (wu_hbm, wboth_ref.at[:, pl.ds(fe, fe)]),
            (wd_hbm, wd_ref), (wo_hbm, wo_ref),
        ))
    ]
    for load in loads:
        load.start()
    for load in loads[:4]:
        load.wait()
    pack(ids_ref, wts_ref, d_out_ref, mixed_ref, send_ref, code_ref)
    got_ref[tp, sp] = send_ref[sp]
    for load in loads[4:11]:
        load.wait()
    gates(
        conv_ref, param_ref, slow_ref, shift_ref, wr_ref, wi_ref, saved_ref, drive_ref, reset_ref, norm_ref, inp_ref
    )
    run_forward(first_ref, saved_ref, drive_ref, prev_ref, state_ref)
    factors(
        conv_ref, gate_in_ref, slow_ref, saved_ref, merged_ref, prev_ref, state_ref, reset_ref, norm_ref, inp_ref
    )
    all_here(n_sp, n_tp)

    x_order = (0, 1, 3, 2)
    for dx in x_order:
        for dc in (0, 1):
            if dx or dc:
                to = z * 8 + ((x + dx) % 4) * 2 + (c + dc) % 2
                remote(send_ref.at[to], got_ref.at[tp, sp], send_sem, recv_sem.at[0, dx], to, tp).start()

    def send_group(i, _):
        for dx in x_order:
            for dc in (0, 1):
                to = offset_device(z, x, c, z_offset(i), 2 * dx + dc)
                remote(send_ref.at[to], got_ref.at[tp, sp], send_sem, recv_sem.at[i, dx], to, tp).start()
        return 0

    def source_group(i):
        return (z + 8 - z_offset(i)) % 8

    def gather_pair(i, dx):
        at = source_group(i) * 8 + ((x + 4 - dx) % 4) * 2
        wait_bytes(got_ref.at[tp, pl.ds(at, 1 if isinstance(i, int) and i + dx == 0 else 2)], recv_sem.at[i, dx])
        block = got_ref.at[tp, pl.ds(at, 2)]
        remote(block, block, y_send.at[0], y_recv.at[0, i], sp, right).start()
        remote(block, block, y_send.at[1], y_recv.at[1, i], sp, left).start()

    def gather(i):
        @pl.when(i > 1)
        def _():
            gather_pair(i, 0)

        for dx in x_order[1:]:
            gather_pair(i, dx)

    def relay(i):
        at = source_group(i) * 8
        wait_bytes(got_ref.at[left, pl.ds(at, 8)], y_recv.at[0, i])
        block = got_ref.at[left, pl.ds(at, 4)]
        remote(block, block, f_send.at[0], f_recv.at[0, i], sp, right).start()
        wait_bytes(got_ref.at[right, pl.ds(at, 8)], y_recv.at[1, i])
        block = got_ref.at[right, pl.ds(at + 4, 4)]
        remote(block, block, f_send.at[1], f_recv.at[1, i], sp, left).start()

    def compute(i):
        group = source_group(i)
        at, row = group * 8, pl.multiple_of(group * 96, 32)
        wait_bytes(got_ref.at[far, pl.ds(at, 4)], f_recv.at[0, i])
        wait_bytes(got_ref.at[far, pl.ds(at + 4, 4)], f_recv.at[1, i])
        for q in range(n_tp):
            unpack(got_ref, q, at, row, rows_ref, cot_ref)
        expert_terms(row, rows_ref, cot_ref, grad_ref, hidden_ref, wboth_ref, wd_ref)
        for q in range(n_tp):
            row_part(q, at, row, grad_ref, wboth_ref, part_ref)

    def reduce(i):
        at = source_group(i) * 8
        lower, upper = pl.ds(at, 4), pl.ds(at + 4, 4)
        remote(part_ref.at[far, lower], far_ref.at[0, i], far_send.at[0], far_recv.at[0, i], sp, left).start()
        remote(part_ref.at[far, upper], far_ref.at[1, i], far_send.at[1], far_recv.at[1, i], sp, right).start()
        remote(
            part_ref.at[left, upper], near_ref.at[0, i, pl.ds(4, 4)], near_send.at[0], near_recv.at[0, i], sp, left
        ).start()
        remote(
            part_ref.at[right, lower], near_ref.at[1, i, pl.ds(0, 4)], near_send.at[1], near_recv.at[1, i], sp, right
        ).start()

    def add_far(i):
        at = source_group(i) * 8
        for side, (to, first) in enumerate(((left, 0), (right, 4))):
            wait_bytes(far_ref.at[side, i], far_recv.at[side, i])
            own = part_ref[to, pl.ds(at + first, 4)].astype(F32)
            comb_ref[side, i] = (own + far_ref[side, i].astype(F32)).astype(BF16)
            remote(
                comb_ref.at[side, i], near_ref.at[side, i, pl.ds(first, 4)],
                near_send.at[side], near_recv.at[side, i], sp, to,
            ).start()

    def give_back(i):
        group = source_group(i)
        at = group * 8
        wait_bytes(near_ref.at[0, i], near_recv.at[0, i])
        wait_bytes(near_ref.at[1, i], near_recv.at[1, i])
        total = part_ref[tp, pl.ds(at, 8)].astype(F32) + near_ref[0, i].astype(F32) + near_ref[1, i].astype(F32)
        back_ref[pl.ds(at, 8)] = total.astype(BF16)

        def send(j, _):
            to = group * 8 + ((x + j // 2) % 4) * 2 + (c + j % 2) % 2
            remote(back_ref.at[to], ret_ref.at[sp], ret_send, ret_recv, to, tp).start()
            return 0

        lax.fori_loop(jnp.where(i == 0, 1, 0), 8, send, 0)

    gather_pair(0, 0)
    lax.fori_loop(1, GROUPS, send_group, 0)
    gather_pair(0, 1)
    gather_pair(0, 3)
    gather_pair(1, 0)
    gather_pair(0, 2)

    stages = (
        (reduce, 5, 0, 5), (gather, 0, 1, 7), (relay, 1, 0, 8), (compute, 2, 0, 8), (add_far, 6, 0, 4),
        (give_back, 7, 0, 3),
    )

    def step(s, _):
        for stage, begin, group, count in stages:
            if stage is compute:

                @pl.when(s == begin)
                def _():
                    for load in loads[11:14]:
                        load.wait()

            @pl.when(jnp.logical_and(s >= begin, s < begin + count))
            def _():
                stage(s - begin + group)

        return 0

    lax.fori_loop(0, 10, step, 0)
    lax.fori_loop(5, GROUPS, lambda i, _: reduce(i) or 0, 0)

    over_rows = ((0,), (0,))

    def weight_grads(k, _):
        cols = pl.ds(pl.multiple_of(k * 512, 512), 512)
        both_ref[cols, :] = dot(rows_ref[:, cols], grad_ref[...], over_rows).astype(BF16)
        down_ref[:, cols] = dot(hidden_ref[...], cot_ref[:, cols], over_rows).astype(BF16)
        return 0

    lax.fori_loop(0, rows_ref.shape[1] // 512, weight_grads, 0)
    stores = [
        pltpu.make_async_copy(both_ref, both_hbm, store_sem.at[0]),
        pltpu.make_async_copy(down_ref, down_hbm, store_sem.at[1]),
    ]
    for store in stores:
        store.start()

    def finish_rows(i, _):
        add_far(i)
        give_back(i - 1)
        return 0

    lax.fori_loop(4, GROUPS, finish_rows, 0)

    (main, tail), low = slot_tests(code_ref[...], n_sp)
    main_pick = jnp.where(main[0] | main[1], 1.0, 0.0).astype(BF16)
    in_tail = tail[0] | tail[1]
    low_pick = jnp.where(in_tail & low, 1.0, 0.0).astype(BF16)
    high_pick = jnp.where(in_tail & ~low, 1.0, 0.0).astype(BF16)
    give_back(GROUPS - 1)
    ret_ref[sp] = back_ref[sp]
    wait_bytes(ret_ref.at[pl.ds(0, n_sp - 1)], ret_recv)
    main_rows = ret_ref[:, :, :width].astype(F32).reshape(n_sp * 8, width).astype(BF16)
    tail_rows = ret_ref[:, :, width:].astype(F32).reshape(n_sp * 8, half).astype(BF16)
    summed = dot(main_pick, main_rows, over_rows) + jnp.concatenate(
        [dot(low_pick, tail_rows, over_rows), dot(high_pick, tail_rows, over_rows)], axis=1
    )
    mix_ref[tp] = (d_out_ref[...].astype(F32) + summed).astype(BF16)
    for side, to in enumerate((right, left)):
        remote(mix_ref.at[tp], mix_ref.at[tp], mix_send.at[side], mix_recv.at[side], sp, to).start()
    loads[14].wait()

    blocks = (tp, left, right, far)
    x_right, x_left, x_far = (x + 1) % 4, (x + 3) % 4, (x + 2) % 4
    part_rows = half // 8
    cut = part_rows // 2

    def along(x_to, z_to=z):
        return z_to * 8 + x_to * 2 + c

    def products(n):
        q = blocks[n]
        whole = mix_ref[q]
        block = dot(whole, wo_ref[:, pl.ds(pl.multiple_of(q * width, width), width)], ((1,), (1,)))
        if n == 0:
            acc_ref[...] = block
        else:
            acc_ref[...] += block
        for h in (0, 1):
            slot = 2 * n + h
            grad = dot(whole[:, h * half : (h + 1) * half], merged_ref[...], over_rows)
            grad = grad.reshape(4, 2, part_rows, width)
            keep_ref[slot] = jnp.where(c == 0, grad[:, 0], grad[:, 1])
            pair_ref[slot] = jnp.where(c == 0, grad[:, 1], grad[:, 0]).astype(BF16)
            remote(
                pair_ref.at[slot], pair_got.at[slot], pair_send, pair_recv.at[slot], sp + 1 - 2 * c, tp
            ).start()

    def x_start(n):
        for slot in (2 * n, 2 * n + 1):
            wait_bytes(pair_got.at[slot], pair_recv.at[slot])
            total = keep_ref[slot] + pair_got[slot].astype(F32)
            keep_ref[slot] = total
            x_ref[slot] = total.astype(BF16)
            lower, upper = pl.ds(0, cut), pl.ds(cut, cut)
            for block, rows, ref, side, at, to in (
                (x_far, lower, x_far_ref, 0, None, x_left),
                (x_far, upper, x_far_ref, 1, None, x_right),
                (x_left, upper, x_near_ref, 0, upper, x_left),
                (x_right, lower, x_near_ref, 1, lower, x_right),
            ):
                goal = ref.at[slot, side] if at is None else ref.at[slot, side, at]
                send, recv = (x_send.at[0], x_recv.at[0, slot, side]) if at is None else (x_send.at[1], x_recv.at[1, slot, side])
                remote(x_ref.at[slot, block, rows], goal, send, recv, along(to), tp).start()

    def x_relay(n):
        for slot in (2 * n, 2 * n + 1):
            for side, to, first in ((0, x_left, 0), (1, x_right, cut)):
                wait_bytes(x_far_ref.at[slot, side], x_recv.at[0, slot, side])
                own = keep_ref[slot, to, first : first + cut]
                x_comb_ref[slot, side] = (own + x_far_ref[slot, side].astype(F32)).astype(BF16)
                remote(
                    x_comb_ref.at[slot, side], x_near_ref.at[slot, side, pl.ds(first, cut)],
                    x_send.at[1], x_recv.at[1, slot, side], along(to), tp,
                ).start()

    def z_start(n):
        for h in (0, 1):
            slot = 2 * n + h
            total = keep_ref[slot, x]
            for side in (0, 1):
                wait_bytes(x_near_ref.at[slot, side], x_recv.at[1, slot, side])
                total = total + x_near_ref[slot, side].astype(F32)
            z_ref[slot] = total.astype(BF16)
            to = 2 * blocks[n] + h

            @pl.when(to == z)
            def _():
                own_ref[...] = total

            @pl.when(to != z)
            def _():
                remote(z_ref.at[slot], z_got.at[z], z_send, z_recv, along(x, to), tp).start()

    upper_half = tokens // 2
    products(0)
    x_start(0)
    wait_bytes(mix_ref.at[left], mix_recv.at[0])
    piece = mix_ref.at[left, pl.ds(0, upper_half)]
    remote(piece, piece, mix_send.at[2], mix_recv.at[2], sp, right).start()
    wait_bytes(mix_ref.at[right], mix_recv.at[1])
    piece = mix_ref.at[right, pl.ds(upper_half, upper_half)]
    remote(piece, piece, mix_send.at[3], mix_recv.at[3], sp, left).start()
    products(1)
    products(2)
    x_start(1)
    x_relay(0)
    x_start(2)
    wait_bytes(mix_ref.at[far, pl.ds(0, upper_half)], mix_recv.at[2])
    wait_bytes(mix_ref.at[far, pl.ds(upper_half, upper_half)], mix_recv.at[3])
    products(3)

    d_merged = acc_ref[...]
    gate_ref[...] = (d_merged * saved_ref[5]).astype(BF16)
    acc_ref[...] = d_merged * saved_ref[6]

    def back(group, carry):
        for i in range(8):
            t = pl.ds(tokens - 1 - (group * 8 + i), 1)
            grad = acc_ref[t, :] + carry
            local_ref[t, :] = grad
            carry = grad * saved_ref[0, t, :]
        return carry

    lead = lax.fori_loop(0, tokens // 8, back, jnp.zeros((1, width), F32))
    lead_ref[0, 0:1, :] = saved_ref[1, 0:1, :] * saved_ref[0, 0:1, :]
    lead_ref[0, 1:2, :] = lead
    own_at = sp % 8
    plane_got[own_at] = lead_ref[0]
    for dx in (2, 1, 3, 0):
        for dc in (1, 0):
            if dx or dc:
                to = z * 8 + ((x + dx) % 4) * 2 + (c + dc) % 2
                remote(lead_ref.at[0], plane_got.at[own_at], plane_send, plane_recv, to, tp).start()
    x_start(3)
    x_relay(1)
    x_relay(2)

    wait_bytes(plane_got.at[pl.ds(0, 7)], plane_recv)
    prod, carry = jnp.ones((1, width), F32), jnp.zeros((1, width), F32)
    own_prod, own_carry = prod, carry
    for k in range(7, -1, -1):
        own_prod, own_carry = jnp.where(k == own_at, prod, own_prod), jnp.where(k == own_at, carry, own_carry)
        pair = plane_got[k]
        carry = pair[1:2, :] + pair[0:1, :] * carry
        prod = pair[0:1, :] * prod
    plane_ref[0, 0:1, :] = prod
    plane_ref[0, 1:2, :] = carry
    line_got[z] = plane_ref[0]
    for dz in (4, 3, 5, 2, 6, 1, 7):
        remote(plane_ref.at[0], line_got.at[z], line_send, line_recv, along(x, (z + dz) % 8), tp).start()
    z_start(0)
    x_relay(3)
    for n in (1, 2, 3):
        z_start(n)

    wait_bytes(line_got.at[pl.ds(0, 7)], line_recv)
    carry = jnp.zeros((1, width), F32)
    for k in range(7, 0, -1):
        pair = line_got[k]
        carry = jnp.where(k > z, pair[1:2, :] + pair[0:1, :] * carry, carry)
    incoming = own_carry + own_prod * carry
    heads, hd = wr_ref.shape[0], wr_ref.shape[1]
    for h in range(heads):
        cols = slice(h * hd, (h + 1) * hd)
        grad = local_ref[:, cols] + saved_ref[1, :, cols] * incoming[:, cols]
        by_reset = (grad * saved_ref[2, :, cols]).astype(BF16)
        by_input = (grad * saved_ref[3, :, cols]).astype(BF16)
        rec_ref[:, cols] = (
            grad * saved_ref[4, :, cols]
            + dot(by_reset, wr_ref[h], ((1,), (1,)))
            + dot(by_input, wi_ref[h], ((1,), (1,)))
        ).astype(BF16)

    wait_bytes(z_got.at[pl.ds(0, 7)], z_recv)
    total = own_ref[...]
    for d in range(1, 8):
        total = total + z_got[(z + d) % 8].astype(F32)
    proj_ref[...] = total

    wait_bytes(send_ref.at[pl.ds(0, n_sp - 1)], send_sem)
    for side in (0, 1):
        wait_bytes(got_ref.at[tp], y_send.at[side])
        wait_bytes(got_ref.at[tp, pl.ds(0, n_sp // 2)], f_send.at[side])
        wait_bytes(part_ref.at[tp, pl.ds(0, n_sp // 2)], far_send.at[side])
        wait_bytes(part_ref.at[tp], near_send.at[side])
        wait_bytes(mix_ref.at[tp], mix_send.at[side])
        wait_bytes(mix_ref.at[tp, pl.ds(0, upper_half)], mix_send.at[2 + side])
    wait_bytes(back_ref.at[pl.ds(0, n_sp - 1)], ret_send)
    wait_bytes(pair_ref, pair_send)
    wait_bytes(x_far_ref, x_send.at[0])
    wait_bytes(x_near_ref, x_send.at[1])
    wait_bytes(z_ref.at[pl.ds(0, 7)], z_send)
    wait_bytes(plane_got.at[pl.ds(0, 7)], plane_send)
    wait_bytes(line_got.at[pl.ds(0, 7)], line_send)
    for store in stores:
        store.wait()


def whole_step(n_sp, n_tp, *args):
    conv, w_gate = args[0], args[12]
    tokens, width = conv.shape
    model, fe = w_gate.shape
    packed = width + width // 2
    rows = n_sp * 12
    block = (model // n_sp, width)
    dma = pltpu.SemaphoreType.DMA
    inner = (0, 1, 2, 3, 4, 5, 6, 8, 9, 10, 11)
    return pl.pallas_call(
        step_kernel,
        out_shape=(
            jax.ShapeDtypeStruct((model, 2 * fe), BF16),
            jax.ShapeDtypeStruct((fe, model), BF16),
            jax.ShapeDtypeStruct(block, F32),
            jax.ShapeDtypeStruct((tokens, width), BF16),
            jax.ShapeDtypeStruct((tokens, width), BF16),
        ),
        in_specs=[ANY] * 15,
        out_specs=(ANY, ANY, VM, VM, VM),
        scratch_shapes=[
            *(pltpu.VMEM(args[k].shape, args[k].dtype) for k in inner),
            pltpu.VMEM((n_sp, 16, packed), BF16),
            pltpu.VMEM((2, tokens), jnp.int32),
            pltpu.VMEM((n_tp, n_sp, 16, packed), BF16),
            pltpu.VMEM((rows, model), BF16),
            pltpu.VMEM((rows, model), BF16),
            pltpu.VMEM((rows, 2 * fe), BF16),
            pltpu.VMEM((rows, fe), BF16),
            pltpu.VMEM((n_tp, n_sp, 8, packed), BF16),
            pltpu.VMEM((2, GROUPS, 4, 8, packed), BF16),
            pltpu.VMEM((2, GROUPS, 4, 8, packed), BF16),
            pltpu.VMEM((2, GROUPS, 8, 8, packed), BF16),
            pltpu.VMEM((n_sp, 8, packed), BF16),
            pltpu.VMEM((n_sp, 8, packed), BF16),
            pltpu.VMEM((7, tokens, width), F32),
            pltpu.VMEM((tokens, width), BF16),
            pltpu.VMEM((6, tokens, width), F32),
            pltpu.VMEM((1, width), F32),
            pltpu.VMEM((model, 2 * fe), BF16),
            pltpu.VMEM((fe, model), BF16),
            pltpu.VMEM((width, model), BF16),
            pltpu.VMEM((model, 2 * fe), BF16),
            pltpu.VMEM((fe, model), BF16),
            pltpu.VMEM((n_tp, tokens, width), BF16),
            pltpu.VMEM((tokens, width), F32),
            pltpu.VMEM((tokens, width), F32),
            pltpu.VMEM((8, 4, *block), F32),
            pltpu.VMEM((8, 4, *block), BF16),
            pltpu.VMEM((8, 4, *block), BF16),
            pltpu.VMEM((8, 4, *block), BF16),
            pltpu.VMEM((8, 2, block[0] // 2, width), BF16),
            pltpu.VMEM((8, 2, block[0] // 2, width), BF16),
            pltpu.VMEM((8, 2, *block), BF16),
            pltpu.VMEM((8, *block), BF16),
            pltpu.VMEM((8, *block), BF16),
            pltpu.VMEM(block, F32),
            pltpu.VMEM((1, 2, width), F32),
            pltpu.VMEM((1, 2, width), F32),
            pltpu.VMEM((8, 2, width), F32),
            pltpu.VMEM((8, 2, width), F32),
            dma((15,)), dma((2,)), dma, dma((8, 4)), dma((2,)), dma((2, 8)), dma((2,)), dma((2, 8)),
            dma((2,)), dma((2, 8)), dma((2,)), dma((2, 8)), dma, dma, dma((4,)), dma((4,)),
            dma, dma((8,)), dma((2,)), dma((2, 8, 2)), dma, dma, dma, dma, dma, dma,
        ],
        compiler_params=pltpu.CompilerParams(
            collective_id=0, has_side_effects=True, vmem_limit_bytes=63 * 2**20
        ),
        name="whole_step",
    )(*args)


def write_kernel(both_ref, down_ref, proj_ref, rec_ref, gate_ref, gg_ref, gu_ref, gd_ref, p_ref, r_ref, g_ref):
    fe = gg_ref.shape[1]
    gg_ref[...] = both_ref[:, :fe].astype(F32)
    gu_ref[...] = both_ref[:, fe:].astype(F32)
    gd_ref[...] = down_ref[...].astype(F32)
    p_ref[...] = proj_ref[...]
    r_ref[...] = rec_ref[...]
    g_ref[...] = gate_ref[...]


def write_out(both, down, proj, rec, gate, parts=4):
    model, fe = both.shape[0], both.shape[1] // 2

    def cut(array):
        return pl.BlockSpec((array.shape[0] // parts, array.shape[1]), lambda i: (i, 0))

    outs = (
        jax.ShapeDtypeStruct((model, fe), F32),
        jax.ShapeDtypeStruct((model, fe), F32),
        jax.ShapeDtypeStruct((fe, model), F32),
        jax.ShapeDtypeStruct(proj.shape, proj.dtype),
        jax.ShapeDtypeStruct(rec.shape, rec.dtype),
        jax.ShapeDtypeStruct(gate.shape, gate.dtype),
    )
    ins = (both, down, proj, rec, gate)
    return pl.pallas_call(
        write_kernel,
        grid=(parts,),
        out_shape=outs,
        in_specs=[cut(a) for a in ins],
        out_specs=tuple(cut(a) for a in outs),
        name="write_out",
    )(*ins)


def body(
    n_sp, n_tp, conv_out, gate_in, block_states, decay_param, decay_shift, w_reset, w_input, w_out,
    mixed, d_out, expert_ids, route_weights, w_gate, w_up, w_down,
):
    both, down, proj, rec, gate = whole_step(
        n_sp, n_tp, conv_out, gate_in, block_states, decay_param[None, :], decay_shift[None, :], w_reset, w_input, w_out,
        mixed, d_out, expert_ids.T, route_weights.T, w_gate[0], w_up[0], w_down[0],
    )
    gg, gu, gd, proj, rec, gate = write_out(both, down, proj, rec, gate)
    return gg[None], gu[None], gd[None], proj, rec, gate


def solution(mesh):
    in_specs = (
        P("sp", "tp"), P("sp", "tp"), P("sp", "tp"), P("tp"), P("sp"),
        P("tp", None, None), P("tp", None, None), P("tp", None),
        P("sp", "tp"), P("sp", "tp"), P("sp", None), P("sp", None),
        P("sp", None, "tp"), P("sp", None, "tp"), P("sp", "tp", None),
    )
    out_specs = (
        P("sp", None, "tp"), P("sp", None, "tp"), P("sp", "tp", None),
        P("sp", "tp"), P("sp", "tp"), P("sp", "tp"),
    )
    run = functools.partial(body, mesh.shape["sp"], mesh.shape["tp"])
    return jax.shard_map(run, mesh=mesh, in_specs=in_specs, out_specs=out_specs, check_vma=False)
```

```python
import functools

import jax
import jax.numpy as jnp
from jax import lax
from jax.experimental import pallas as pl
from jax.experimental.pallas import tpu as pltpu
from jax.sharding import PartitionSpec as P

F32 = jnp.float32
BF16 = jnp.bfloat16
MESH = pl.DeviceIdType.MESH
VM = pl.BlockSpec(memory_space=pltpu.VMEM)
ANY = pl.BlockSpec(memory_space=pl.ANY)


def dot(a, b, dims=((1,), (0,))):
    return lax.dot_general(a, b, (dims, ((), ())), preferred_element_type=F32)


def swap4(value):
    return pltpu.roll(value, 4, axis=1)


def low_half(shape):
    return lax.broadcasted_iota(jnp.int32, shape, 1) < 4


def gates(conv_ref, param_ref, slow_ref, shift_ref, wr_ref, wi_ref, saved_ref, drive_ref, reset_ref, norm_ref, inp_ref):
    hd = wr_ref.shape[1]
    rows = conv_ref.shape[0]
    shift = jnp.transpose(jnp.broadcast_to(shift_ref[...], (8, rows)))[:, 0:1]
    param = param_ref[...]
    slow_ref[...] = jnp.maximum(-param, 0.0) + jnp.log1p(jnp.exp(-jnp.abs(param)))
    for h in range(wr_ref.shape[0]):
        cols = slice(h * hd, (h + 1) * hd)
        conv = conv_ref[:, cols]
        reset = jax.nn.sigmoid(dot(conv, wr_ref[h]))
        inp = jax.nn.sigmoid(dot(conv, wi_ref[h]))
        log_decay = -8.0 * reset * slow_ref[:, cols] + shift
        decay = jnp.exp(log_decay)
        twice = 2.0 * log_decay
        small = jnp.maximum(twice, -0.5)
        series = 1.0 + small * (1.0 / 10.0)
        for n in (9, 8, 7, 6, 5, 4, 3, 2):
            series = 1.0 + small * (1.0 / n) * series
        less = jnp.where(twice > -0.5, small * series, jnp.exp(twice) - 1.0)
        norm = jnp.sqrt(-less)
        saved_ref[0, :, cols] = decay
        reset_ref[:, cols] = reset
        norm_ref[:, cols] = norm
        inp_ref[:, cols] = inp
        drive_ref[:, cols] = norm * inp * conv.astype(F32)


def run_forward(first_ref, saved_ref, drive_ref, prev_ref, state_ref):
    rows, width = drive_ref.shape

    def step(group, state):
        for i in range(8):
            t = pl.ds(group * 8 + i, 1)
            prev_ref[t, :] = state
            state = saved_ref[0, t, :] * state + drive_ref[t, :]
            state_ref[t, :] = state
        return state

    lax.fori_loop(0, rows // 8, step, first_ref[...])

    def back(group, prod):
        for i in range(8):
            t = rows - 1 - (group * 8 + i)
            saved_ref[1, pl.ds(t, 1), :] = prod
            prod = prod * saved_ref[0, pl.ds(t, 1), :]
        return prod

    lax.fori_loop(0, rows // 8, back, jnp.ones((1, width), F32))


def factors(
    conv_ref, gate_ref, slow_ref, saved_ref, merged_ref, prev_ref, state_ref, reset_ref, norm_ref, inp_ref
):
    hd = 128
    for h in range(conv_ref.shape[1] // hd):
        cols = slice(h * hd, (h + 1) * hd)
        conv = conv_ref[:, cols].astype(F32)
        decay, reset, norm, inp = saved_ref[0, :, cols], reset_ref[:, cols], norm_ref[:, cols], inp_ref[:, cols]
        by_log = decay * prev_ref[:, cols] - inp * conv * decay * decay / norm
        saved_ref[2, :, cols] = by_log * (-8.0 * slow_ref[:, cols]) * reset * (1.0 - reset)
        saved_ref[3, :, cols] = norm * conv * inp * (1.0 - inp)
        saved_ref[4, :, cols] = norm * inp
        state = state_ref[:, cols]
        value = gate_ref[:, cols].astype(F32)
        k = 0.7978845608028654
        square = value * value
        bent = jnp.tanh(k * (value + 0.044715 * value * square))
        act = 0.5 * value * (1.0 + bent)
        slope = 0.5 * (1.0 + bent) + 0.5 * value * (1.0 - bent * bent) * k * (1.0 + 3.0 * 0.044715 * square)
        saved_ref[5, :, cols] = state * slope
        saved_ref[6, :, cols] = act
        merged_ref[:, cols] = (act * state).astype(BF16)


def slot_tests(codes, experts):
    tokens = codes.shape[1]
    row = lax.broadcasted_iota(jnp.int32, (experts * 8, tokens), 0)
    base = (row // 8) * 16
    main = base + row % 8
    tail = base + 8 + row % 4
    return [[codes[k : k + 1, :] == want for k in (0, 1)] for want in (main, tail)], row % 8 < 4


def pack(ids_ref, wts_ref, d_out_ref, mixed_ref, send_ref, code_ref):
    experts = send_ref.shape[0]
    tokens, width = d_out_ref.shape
    half = width // 2
    each = lax.broadcasted_iota(jnp.int32, (experts, tokens), 0)
    named = [ids_ref[k : k + 1, :] == each for k in (0, 1)]
    both = jnp.where(named[0] | named[1], 1.0, 0.0).astype(BF16)
    earlier = (
        lax.broadcasted_iota(jnp.int32, (tokens, tokens), 0)
        < lax.broadcasted_iota(jnp.int32, (tokens, tokens), 1)
    )
    count = dot(both, jnp.where(earlier, 1.0, 0.0).astype(BF16))
    codes = []
    for k in (0, 1):
        rank = jnp.sum(jnp.where(named[k], count, 0.0), axis=0, keepdims=True)
        codes.append(ids_ref[k : k + 1, :] * 16 + rank.astype(jnp.int32))
        code_ref[k : k + 1, :] = codes[k]
    codes = jnp.concatenate(codes, axis=0)
    (main, tail), low = slot_tests(codes, experts)

    def weight(tests):
        return jnp.sum(
            jnp.where(tests[0], wts_ref[0:1, :], 0.0) + jnp.where(tests[1], wts_ref[1:2, :], 0.0),
            axis=1,
            keepdims=True,
        )

    main_pick = jnp.where(main[0] | main[1], 1.0, 0.0).astype(BF16)
    in_tail = tail[0] | tail[1]
    low_pick = jnp.where(in_tail & low, 1.0, 0.0).astype(BF16)
    high_pick = jnp.where(in_tail & ~low, 1.0, 0.0).astype(BF16)

    for at, (ref, w_main, w_tail) in enumerate(
        ((d_out_ref, weight(main), weight(tail)), (mixed_ref, None, None))
    ):
        first = dot(main_pick, ref[...])
        second = dot(low_pick, ref[:, :half]) + dot(high_pick, ref[:, half:])
        if w_main is not None:
            first, second = first * w_main, second * w_tail
        rows = slice(at * 8, at * 8 + 8)
        send_ref[:, rows, :width] = first.reshape(experts, 8, width).astype(BF16)
        send_ref[:, rows, width:] = second.reshape(experts, 8, half).astype(BF16)


def place():
    sp, tp = lax.axis_index("sp"), lax.axis_index("tp")
    return sp, tp, sp // 8, (sp // 2) % 4, sp % 2


Z_ORDER = (0, 1, 6, 3, 5, 4, 2, 7)


WORK_ORDER = (2, 3, 4, 5, 6, 1, 7, 0)


def z_offset(i):
    return sum(jnp.where(i == k, dz, 0) for k, dz in enumerate(Z_ORDER))


def work_order(i):
    return sum(jnp.where(i == k, group, 0) for k, group in enumerate(WORK_ORDER))


def offset_device(z, x, c, dz, j):
    return ((z + dz) % 8) * 8 + ((x + j // 2) % 4) * 2 + (c + j % 2) % 2


def greet(sp, tp, n_sp, n_tp):
    barrier = pltpu.get_barrier_semaphore()

    def to_sp(k, _):
        to = (sp + n_sp // 2 + k) % n_sp
        pl.semaphore_signal(barrier, inc=1, device_id=(to, tp), device_id_type=MESH)
        return 0

    lax.fori_loop(0, n_sp // 2, to_sp, 0)
    lax.fori_loop(1 - n_sp // 2, 0, to_sp, 0)
    for k in range(1, n_tp):
        pl.semaphore_signal(barrier, inc=1, device_id=(sp, (tp + k) % n_tp), device_id_type=MESH)


def all_here(n_sp, n_tp):
    pl.semaphore_wait(pltpu.get_barrier_semaphore(), n_sp - 1 + n_tp - 1)


def remote(src, dst, send_sem, recv_sem, sp, tp):
    return pltpu.make_async_remote_copy(
        src_ref=src, dst_ref=dst, send_sem=send_sem, recv_sem=recv_sem,
        device_id=(sp, tp), device_id_type=MESH,
    )


def wait_bytes(ref, sem):
    pltpu.make_async_copy(ref, ref, sem).wait()


def unpack(got_ref, q, at, row, rows_ref, cot_ref):
    packed = got_ref.shape[3]
    width, half = packed * 2 // 3, packed // 3
    cols = slice(q * width, (q + 1) * width)
    for first, ref in ((0, cot_ref), (8, rows_ref)):
        block = got_ref[q, pl.ds(at, 8), first : first + 8, :].astype(F32)
        ref[pl.ds(row, 64), cols] = block[:, :, :width].reshape(64, width).astype(BF16)
        tails = block[:, :, width:]
        turned = swap4(tails)
        tails, turned = tails.reshape(4, 2, 8, half), turned.reshape(4, 2, 8, half)
        low = low_half((4, 8, half))
        left = jnp.where(low, tails[:, 0], turned[:, 1])
        right = jnp.where(low, turned[:, 0], tails[:, 1])
        both = jnp.concatenate([left, right], axis=2).reshape(32, width)
        ref[pl.ds(row + 64, 32), cols] = both.astype(BF16)


def expert_terms(row, rows_ref, cot_ref, grad_ref, hidden_ref, wboth_ref, wd_ref):
    fe = wd_ref.shape[0]
    rows = pl.ds(row, 96)
    both = dot(rows_ref[rows, :], wboth_ref[...])
    up_pre, linear = both[:, :fe], both[:, fe:]
    d_hidden = dot(cot_ref[rows, :], wd_ref[...], ((1,), (1,)))
    gate = jax.nn.sigmoid(up_pre)
    silu = up_pre * gate
    hidden_ref[rows, :] = (silu * linear).astype(BF16)
    d_linear = (d_hidden * silu).astype(BF16)
    d_up = (d_hidden * linear * gate * (1.0 + up_pre * (1.0 - gate))).astype(BF16)
    grad_ref[rows, :fe] = d_up
    grad_ref[rows, fe:] = d_linear


def row_part(q, at, row, grad_ref, wboth_ref, part_ref):
    packed = part_ref.shape[3]
    width, half = packed * 2 // 3, packed // 3
    part = dot(grad_ref[pl.ds(row, 96), :], wboth_ref[pl.ds(pl.multiple_of(q * width, width), width), :], ((1,), (1,)))
    part_ref[q, pl.ds(at, 8), :, :width] = part[:64].reshape(8, 8, width).astype(BF16)
    tails = part[64:].reshape(4, 8, width)
    left, right = tails[:, :, :half], tails[:, :, half:]
    low = low_half((4, 8, half))
    one = jnp.where(low, left, swap4(right))
    two = jnp.where(low, swap4(left), right)
    part_ref[q, pl.ds(at, 8), :, width:] = jnp.stack([one, two], axis=1).reshape(8, 8, half).astype(BF16)


GROUPS = 8


def step_kernel(
    conv_hbm, gate_in_hbm, first_hbm, param_hbm, shift_hbm, wr_hbm, wi_hbm, wo_hbm, mixed_hbm, d_out_hbm,
    ids_hbm, wts_hbm, wg_hbm, wu_hbm, wd_hbm,
    both_hbm, down_hbm, proj_hbm, rec_hbm, gate_hbm,
    conv_ref, gate_in_ref, first_ref, param_ref, shift_ref, wr_ref, wi_ref, mixed_ref, d_out_ref, ids_ref, wts_ref,
    proj_ref, rec_ref, gate_ref, send_ref, code_ref, got_ref, rows_ref, cot_ref, grad_ref, hidden_ref, part_ref, far_ref, comb_ref,
    near_ref, back_ref, ret_ref, saved_ref, merged_ref, temp_ref, slow_ref, wboth_ref, wd_ref, wo_ref, both_ref,
    down_ref, mix_ref, acc_ref, local_ref, keep_ref, pair_ref, pair_got, x_ref, x_far_ref, x_comb_ref, x_near_ref, z_ref, z_got,
    own_ref, lead_ref, plane_ref, plane_got, line_got,
    load_sem, store_sem, send_sem, recv_sem, y_send, y_recv, f_send, f_recv, far_send, far_recv,
    near_send, near_recv, ret_send, ret_recv, mix_send, mix_recv, pair_send, pair_recv,
    x_send, x_recv, z_send, z_recv, plane_send, plane_recv, line_send, line_recv,
):
    sp, tp, z, x, c = place()
    n_tp, n_sp = part_ref.shape[0], part_ref.shape[1]
    tokens, width = d_out_ref.shape
    half = width // 2
    fe = wd_ref.shape[0]
    right, left, far = (tp + 1) % n_tp, (tp + n_tp - 1) % n_tp, (tp + 2) % n_tp
    drive_ref, prev_ref, state_ref, reset_ref, norm_ref, inp_ref = [temp_ref.at[k] for k in range(6)]

    greet(sp, tp, n_sp, n_tp)
    loads = [
        pltpu.make_async_copy(src, dst, load_sem.at[k])
        for k, (src, dst) in enumerate((
            (ids_hbm, ids_ref), (wts_hbm, wts_ref), (d_out_hbm, d_out_ref), (mixed_hbm, mixed_ref),
            (conv_hbm, conv_ref), (param_hbm, param_ref), (shift_hbm, shift_ref), (wr_hbm, wr_ref), (wi_hbm, wi_ref),
            (first_hbm, first_ref), (gate_in_hbm, gate_in_ref),
            (wg_hbm, wboth_ref.at[:, pl.ds(0, fe)]), (wu_hbm, wboth_ref.at[:, pl.ds(fe, fe)]),
            (wd_hbm, wd_ref), (wo_hbm, wo_ref),
        ))
    ]
    for load in loads:
        load.start()
    for load in loads[:4]:
        load.wait()
    pack(ids_ref, wts_ref, d_out_ref, mixed_ref, send_ref, code_ref)
    got_ref[tp, sp] = send_ref[sp]
    for load in loads[4:11]:
        load.wait()
    gates(
        conv_ref, param_ref, slow_ref, shift_ref, wr_ref, wi_ref, saved_ref, drive_ref, reset_ref, norm_ref, inp_ref
    )
    run_forward(first_ref, saved_ref, drive_ref, prev_ref, state_ref)
    factors(
        conv_ref, gate_in_ref, slow_ref, saved_ref, merged_ref, prev_ref, state_ref, reset_ref, norm_ref, inp_ref
    )
    all_here(n_sp, n_tp)

    x_order = (0, 1, 3, 2)
    for dx in x_order:
        for dc in (0, 1):
            if dx or dc:
                to = z * 8 + ((x + dx) % 4) * 2 + (c + dc) % 2
                remote(send_ref.at[to], got_ref.at[tp, sp], send_sem, recv_sem.at[0, dx], to, tp).start()

    def send_group(i, _):
        for dx in x_order:
            for dc in (0, 1):
                to = offset_device(z, x, c, z_offset(i), 2 * dx + dc)
                remote(send_ref.at[to], got_ref.at[tp, sp], send_sem, recv_sem.at[i, dx], to, tp).start()
        return 0

    def source_group(i):
        return (z + 8 - z_offset(i)) % 8

    def gather_pair(i, dx):
        at = source_group(i) * 8 + ((x + 4 - dx) % 4) * 2
        wait_bytes(got_ref.at[tp, pl.ds(at, 1 if isinstance(i, int) and i + dx == 0 else 2)], recv_sem.at[i, dx])
        block = got_ref.at[tp, pl.ds(at, 2)]
        remote(block, block, y_send.at[0], y_recv.at[0, i], sp, right).start()
        remote(block, block, y_send.at[1], y_recv.at[1, i], sp, left).start()

    def gather(i):
        @pl.when(i > 1)
        def _():
            gather_pair(i, 0)

        for dx in x_order[1:]:
            gather_pair(i, dx)

    def relay(i):
        at = source_group(i) * 8
        wait_bytes(got_ref.at[left, pl.ds(at, 8)], y_recv.at[0, i])
        block = got_ref.at[left, pl.ds(at, 4)]
        remote(block, block, f_send.at[0], f_recv.at[0, i], sp, right).start()
        wait_bytes(got_ref.at[right, pl.ds(at, 8)], y_recv.at[1, i])
        block = got_ref.at[right, pl.ds(at + 4, 4)]
        remote(block, block, f_send.at[1], f_recv.at[1, i], sp, left).start()

    def compute(i):
        group = source_group(i)
        at, row = group * 8, pl.multiple_of(group * 96, 32)
        wait_bytes(got_ref.at[far, pl.ds(at, 4)], f_recv.at[0, i])
        wait_bytes(got_ref.at[far, pl.ds(at + 4, 4)], f_recv.at[1, i])
        for q in range(n_tp):
            unpack(got_ref, q, at, row, rows_ref, cot_ref)
        expert_terms(row, rows_ref, cot_ref, grad_ref, hidden_ref, wboth_ref, wd_ref)
        for q in range(n_tp):
            row_part(q, at, row, grad_ref, wboth_ref, part_ref)

    def reduce(i):
        at = source_group(i) * 8
        lower, upper = pl.ds(at, 4), pl.ds(at + 4, 4)
        remote(part_ref.at[far, lower], far_ref.at[0, i], far_send.at[0], far_recv.at[0, i], sp, left).start()
        remote(part_ref.at[far, upper], far_ref.at[1, i], far_send.at[1], far_recv.at[1, i], sp, right).start()
        remote(
            part_ref.at[left, upper], near_ref.at[0, i, pl.ds(4, 4)], near_send.at[0], near_recv.at[0, i], sp, left
        ).start()
        remote(
            part_ref.at[right, lower], near_ref.at[1, i, pl.ds(0, 4)], near_send.at[1], near_recv.at[1, i], sp, right
        ).start()

    def add_far(i):
        at = source_group(i) * 8
        for side, (to, first) in enumerate(((left, 0), (right, 4))):
            wait_bytes(far_ref.at[side, i], far_recv.at[side, i])
            own = part_ref[to, pl.ds(at + first, 4)].astype(F32)
            comb_ref[side, i] = (own + far_ref[side, i].astype(F32)).astype(BF16)
            remote(
                comb_ref.at[side, i], near_ref.at[side, i, pl.ds(first, 4)],
                near_send.at[side], near_recv.at[side, i], sp, to,
            ).start()

    def give_back(i):
        group = source_group(i)
        at = group * 8
        wait_bytes(near_ref.at[0, i], near_recv.at[0, i])
        wait_bytes(near_ref.at[1, i], near_recv.at[1, i])
        total = part_ref[tp, pl.ds(at, 8)].astype(F32) + near_ref[0, i].astype(F32) + near_ref[1, i].astype(F32)
        back_ref[pl.ds(at, 8)] = total.astype(BF16)

        def send(j, _):
            to = group * 8 + ((x + j // 2) % 4) * 2 + (c + j % 2) % 2
            remote(back_ref.at[to], ret_ref.at[sp], ret_send, ret_recv, to, tp).start()
            return 0

        lax.fori_loop(jnp.where(i == 0, 1, 0), 8, send, 0)

    gather_pair(0, 0)
    lax.fori_loop(1, GROUPS, send_group, 0)
    gather_pair(0, 1)
    gather_pair(0, 3)
    gather_pair(1, 0)
    gather_pair(0, 2)

    stages = (
        (compute, 4, 0, 8), (add_far, 6, 0, 8), (give_back, 7, 0, 8), (reduce, 4, 0, 8), (gather, 0, 1, 7),
        (relay, 0, 0, 8),
    )

    def step(s, _):
        for stage, begin, group, count in stages:
            if stage is compute:

                @pl.when(s == begin)
                def _():
                    for load in loads[11:14]:
                        load.wait()

            @pl.when(jnp.logical_and(s >= begin, s < begin + count))
            def _():
                number = s - begin + group
                stage(number if stage in (gather, relay) else work_order(number))

        return 0

    lax.fori_loop(0, GROUPS + 7, step, 0)

    over_rows = ((0,), (0,))

    def weight_grads(k, _):
        cols = pl.ds(pl.multiple_of(k * 512, 512), 512)
        both_ref[cols, :] = dot(rows_ref[:, cols], grad_ref[...], over_rows).astype(BF16)
        down_ref[:, cols] = dot(hidden_ref[...], cot_ref[:, cols], over_rows).astype(BF16)
        return 0

    lax.fori_loop(0, rows_ref.shape[1] // 512, weight_grads, 0)
    stores = [
        pltpu.make_async_copy(both_ref, both_hbm, store_sem.at[0]),
        pltpu.make_async_copy(down_ref, down_hbm, store_sem.at[1]),
        pltpu.make_async_copy(gate_ref, gate_hbm, store_sem.at[2]),
        pltpu.make_async_copy(rec_ref, rec_hbm, store_sem.at[3]),
        pltpu.make_async_copy(proj_ref, proj_hbm, store_sem.at[4]),
    ]
    for store in stores[:2]:
        store.start()

    (main, tail), low = slot_tests(code_ref[...], n_sp)
    main_pick = jnp.where(main[0] | main[1], 1.0, 0.0).astype(BF16)
    in_tail = tail[0] | tail[1]
    low_pick = jnp.where(in_tail & low, 1.0, 0.0).astype(BF16)
    high_pick = jnp.where(in_tail & ~low, 1.0, 0.0).astype(BF16)
    ret_ref[sp] = back_ref[sp]
    wait_bytes(ret_ref.at[pl.ds(0, n_sp - 1)], ret_recv)
    main_rows = ret_ref[:, :, :width].astype(F32).reshape(n_sp * 8, width).astype(BF16)
    tail_rows = ret_ref[:, :, width:].astype(F32).reshape(n_sp * 8, half).astype(BF16)
    summed = dot(main_pick, main_rows, over_rows) + jnp.concatenate(
        [dot(low_pick, tail_rows, over_rows), dot(high_pick, tail_rows, over_rows)], axis=1
    )
    mixed_rows = (d_out_ref[...].astype(F32) + summed).astype(BF16)
    for h in (0, 1):
        mix_ref[tp, h] = mixed_rows[:, h * half : (h + 1) * half]
    for order in (0, 1):
        for side, to in enumerate((right, left)):
            piece = mix_ref.at[tp, (order + side) % 2]
            remote(piece, piece, mix_send.at[side], mix_recv.at[side, order], sp, to).start()
    loads[14].wait()

    blocks = (tp, left, right, far)
    x_right, x_left, x_far = (x + 1) % 4, (x + 3) % 4, (x + 2) % 4
    part_rows = half // 8
    cut = part_rows // 2

    def along(x_to, z_to=z):
        return z_to * 8 + x_to * 2 + c

    def products(n, h):
        q, slot = blocks[n], 2 * n + h
        part = mix_ref[q, h]
        columns = pl.ds(pl.multiple_of(q * width + h * half, half), half)
        block = dot(part, wo_ref[:, columns], ((1,), (1,)))
        if slot == 0:
            acc_ref[...] = block
        else:
            acc_ref[...] += block
        grad = dot(part, merged_ref[...], over_rows).reshape(4, 2, part_rows, width)
        keep_ref[slot] = jnp.where(c == 0, grad[:, 0], grad[:, 1])
        pair_ref[slot] = jnp.where(c == 0, grad[:, 1], grad[:, 0]).astype(BF16)
        remote(
            pair_ref.at[slot], pair_got.at[slot], pair_send, pair_recv.at[slot], sp + 1 - 2 * c, tp
        ).start()

    def x_start(*slots):
        for slot in slots:
            wait_bytes(pair_got.at[slot], pair_recv.at[slot])
            total = keep_ref[slot] + pair_got[slot].astype(F32)
            keep_ref[slot] = total
            x_ref[slot] = total.astype(BF16)
            lower, upper = pl.ds(0, cut), pl.ds(cut, cut)
            for block, rows, ref, side, at, to in (
                (x_far, lower, x_far_ref, 0, None, x_left),
                (x_far, upper, x_far_ref, 1, None, x_right),
                (x_left, upper, x_near_ref, 0, upper, x_left),
                (x_right, lower, x_near_ref, 1, lower, x_right),
            ):
                goal = ref.at[slot, side] if at is None else ref.at[slot, side, at]
                send, recv = (x_send.at[0], x_recv.at[0, slot, side]) if at is None else (x_send.at[1], x_recv.at[1, slot, side])
                remote(x_ref.at[slot, block, rows], goal, send, recv, along(to), tp).start()

    def x_relay(*slots):
        for slot in slots:
            for side, to, first in ((0, x_left, 0), (1, x_right, cut)):
                wait_bytes(x_far_ref.at[slot, side], x_recv.at[0, slot, side])
                own = keep_ref[slot, to, first : first + cut]
                x_comb_ref[slot, side] = (own + x_far_ref[slot, side].astype(F32)).astype(BF16)
                remote(
                    x_comb_ref.at[slot, side], x_near_ref.at[slot, side, pl.ds(first, cut)],
                    x_send.at[1], x_recv.at[1, slot, side], along(to), tp,
                ).start()

    def z_start(*slots):
        for slot in slots:
            total = keep_ref[slot, x]
            for side in (0, 1):
                wait_bytes(x_near_ref.at[slot, side], x_recv.at[1, slot, side])
                total = total + x_near_ref[slot, side].astype(F32)
            z_ref[slot] = total.astype(BF16)
            to = 2 * blocks[slot // 2] + slot % 2

            @pl.when(to == z)
            def _():
                own_ref[...] = total

            @pl.when(to != z)
            def _():
                remote(z_ref.at[slot], z_got.at[z], z_send, z_recv, along(x, to), tp).start()

    def mix_arrived(side, order):
        q, h = (left, right)[side], (order + side) % 2
        wait_bytes(mix_ref.at[q, h], mix_recv.at[side, order])
        if order == 0:
            piece = mix_ref.at[q, h]
            remote(piece, piece, mix_send.at[2 + side], mix_recv.at[2, side], sp, (right, left)[side]).start()

    products(0, 0)
    products(0, 1)
    x_start(0, 1)
    mix_arrived(0, 0)
    mix_arrived(1, 0)
    products(1, 0)
    products(2, 1)
    x_relay(0, 1)
    x_start(2, 5)
    mix_arrived(0, 1)
    mix_arrived(1, 1)
    products(1, 1)
    products(2, 0)
    x_start(3, 4)
    for h in (0, 1):
        wait_bytes(mix_ref.at[far, h], mix_recv.at[2, h])
        products(3, h)

    d_merged = acc_ref[...]
    gate_ref[...] = (d_merged * saved_ref[5]).astype(BF16)
    stores[2].start()
    acc_ref[...] = d_merged * saved_ref[6]

    def back(group, carry):
        for i in range(8):
            t = pl.ds(tokens - 1 - (group * 8 + i), 1)
            grad = acc_ref[t, :] + carry
            local_ref[t, :] = grad
            carry = grad * saved_ref[0, t, :]
        return carry

    lead = lax.fori_loop(0, tokens // 8, back, jnp.zeros((1, width), F32))
    lead_ref[0, 0:1, :] = saved_ref[1, 0:1, :] * saved_ref[0, 0:1, :]
    lead_ref[0, 1:2, :] = lead
    own_at = sp % 8
    plane_got[own_at] = lead_ref[0]
    for dx in (2, 1, 3, 0):
        for dc in (1, 0):
            if dx or dc:
                to = z * 8 + ((x + dx) % 4) * 2 + (c + dc) % 2
                remote(lead_ref.at[0], plane_got.at[own_at], plane_send, plane_recv, to, tp).start()
    x_relay(2, 5)
    x_start(6, 7)
    z_start(0, 1)
    x_relay(3, 4)

    wait_bytes(plane_got.at[pl.ds(0, 7)], plane_recv)
    prod, carry = jnp.ones((1, width), F32), jnp.zeros((1, width), F32)
    own_prod, own_carry = prod, carry
    for k in range(7, -1, -1):
        own_prod, own_carry = jnp.where(k == own_at, prod, own_prod), jnp.where(k == own_at, carry, own_carry)
        pair = plane_got[k]
        carry = pair[1:2, :] + pair[0:1, :] * carry
        prod = pair[0:1, :] * prod
    plane_ref[0, 0:1, :] = prod
    plane_ref[0, 1:2, :] = carry
    line_got[z] = plane_ref[0]
    for dz in (4, 3, 5, 2, 6, 1, 7):
        remote(plane_ref.at[0], line_got.at[z], line_send, line_recv, along(x, (z + dz) % 8), tp).start()
    z_start(2, 5)
    x_relay(6, 7)
    z_start(3, 4, 6, 7)

    wait_bytes(line_got.at[pl.ds(0, 7)], line_recv)
    carry = jnp.zeros((1, width), F32)
    for k in range(7, 0, -1):
        pair = line_got[k]
        carry = jnp.where(k > z, pair[1:2, :] + pair[0:1, :] * carry, carry)
    incoming = own_carry + own_prod * carry
    heads, hd = wr_ref.shape[0], wr_ref.shape[1]
    for h in range(heads):
        cols = slice(h * hd, (h + 1) * hd)
        grad = local_ref[:, cols] + saved_ref[1, :, cols] * incoming[:, cols]
        by_reset = (grad * saved_ref[2, :, cols]).astype(BF16)
        by_input = (grad * saved_ref[3, :, cols]).astype(BF16)
        rec_ref[:, cols] = (
            grad * saved_ref[4, :, cols]
            + dot(by_reset, wr_ref[h], ((1,), (1,)))
            + dot(by_input, wi_ref[h], ((1,), (1,)))
        ).astype(BF16)

    stores[3].start()
    wait_bytes(z_got.at[pl.ds(0, 7)], z_recv)
    total = own_ref[...]
    for d in range(1, 8):
        total = total + z_got[(z + d) % 8].astype(F32)
    proj_ref[...] = total
    stores[4].start()

    wait_bytes(send_ref.at[pl.ds(0, n_sp - 1)], send_sem)
    for side in (0, 1):
        wait_bytes(got_ref.at[tp], y_send.at[side])
        wait_bytes(got_ref.at[tp, pl.ds(0, n_sp // 2)], f_send.at[side])
        wait_bytes(part_ref.at[tp, pl.ds(0, n_sp // 2)], far_send.at[side])
        wait_bytes(part_ref.at[tp], near_send.at[side])
        wait_bytes(mix_ref.at[tp], mix_send.at[side])
        wait_bytes(mix_ref.at[tp, 0], mix_send.at[2 + side])
    wait_bytes(back_ref.at[pl.ds(0, n_sp - 1)], ret_send)
    wait_bytes(pair_ref, pair_send)
    wait_bytes(x_far_ref, x_send.at[0])
    wait_bytes(x_near_ref, x_send.at[1])
    wait_bytes(z_ref.at[pl.ds(0, 7)], z_send)
    wait_bytes(plane_got.at[pl.ds(0, 7)], plane_send)
    wait_bytes(line_got.at[pl.ds(0, 7)], line_send)
    for store in stores:
        store.wait()


def whole_step(n_sp, n_tp, *args):
    conv, w_gate = args[0], args[12]
    tokens, width = conv.shape
    model, fe = w_gate.shape
    packed = width + width // 2
    rows = n_sp * 12
    block = (model // n_sp, width)
    dma = pltpu.SemaphoreType.DMA
    inner = (0, 1, 2, 3, 4, 5, 6, 8, 9, 10, 11)
    return pl.pallas_call(
        step_kernel,
        out_shape=(
            jax.ShapeDtypeStruct((model, 2 * fe), BF16),
            jax.ShapeDtypeStruct((fe, model), BF16),
            jax.ShapeDtypeStruct(block, F32),
            jax.ShapeDtypeStruct((tokens, width), BF16),
            jax.ShapeDtypeStruct((tokens, width), BF16),
        ),
        in_specs=[ANY] * 15,
        out_specs=(ANY,) * 5,
        scratch_shapes=[
            *(pltpu.VMEM(args[k].shape, args[k].dtype) for k in inner),
            pltpu.VMEM(block, F32),
            pltpu.VMEM((tokens, width), BF16),
            pltpu.VMEM((tokens, width), BF16),
            pltpu.VMEM((n_sp, 16, packed), BF16),
            pltpu.VMEM((2, tokens), jnp.int32),
            pltpu.VMEM((n_tp, n_sp, 16, packed), BF16),
            pltpu.VMEM((rows, model), BF16),
            pltpu.VMEM((rows, model), BF16),
            pltpu.VMEM((rows, 2 * fe), BF16),
            pltpu.VMEM((rows, fe), BF16),
            pltpu.VMEM((n_tp, n_sp, 8, packed), BF16),
            pltpu.VMEM((2, GROUPS, 4, 8, packed), BF16),
            pltpu.VMEM((2, GROUPS, 4, 8, packed), BF16),
            pltpu.VMEM((2, GROUPS, 8, 8, packed), BF16),
            pltpu.VMEM((n_sp, 8, packed), BF16),
            pltpu.VMEM((n_sp, 8, packed), BF16),
            pltpu.VMEM((7, tokens, width), F32),
            pltpu.VMEM((tokens, width), BF16),
            pltpu.VMEM((6, tokens, width), F32),
            pltpu.VMEM((1, width), F32),
            pltpu.VMEM((model, 2 * fe), BF16),
            pltpu.VMEM((fe, model), BF16),
            pltpu.VMEM((width, model), BF16),
            pltpu.VMEM((model, 2 * fe), BF16),
            pltpu.VMEM((fe, model), BF16),
            pltpu.VMEM((n_tp, 2, tokens, width // 2), BF16),
            pltpu.VMEM((tokens, width), F32),
            pltpu.VMEM((tokens, width), F32),
            pltpu.VMEM((8, 4, *block), F32),
            pltpu.VMEM((8, 4, *block), BF16),
            pltpu.VMEM((8, 4, *block), BF16),
            pltpu.VMEM((8, 4, *block), BF16),
            pltpu.VMEM((8, 2, block[0] // 2, width), BF16),
            pltpu.VMEM((8, 2, block[0] // 2, width), BF16),
            pltpu.VMEM((8, 2, *block), BF16),
            pltpu.VMEM((8, *block), BF16),
            pltpu.VMEM((8, *block), BF16),
            pltpu.VMEM(block, F32),
            pltpu.VMEM((1, 2, width), F32),
            pltpu.VMEM((1, 2, width), F32),
            pltpu.VMEM((8, 2, width), F32),
            pltpu.VMEM((8, 2, width), F32),
            dma((15,)), dma((5,)), dma, dma((8, 4)), dma((2,)), dma((2, 8)), dma((2,)), dma((2, 8)),
            dma((2,)), dma((2, 8)), dma((2,)), dma((2, 8)), dma, dma, dma((4,)), dma((3, 2)),
            dma, dma((8,)), dma((2,)), dma((2, 8, 2)), dma, dma, dma, dma, dma, dma,
        ],
        compiler_params=pltpu.CompilerParams(
            collective_id=0, has_side_effects=True, vmem_limit_bytes=63 * 2**20
        ),
        name="whole_step",
    )(*args)


def write_kernel(both_ref, down_ref, proj_ref, rec_ref, gate_ref, gg_ref, gu_ref, gd_ref, p_ref, r_ref, g_ref):
    fe = gg_ref.shape[1]
    gg_ref[...] = both_ref[:, :fe].astype(F32)
    gu_ref[...] = both_ref[:, fe:].astype(F32)
    gd_ref[...] = down_ref[...].astype(F32)
    p_ref[...] = proj_ref[...]
    r_ref[...] = rec_ref[...]
    g_ref[...] = gate_ref[...]


def write_out(both, down, proj, rec, gate, parts=2):
    model, fe = both.shape[0], both.shape[1] // 2

    def cut(array):
        return pl.BlockSpec((array.shape[0] // parts, array.shape[1]), lambda i: (i, 0))

    outs = (
        jax.ShapeDtypeStruct((model, fe), F32),
        jax.ShapeDtypeStruct((model, fe), F32),
        jax.ShapeDtypeStruct((fe, model), F32),
        jax.ShapeDtypeStruct(proj.shape, proj.dtype),
        jax.ShapeDtypeStruct(rec.shape, rec.dtype),
        jax.ShapeDtypeStruct(gate.shape, gate.dtype),
    )
    ins = (both, down, proj, rec, gate)
    return pl.pallas_call(
        write_kernel,
        grid=(parts,),
        out_shape=outs,
        in_specs=[cut(a) for a in ins],
        out_specs=tuple(cut(a) for a in outs),
        name="write_out",
    )(*ins)


def body(
    n_sp, n_tp, conv_out, gate_in, block_states, decay_param, decay_shift, w_reset, w_input, w_out,
    mixed, d_out, expert_ids, route_weights, w_gate, w_up, w_down,
):
    both, down, proj, rec, gate = whole_step(
        n_sp, n_tp, conv_out, gate_in, block_states, decay_param[None, :], decay_shift[None, :], w_reset, w_input, w_out,
        mixed, d_out, expert_ids.T, route_weights.T, w_gate[0], w_up[0], w_down[0],
    )
    gg, gu, gd, proj, rec, gate = write_out(both, down, proj, rec, gate)
    return gg[None], gu[None], gd[None], proj, rec, gate


def solution(mesh):
    in_specs = (
        P("sp", "tp"), P("sp", "tp"), P("sp", "tp"), P("tp"), P("sp"),
        P("tp", None, None), P("tp", None, None), P("tp", None),
        P("sp", "tp"), P("sp", "tp"), P("sp", None), P("sp", None),
        P("sp", None, "tp"), P("sp", None, "tp"), P("sp", "tp", None),
    )
    out_specs = (
        P("sp", None, "tp"), P("sp", None, "tp"), P("sp", "tp", None),
        P("sp", "tp"), P("sp", "tp"), P("sp", "tp"),
    )
    run = functools.partial(body, mesh.shape["sp"], mesh.shape["tp"])
    return jax.shard_map(run, mesh=mesh, in_specs=in_specs, out_specs=out_specs, check_vma=False)
```

```python
import functools

import jax
import jax.numpy as jnp
from jax import lax
from jax.experimental import pallas as pl
from jax.experimental.pallas import tpu as pltpu
from jax.sharding import PartitionSpec as P

F32 = jnp.float32
BF16 = jnp.bfloat16
MESH = pl.DeviceIdType.MESH
VM = pl.BlockSpec(memory_space=pltpu.VMEM)
ANY = pl.BlockSpec(memory_space=pl.ANY)


def dot(a, b, dims=((1,), (0,))):
    return lax.dot_general(a, b, (dims, ((), ())), preferred_element_type=F32)


def swap4(value):
    return pltpu.roll(value, 4, axis=1)


def low_half(shape):
    return lax.broadcasted_iota(jnp.int32, shape, 1) < 4


def gates(conv_ref, param_ref, slow_ref, shift_ref, wr_ref, wi_ref, saved_ref, drive_ref, reset_ref, norm_ref, inp_ref):
    hd = wr_ref.shape[1]
    rows = conv_ref.shape[0]
    shift = jnp.transpose(jnp.broadcast_to(shift_ref[...], (8, rows)))[:, 0:1]
    param = param_ref[...]
    slow_ref[...] = jnp.maximum(-param, 0.0) + jnp.log1p(jnp.exp(-jnp.abs(param)))
    for h in range(wr_ref.shape[0]):
        cols = slice(h * hd, (h + 1) * hd)
        conv = conv_ref[:, cols]
        reset = jax.nn.sigmoid(dot(conv, wr_ref[h]))
        inp = jax.nn.sigmoid(dot(conv, wi_ref[h]))
        log_decay = -8.0 * reset * slow_ref[:, cols] + shift
        decay = jnp.exp(log_decay)
        twice = 2.0 * log_decay
        small = jnp.maximum(twice, -0.5)
        series = 1.0 + small * (1.0 / 10.0)
        for n in (9, 8, 7, 6, 5, 4, 3, 2):
            series = 1.0 + small * (1.0 / n) * series
        less = jnp.where(twice > -0.5, small * series, jnp.exp(twice) - 1.0)
        norm = jnp.sqrt(-less)
        saved_ref[0, :, cols] = decay
        reset_ref[:, cols] = reset
        norm_ref[:, cols] = norm
        inp_ref[:, cols] = inp
        drive_ref[:, cols] = norm * inp * conv.astype(F32)


def run_forward(first_ref, saved_ref, drive_ref, prev_ref, state_ref):
    rows, width = drive_ref.shape

    def step(group, state):
        for i in range(8):
            t = pl.ds(group * 8 + i, 1)
            prev_ref[t, :] = state
            state = saved_ref[0, t, :] * state + drive_ref[t, :]
            state_ref[t, :] = state
        return state

    lax.fori_loop(0, rows // 8, step, first_ref[...])

    def back(group, prod):
        for i in range(8):
            t = rows - 1 - (group * 8 + i)
            saved_ref[1, pl.ds(t, 1), :] = prod
            prod = prod * saved_ref[0, pl.ds(t, 1), :]
        return prod

    lax.fori_loop(0, rows // 8, back, jnp.ones((1, width), F32))


def factors(
    conv_ref, gate_ref, slow_ref, saved_ref, merged_ref, prev_ref, state_ref, reset_ref, norm_ref, inp_ref
):
    hd = 128
    for h in range(conv_ref.shape[1] // hd):
        cols = slice(h * hd, (h + 1) * hd)
        conv = conv_ref[:, cols].astype(F32)
        decay, reset, norm, inp = saved_ref[0, :, cols], reset_ref[:, cols], norm_ref[:, cols], inp_ref[:, cols]
        by_log = decay * prev_ref[:, cols] - inp * conv * decay * decay / norm
        saved_ref[2, :, cols] = by_log * (-8.0 * slow_ref[:, cols]) * reset * (1.0 - reset)
        saved_ref[3, :, cols] = norm * conv * inp * (1.0 - inp)
        saved_ref[4, :, cols] = norm * inp
        state = state_ref[:, cols]
        value = gate_ref[:, cols].astype(F32)
        k = 0.7978845608028654
        square = value * value
        bent = jnp.tanh(k * (value + 0.044715 * value * square))
        act = 0.5 * value * (1.0 + bent)
        slope = 0.5 * (1.0 + bent) + 0.5 * value * (1.0 - bent * bent) * k * (1.0 + 3.0 * 0.044715 * square)
        saved_ref[5, :, cols] = state * slope
        saved_ref[6, :, cols] = act
        merged_ref[:, cols] = (act * state).astype(BF16)


def slot_tests(codes, experts, first=0):
    tokens = codes.shape[1]
    row = lax.broadcasted_iota(jnp.int32, (experts * 8, tokens), 0)
    base = (row // 8 + first) * 16
    main = base + row % 8
    tail = base + 8 + row % 4
    return [[codes[k : k + 1, :] == want for k in (0, 1)] for want in (main, tail)], row % 8 < 4


def rank_codes(ids_ref, code_ref, experts):
    tokens = ids_ref.shape[1]
    each = lax.broadcasted_iota(jnp.int32, (experts, tokens), 0)
    named = [ids_ref[k : k + 1, :] == each for k in (0, 1)]
    both = jnp.where(named[0] | named[1], 1.0, 0.0).astype(BF16)
    earlier = (
        lax.broadcasted_iota(jnp.int32, (tokens, tokens), 0)
        < lax.broadcasted_iota(jnp.int32, (tokens, tokens), 1)
    )
    count = dot(both, jnp.where(earlier, 1.0, 0.0).astype(BF16))
    for k in (0, 1):
        rank = jnp.sum(jnp.where(named[k], count, 0.0), axis=0, keepdims=True)
        code_ref[k : k + 1, :] = ids_ref[k : k + 1, :] * 16 + rank.astype(jnp.int32)


def pack(code_ref, wts_ref, raw_ref, columns, experts, first, store):
    width = raw_ref.shape[3]
    half = width // 2
    (main, tail), low = slot_tests(code_ref[...], experts, first)

    def weight(tests):
        return jnp.sum(
            jnp.where(tests[0], wts_ref[0:1, :], 0.0) + jnp.where(tests[1], wts_ref[1:2, :], 0.0),
            axis=1,
            keepdims=True,
        )

    main_pick = jnp.where(main[0] | main[1], 1.0, 0.0).astype(BF16)
    in_tail = tail[0] | tail[1]
    low_pick = jnp.where(in_tail & low, 1.0, 0.0).astype(BF16)
    high_pick = jnp.where(in_tail & ~low, 1.0, 0.0).astype(BF16)
    weights = (weight(main), weight(tail))
    for q in columns:
        for at in (0, 1):
            rows = raw_ref[at, q]
            block = dot(main_pick, rows)
            ends = dot(low_pick, rows[:, :half]) + dot(high_pick, rows[:, half:])
            if at == 0:
                block, ends = block * weights[0], ends * weights[1]
            both = jnp.concatenate(
                [block.reshape(experts, 8, width), ends.reshape(experts, 8, half)], axis=2
            ).astype(BF16)
            store(q, slice(at * 8, at * 8 + 8), both)


def place():
    sp, tp = lax.axis_index("sp"), lax.axis_index("tp")
    return sp, tp, sp // 8, (sp // 2) % 4, sp % 2


Z_ORDER = (2, 6, 3, 4, 5, 1, 7, 0)
FAR_GROUPS = 5
PLAN = (
    1, 8, 9, 2, 17, 3, 16, 24, 11, 32, 10, 4, 40, 18,
    26, 12, 34, 19, 25, 27, 20, 42, 33, 28, 23, 35, 22, 41,
    30, 21, 36, 29, 31, 43, 44, 38, 37, 39, 46, 45, 47,
)


def z_offset(i):
    return sum(jnp.where(i == k, dz, 0) for k, dz in enumerate(Z_ORDER))


def offset_device(z, x, c, dz, j):
    return ((z + dz) % 8) * 8 + ((x + j // 2) % 4) * 2 + (c + j % 2) % 2


def greet(sp, tp, n_sp, n_tp):
    barrier = pltpu.get_barrier_semaphore()

    def to_sp(k, _):
        to = (sp + n_sp // 2 + k) % n_sp
        pl.semaphore_signal(barrier, inc=1, device_id=(to, tp), device_id_type=MESH)
        return 0

    lax.fori_loop(0, n_sp // 2, to_sp, 0)
    lax.fori_loop(1 - n_sp // 2, 0, to_sp, 0)
    for k in range(1, n_tp):
        pl.semaphore_signal(barrier, inc=1, device_id=(sp, (tp + k) % n_tp), device_id_type=MESH)


def all_here(n_sp, n_tp):
    pl.semaphore_wait(pltpu.get_barrier_semaphore(), n_sp - 1 + n_tp - 1)


def remote(src, dst, send_sem, recv_sem, sp, tp):
    return pltpu.make_async_remote_copy(
        src_ref=src, dst_ref=dst, send_sem=send_sem, recv_sem=recv_sem,
        device_id=(sp, tp), device_id_type=MESH,
    )


def wait_bytes(ref, sem):
    pltpu.make_async_copy(ref, ref, sem).wait()


def unpack(got_ref, q, at, row, rows_ref, cot_ref):
    packed = got_ref.shape[3]
    width, half = packed * 2 // 3, packed // 3
    cols = slice(q * width, (q + 1) * width)
    for first, ref in ((0, cot_ref), (8, rows_ref)):
        block = got_ref[q, pl.ds(at, 8), first : first + 8, :].astype(F32)
        ref[pl.ds(row, 64), cols] = block[:, :, :width].reshape(64, width).astype(BF16)
        tails = block[:, :, width:]
        turned = swap4(tails)
        tails, turned = tails.reshape(4, 2, 8, half), turned.reshape(4, 2, 8, half)
        low = low_half((4, 8, half))
        left = jnp.where(low, tails[:, 0], turned[:, 1])
        right = jnp.where(low, turned[:, 0], tails[:, 1])
        both = jnp.concatenate([left, right], axis=2).reshape(32, width)
        ref[pl.ds(row + 64, 32), cols] = both.astype(BF16)


def expert_terms(row, rows_ref, cot_ref, grad_ref, hidden_ref, wboth_ref, wd_ref):
    fe = wd_ref.shape[0]
    rows = pl.ds(row, 96)
    both = dot(rows_ref[rows, :], wboth_ref[...])
    up_pre, linear = both[:, :fe], both[:, fe:]
    d_hidden = dot(cot_ref[rows, :], wd_ref[...], ((1,), (1,)))
    gate = jax.nn.sigmoid(up_pre)
    silu = up_pre * gate
    hidden_ref[rows, :] = (silu * linear).astype(BF16)
    d_linear = (d_hidden * silu).astype(BF16)
    d_up = (d_hidden * linear * gate * (1.0 + up_pre * (1.0 - gate))).astype(BF16)
    grad_ref[rows, :fe] = d_up
    grad_ref[rows, fe:] = d_linear


def row_part(q, at, row, grad_ref, wboth_ref, part_ref):
    packed = part_ref.shape[3]
    width, half = packed * 2 // 3, packed // 3
    part = dot(grad_ref[pl.ds(row, 96), :], wboth_ref[pl.ds(pl.multiple_of(q * width, width), width), :], ((1,), (1,)))
    part_ref[q, pl.ds(at, 8), :, :width] = part[:64].reshape(8, 8, width).astype(BF16)
    tails = part[64:].reshape(4, 8, width)
    left, right = tails[:, :, :half], tails[:, :, half:]
    low = low_half((4, 8, half))
    one = jnp.where(low, left, swap4(right))
    two = jnp.where(low, swap4(left), right)
    part_ref[q, pl.ds(at, 8), :, width:] = jnp.stack([one, two], axis=1).reshape(8, 8, half).astype(BF16)


GROUPS = 8


def step_kernel(
    conv_hbm, gate_in_hbm, first_hbm, param_hbm, shift_hbm, wr_hbm, wi_hbm, wo_hbm, mixed_hbm, d_out_hbm,
    ids_hbm, wts_hbm, wg_hbm, wu_hbm, wd_hbm,
    both_hbm, down_hbm, proj_hbm, rec_hbm, gate_hbm,
    conv_ref, gate_in_ref, first_ref, param_ref, shift_ref, wr_ref, wi_ref, raw_ref, near_out, ids_ref, wts_ref,
    proj_ref, rec_ref, gate_ref, send_ref, code_ref, got_ref, rows_ref, cot_ref, grad_ref, hidden_ref, part_ref, far_ref, comb_ref,
    near_ref, back_ref, ret_ref, saved_ref, merged_ref, temp_ref, slow_ref, wboth_ref, wd_ref, wo_ref, both_ref,
    down_ref, mix_ref, acc_ref, local_ref, keep_ref, pair_ref, pair_got, x_ref, x_far_ref, x_comb_ref, x_near_ref, z_ref, z_got,
    own_ref, lead_ref, plane_ref, plane_got, line_got,
    load_sem, store_sem, raw_send, raw_recv, near_g_send, send_sem, recv_sem, y_send, y_recv, f_send, f_recv, far_send, far_recv,
    near_send, near_recv, ret_send, ret_recv, mix_send, mix_recv, pair_send, pair_recv,
    x_send, x_recv, z_send, z_recv, plane_send, plane_recv, line_send, line_recv,
):
    sp, tp, z, x, c = place()
    n_tp, n_sp = part_ref.shape[0], part_ref.shape[1]
    tokens, width = raw_ref.shape[2:]
    half = width // 2
    fe = wd_ref.shape[0]
    right, left, far = (tp + 1) % n_tp, (tp + n_tp - 1) % n_tp, (tp + 2) % n_tp
    drive_ref, prev_ref, state_ref, reset_ref, norm_ref, inp_ref = [temp_ref.at[k] for k in range(6)]

    greet(sp, tp, n_sp, n_tp)
    loads = [
        pltpu.make_async_copy(src, dst, load_sem.at[k])
        for k, (src, dst) in enumerate((
            (ids_hbm, ids_ref), (wts_hbm, wts_ref), (d_out_hbm, raw_ref.at[0, tp]), (mixed_hbm, raw_ref.at[1, tp]),
            (conv_hbm, conv_ref), (param_hbm, param_ref), (shift_hbm, shift_ref), (wr_hbm, wr_ref), (wi_hbm, wi_ref),
            (first_hbm, first_ref), (gate_in_hbm, gate_in_ref),
            (wg_hbm, wboth_ref.at[:, pl.ds(0, fe)]), (wu_hbm, wboth_ref.at[:, pl.ds(fe, fe)]),
            (wd_hbm, wd_ref), (wo_hbm, wo_ref),
        ))
    ]
    for load in loads:
        load.start()
    for load in loads[:4]:
        load.wait()
    rank_codes(ids_ref, code_ref, n_sp)

    def store_all(q, rows, value):
        send_ref[:, rows, :] = value

    pack(code_ref, wts_ref, raw_ref, (tp,), n_sp, 0, store_all)
    got_ref[tp, sp] = send_ref[sp]
    all_here(n_sp, n_tp)

    sides = (right, left)
    for order in (0, 1):
        for side in (0, 1):
            piece = raw_ref.at[(order + side) % 2, tp]
            remote(piece, piece, raw_send.at[side], raw_recv.at[side, order], sp, sides[side]).start()

    def send_far(i, _):
        def send(j, _):
            to = offset_device(z, x, c, z_offset(i), j)
            remote(send_ref.at[to], got_ref.at[tp, sp], send_sem, recv_sem.at[i], to, tp).start()
            return 0

        lax.fori_loop(0, 8, send, 0)
        return 0

    def send_near(g, _):
        def send(j, _):
            to = offset_device(z, x, c, z_offset(g), j)
            remote(send_ref.at[to], got_ref.at[tp, sp], send_sem, recv_sem.at[g], to, tp).start()
            return 0

        lax.fori_loop(jnp.where(g == GROUPS - 1, 1, 0), 8, send, 0)
        return 0

    lax.fori_loop(0, 2, send_far, 0)

    def source_group(i):
        return (z + 8 - z_offset(i)) % 8

    def near_blocks(columns):
        def one(g, _):
            target = (z + z_offset(g)) % 8
            at = g - FAR_GROUPS

            def store(q, rows, value):
                near_out[at, q, :, rows, :] = value

            pack(code_ref, wts_ref, raw_ref, columns, 8, target * 8, store)

            def send(j, _):
                slot = ((x + j // 2) % 4) * 2 + (c + j % 2) % 2
                for q in columns:
                    remote(
                        near_out.at[at, q, slot], got_ref.at[q, sp], near_g_send, recv_sem.at[g], target * 8 + slot, tp
                    ).start()
                return 0

            lax.fori_loop(jnp.where(g == GROUPS - 1, 1, 0), 8, send, 0)
            return 0

        lax.fori_loop(FAR_GROUPS, GROUPS, one, 0)
        for q in columns:
            got_ref[q, sp] = near_out[GROUPS - 1 - FAR_GROUPS, q, sp % 8]

    def raw_arrived(side, order):
        piece = raw_ref.at[(order + side) % 2, (left, right)[side]]
        wait_bytes(piece, raw_recv.at[side, order])
        if order == 0:
            remote(piece, piece, raw_send.at[2 + side], raw_recv.at[2, side], sp, sides[side]).start()

    def gather(i):
        at = source_group(i) * 8
        block = got_ref.at[tp, pl.ds(at, 8)]
        wait_bytes(block, recv_sem.at[i])
        remote(block, block, y_send.at[0], y_recv.at[0, i], sp, right).start()
        remote(block, block, y_send.at[1], y_recv.at[1, i], sp, left).start()

    def relay(i):
        at = source_group(i) * 8
        wait_bytes(got_ref.at[left, pl.ds(at, 8)], y_recv.at[0, i])
        block = got_ref.at[left, pl.ds(at, 4)]
        remote(block, block, f_send.at[0], f_recv.at[0, i], sp, right).start()
        wait_bytes(got_ref.at[right, pl.ds(at, 8)], y_recv.at[1, i])
        block = got_ref.at[right, pl.ds(at + 4, 4)]
        remote(block, block, f_send.at[1], f_recv.at[1, i], sp, left).start()

    def compute(i):
        group = source_group(i)
        at, row = group * 8, pl.multiple_of(group * 96, 32)

        @pl.when(i < FAR_GROUPS)
        def _():
            wait_bytes(got_ref.at[far, pl.ds(at, 4)], f_recv.at[0, i])
            wait_bytes(got_ref.at[far, pl.ds(at + 4, 4)], f_recv.at[1, i])

        @pl.when(jnp.logical_and(i >= FAR_GROUPS, i < GROUPS - 1))
        def _():
            wait_bytes(got_ref.at[:, pl.ds(at, 8)], recv_sem.at[i])

        @pl.when(i == GROUPS - 1)
        def _():
            wait_bytes(got_ref.at[:, pl.ds(at, 7)], recv_sem.at[i])

        for q in range(n_tp):
            unpack(got_ref, q, at, row, rows_ref, cot_ref)
        expert_terms(row, rows_ref, cot_ref, grad_ref, hidden_ref, wboth_ref, wd_ref)
        for q in range(n_tp):
            row_part(q, at, row, grad_ref, wboth_ref, part_ref)

    def reduce(i):
        at = source_group(i) * 8
        lower, upper = pl.ds(at, 4), pl.ds(at + 4, 4)
        remote(part_ref.at[far, lower], far_ref.at[0, i], far_send.at[0], far_recv.at[0, i], sp, left).start()
        remote(part_ref.at[far, upper], far_ref.at[1, i], far_send.at[1], far_recv.at[1, i], sp, right).start()
        remote(
            part_ref.at[left, upper], near_ref.at[0, i, pl.ds(4, 4)], near_send.at[0], near_recv.at[0, i], sp, left
        ).start()
        remote(
            part_ref.at[right, lower], near_ref.at[1, i, pl.ds(0, 4)], near_send.at[1], near_recv.at[1, i], sp, right
        ).start()

    def add_far(i):
        at = source_group(i) * 8
        for side, (to, first) in enumerate(((left, 0), (right, 4))):
            wait_bytes(far_ref.at[side, i], far_recv.at[side, i])
            own = part_ref[to, pl.ds(at + first, 4)].astype(F32)
            comb_ref[side, i] = (own + far_ref[side, i].astype(F32)).astype(BF16)
            remote(
                comb_ref.at[side, i], near_ref.at[side, i, pl.ds(first, 4)],
                near_send.at[side], near_recv.at[side, i], sp, to,
            ).start()

    def give_back(i):
        group = source_group(i)
        at = group * 8
        wait_bytes(near_ref.at[0, i], near_recv.at[0, i])
        wait_bytes(near_ref.at[1, i], near_recv.at[1, i])
        total = part_ref[tp, pl.ds(at, 8)].astype(F32) + near_ref[0, i].astype(F32) + near_ref[1, i].astype(F32)
        back_ref[pl.ds(at, 8)] = total.astype(BF16)

        def send(j, _):
            to = group * 8 + ((x + j // 2) % 4) * 2 + (c + j % 2) % 2
            remote(back_ref.at[to], ret_ref.at[sp], ret_send, ret_recv, to, tp).start()
            return 0

        lax.fori_loop(jnp.where(i == GROUPS - 1, 1, 0), 8, send, 0)

    for load in loads[4:11]:
        load.wait()
    gates(
        conv_ref, param_ref, slow_ref, shift_ref, wr_ref, wi_ref, saved_ref, drive_ref, reset_ref, norm_ref, inp_ref
    )
    raw_arrived(0, 0)
    raw_arrived(1, 0)
    lax.fori_loop(2, 4, send_far, 0)
    run_forward(first_ref, saved_ref, drive_ref, prev_ref, state_ref)
    raw_arrived(0, 1)
    raw_arrived(1, 1)
    gather(0)
    lax.fori_loop(4, FAR_GROUPS, send_far, 0)
    near_blocks((left, right))
    lax.fori_loop(FAR_GROUPS, GROUPS, send_near, 0)
    factors(
        conv_ref, gate_in_ref, slow_ref, saved_ref, merged_ref, prev_ref, state_ref, reset_ref, norm_ref, inp_ref
    )
    for k in (0, 1):
        wait_bytes(raw_ref.at[k, far], raw_recv.at[2, k])
    near_blocks((far,))
    for load in loads[11:14]:
        load.wait()

    stages = (gather, relay, compute, reduce, add_far, give_back)

    def step(s, _):
        code = sum(jnp.where(s == k, entry, 0) for k, entry in enumerate(PLAN))
        for k, stage in enumerate(stages):

            @pl.when(code // 8 == k)
            def _():
                stage(code % 8)

        return 0

    lax.fori_loop(0, len(PLAN), step, 0)

    over_rows = ((0,), (0,))

    def weight_grads(k, _):
        cols = pl.ds(pl.multiple_of(k * 512, 512), 512)
        both_ref[cols, :] = dot(rows_ref[:, cols], grad_ref[...], over_rows).astype(BF16)
        down_ref[:, cols] = dot(hidden_ref[...], cot_ref[:, cols], over_rows).astype(BF16)
        return 0

    stores = [
        pltpu.make_async_copy(both_ref, both_hbm, store_sem.at[0]),
        pltpu.make_async_copy(down_ref, down_hbm, store_sem.at[1]),
        pltpu.make_async_copy(gate_ref, gate_hbm, store_sem.at[2]),
        pltpu.make_async_copy(rec_ref, rec_hbm, store_sem.at[3]),
        pltpu.make_async_copy(proj_ref, proj_hbm, store_sem.at[4]),
    ]
    lax.fori_loop(0, 1, weight_grads, 0)

    (main, tail), low = slot_tests(code_ref[...], n_sp)
    main_pick = jnp.where(main[0] | main[1], 1.0, 0.0).astype(BF16)
    in_tail = tail[0] | tail[1]
    low_pick = jnp.where(in_tail & low, 1.0, 0.0).astype(BF16)
    high_pick = jnp.where(in_tail & ~low, 1.0, 0.0).astype(BF16)
    ret_ref[sp] = back_ref[sp]
    wait_bytes(ret_ref.at[pl.ds(0, n_sp - 1)], ret_recv)
    main_rows = ret_ref[:, :, :width].astype(F32).reshape(n_sp * 8, width).astype(BF16)
    tail_rows = ret_ref[:, :, width:].astype(F32).reshape(n_sp * 8, half).astype(BF16)
    summed = dot(main_pick, main_rows, over_rows) + jnp.concatenate(
        [dot(low_pick, tail_rows, over_rows), dot(high_pick, tail_rows, over_rows)], axis=1
    )
    mixed_rows = (raw_ref[0, tp].astype(F32) + summed).astype(BF16)
    for h in (0, 1):
        mix_ref[tp, h] = mixed_rows[:, h * half : (h + 1) * half]
    for order in (0, 1):
        for side, to in enumerate((right, left)):
            piece = mix_ref.at[tp, (order + side) % 2]
            remote(piece, piece, mix_send.at[side], mix_recv.at[side, order], sp, to).start()
    loads[14].wait()

    blocks = (tp, left, right, far)
    x_right, x_left, x_far = (x + 1) % 4, (x + 3) % 4, (x + 2) % 4
    part_rows = half // 8
    cut = part_rows // 2

    def along(x_to, z_to=z):
        return z_to * 8 + x_to * 2 + c

    def products(n, h):
        q, slot = blocks[n], 2 * n + h
        part = mix_ref[q, h]
        columns = pl.ds(pl.multiple_of(q * width + h * half, half), half)
        block = dot(part, wo_ref[:, columns], ((1,), (1,)))
        if slot == 0:
            acc_ref[...] = block
        else:
            acc_ref[...] += block
        grad = dot(part, merged_ref[...], over_rows).reshape(4, 2, part_rows, width)
        keep_ref[slot] = jnp.where(c == 0, grad[:, 0], grad[:, 1])
        pair_ref[slot] = jnp.where(c == 0, grad[:, 1], grad[:, 0]).astype(BF16)
        remote(
            pair_ref.at[slot], pair_got.at[slot], pair_send, pair_recv.at[slot], sp + 1 - 2 * c, tp
        ).start()

    def x_start(*slots):
        for slot in slots:
            wait_bytes(pair_got.at[slot], pair_recv.at[slot])
            total = keep_ref[slot] + pair_got[slot].astype(F32)
            keep_ref[slot] = total
            x_ref[slot] = total.astype(BF16)
            lower, upper = pl.ds(0, cut), pl.ds(cut, cut)
            for block, rows, ref, side, at, to in (
                (x_far, lower, x_far_ref, 0, None, x_left),
                (x_far, upper, x_far_ref, 1, None, x_right),
                (x_left, upper, x_near_ref, 0, upper, x_left),
                (x_right, lower, x_near_ref, 1, lower, x_right),
            ):
                goal = ref.at[slot, side] if at is None else ref.at[slot, side, at]
                send, recv = (x_send.at[0], x_recv.at[0, slot, side]) if at is None else (x_send.at[1], x_recv.at[1, slot, side])
                remote(x_ref.at[slot, block, rows], goal, send, recv, along(to), tp).start()

    def x_relay(*slots):
        for slot in slots:
            for side, to, first in ((0, x_left, 0), (1, x_right, cut)):
                wait_bytes(x_far_ref.at[slot, side], x_recv.at[0, slot, side])
                own = keep_ref[slot, to, first : first + cut]
                x_comb_ref[slot, side] = (own + x_far_ref[slot, side].astype(F32)).astype(BF16)
                remote(
                    x_comb_ref.at[slot, side], x_near_ref.at[slot, side, pl.ds(first, cut)],
                    x_send.at[1], x_recv.at[1, slot, side], along(to), tp,
                ).start()

    def z_start(*slots):
        for slot in slots:
            total = keep_ref[slot, x]
            for side in (0, 1):
                wait_bytes(x_near_ref.at[slot, side], x_recv.at[1, slot, side])
                total = total + x_near_ref[slot, side].astype(F32)
            z_ref[slot] = total.astype(BF16)
            to = 2 * blocks[slot // 2] + slot % 2

            @pl.when(to == z)
            def _():
                own_ref[...] = total

            @pl.when(to != z)
            def _():
                remote(z_ref.at[slot], z_got.at[z], z_send, z_recv, along(x, to), tp).start()

    def mix_arrived(side, order):
        q, h = (left, right)[side], (order + side) % 2
        wait_bytes(mix_ref.at[q, h], mix_recv.at[side, order])
        if order == 0:
            piece = mix_ref.at[q, h]
            remote(piece, piece, mix_send.at[2 + side], mix_recv.at[2, side], sp, (right, left)[side]).start()

    products(0, 0)
    products(0, 1)
    x_start(0, 1)
    lax.fori_loop(1, 4, weight_grads, 0)
    for store in stores[:2]:
        store.start()
    mix_arrived(0, 0)
    mix_arrived(1, 0)
    products(1, 0)
    products(2, 1)
    x_relay(0, 1)
    x_start(2, 5)
    mix_arrived(0, 1)
    mix_arrived(1, 1)
    products(1, 1)
    products(2, 0)
    x_start(3, 4)
    for h in (0, 1):
        wait_bytes(mix_ref.at[far, h], mix_recv.at[2, h])
        products(3, h)

    d_merged = acc_ref[...]
    gate_ref[...] = (d_merged * saved_ref[5]).astype(BF16)
    stores[2].start()
    acc_ref[...] = d_merged * saved_ref[6]

    def back(group, carry):
        for i in range(8):
            t = pl.ds(tokens - 1 - (group * 8 + i), 1)
            grad = acc_ref[t, :] + carry
            local_ref[t, :] = grad
            carry = grad * saved_ref[0, t, :]
        return carry

    lead = lax.fori_loop(0, tokens // 8, back, jnp.zeros((1, width), F32))
    lead_ref[0, 0:1, :] = saved_ref[1, 0:1, :] * saved_ref[0, 0:1, :]
    lead_ref[0, 1:2, :] = lead
    own_at = sp % 8
    plane_got[own_at] = lead_ref[0]
    for dx in (2, 1, 3, 0):
        for dc in (1, 0):
            if dx or dc:
                to = z * 8 + ((x + dx) % 4) * 2 + (c + dc) % 2
                remote(lead_ref.at[0], plane_got.at[own_at], plane_send, plane_recv, to, tp).start()
    x_start(6, 7)
    x_relay(2, 5)
    z_start(0, 1)
    x_relay(3, 4)
    x_relay(6, 7)

    wait_bytes(plane_got.at[pl.ds(0, 7)], plane_recv)
    prod, carry = jnp.ones((1, width), F32), jnp.zeros((1, width), F32)
    own_prod, own_carry = prod, carry
    for k in range(7, -1, -1):
        own_prod, own_carry = jnp.where(k == own_at, prod, own_prod), jnp.where(k == own_at, carry, own_carry)
        pair = plane_got[k]
        carry = pair[1:2, :] + pair[0:1, :] * carry
        prod = pair[0:1, :] * prod
    plane_ref[0, 0:1, :] = prod
    plane_ref[0, 1:2, :] = carry
    line_got[z] = plane_ref[0]
    for dz in (4, 3, 5, 2, 6, 1, 7):
        remote(plane_ref.at[0], line_got.at[z], line_send, line_recv, along(x, (z + dz) % 8), tp).start()
    z_start(2, 5, 3, 4, 6, 7)

    wait_bytes(line_got.at[pl.ds(0, 7)], line_recv)
    carry = jnp.zeros((1, width), F32)
    for k in range(7, 0, -1):
        pair = line_got[k]
        carry = jnp.where(k > z, pair[1:2, :] + pair[0:1, :] * carry, carry)
    incoming = own_carry + own_prod * carry
    heads, hd = wr_ref.shape[0], wr_ref.shape[1]
    for h in range(heads):
        cols = slice(h * hd, (h + 1) * hd)
        grad = local_ref[:, cols] + saved_ref[1, :, cols] * incoming[:, cols]
        by_reset = (grad * saved_ref[2, :, cols]).astype(BF16)
        by_input = (grad * saved_ref[3, :, cols]).astype(BF16)
        rec_ref[:, cols] = (
            grad * saved_ref[4, :, cols]
            + dot(by_reset, wr_ref[h], ((1,), (1,)))
            + dot(by_input, wi_ref[h], ((1,), (1,)))
        ).astype(BF16)

    stores[3].start()
    wait_bytes(z_got.at[pl.ds(0, 7)], z_recv)
    total = own_ref[...]
    for d in range(1, 8):
        total = total + z_got[(z + d) % 8].astype(F32)
    proj_ref[...] = total
    stores[4].start()

    wait_bytes(send_ref.at[pl.ds(0, n_sp - 1)], send_sem)
    wait_bytes(got_ref.at[pl.ds(0, 3), pl.ds(0, 23)], near_g_send)
    for side in (0, 1):
        wait_bytes(raw_ref.at[:, tp], raw_send.at[side])
        wait_bytes(raw_ref.at[0, tp], raw_send.at[2 + side])
        wait_bytes(got_ref.at[tp, pl.ds(0, FAR_GROUPS * 8)], y_send.at[side])
        wait_bytes(got_ref.at[tp, pl.ds(0, FAR_GROUPS * 4)], f_send.at[side])
        wait_bytes(part_ref.at[tp, pl.ds(0, n_sp // 2)], far_send.at[side])
        wait_bytes(part_ref.at[tp], near_send.at[side])
        wait_bytes(mix_ref.at[tp], mix_send.at[side])
        wait_bytes(mix_ref.at[tp, 0], mix_send.at[2 + side])
    wait_bytes(back_ref.at[pl.ds(0, n_sp - 1)], ret_send)
    wait_bytes(pair_ref, pair_send)
    wait_bytes(x_far_ref, x_send.at[0])
    wait_bytes(x_near_ref, x_send.at[1])
    wait_bytes(z_ref.at[pl.ds(0, 7)], z_send)
    wait_bytes(plane_got.at[pl.ds(0, 7)], plane_send)
    wait_bytes(line_got.at[pl.ds(0, 7)], line_send)
    for store in stores:
        store.wait()


def whole_step(n_sp, n_tp, *args):
    conv, w_gate = args[0], args[12]
    tokens, width = conv.shape
    model, fe = w_gate.shape
    packed = width + width // 2
    rows = n_sp * 12
    block = (model // n_sp, width)
    dma = pltpu.SemaphoreType.DMA
    inner, others = (0, 1, 2, 3, 4, 5, 6), (10, 11)
    return pl.pallas_call(
        step_kernel,
        out_shape=(
            jax.ShapeDtypeStruct((model, 2 * fe), BF16),
            jax.ShapeDtypeStruct((fe, model), BF16),
            jax.ShapeDtypeStruct(block, F32),
            jax.ShapeDtypeStruct((tokens, width), BF16),
            jax.ShapeDtypeStruct((tokens, width), BF16),
        ),
        in_specs=[ANY] * 15,
        out_specs=(ANY,) * 5,
        scratch_shapes=[
            *(pltpu.VMEM(args[k].shape, args[k].dtype) for k in inner),
            pltpu.VMEM((2, n_tp, tokens, width), BF16),
            pltpu.VMEM((3, n_tp, 8, 16, packed), BF16),
            *(pltpu.VMEM(args[k].shape, args[k].dtype) for k in others),
            pltpu.VMEM(block, F32),
            pltpu.VMEM((tokens, width), BF16),
            pltpu.VMEM((tokens, width), BF16),
            pltpu.VMEM((n_sp, 16, packed), BF16),
            pltpu.VMEM((2, tokens), jnp.int32),
            pltpu.VMEM((n_tp, n_sp, 16, packed), BF16),
            pltpu.VMEM((rows, model), BF16),
            pltpu.VMEM((rows, model), BF16),
            pltpu.VMEM((rows, 2 * fe), BF16),
            pltpu.VMEM((rows, fe), BF16),
            pltpu.VMEM((n_tp, n_sp, 8, packed), BF16),
            pltpu.VMEM((2, GROUPS, 4, 8, packed), BF16),
            pltpu.VMEM((2, GROUPS, 4, 8, packed), BF16),
            pltpu.VMEM((2, GROUPS, 8, 8, packed), BF16),
            pltpu.VMEM((n_sp, 8, packed), BF16),
            pltpu.VMEM((n_sp, 8, packed), BF16),
            pltpu.VMEM((7, tokens, width), F32),
            pltpu.VMEM((tokens, width), BF16),
            pltpu.VMEM((6, tokens, width), F32),
            pltpu.VMEM((1, width), F32),
            pltpu.VMEM((model, 2 * fe), BF16),
            pltpu.VMEM((fe, model), BF16),
            pltpu.VMEM((width, model), BF16),
            pltpu.VMEM((model, 2 * fe), BF16),
            pltpu.VMEM((fe, model), BF16),
            pltpu.VMEM((n_tp, 2, tokens, width // 2), BF16),
            pltpu.VMEM((tokens, width), F32),
            pltpu.VMEM((tokens, width), F32),
            pltpu.VMEM((8, 4, *block), F32),
            pltpu.VMEM((8, 4, *block), BF16),
            pltpu.VMEM((8, 4, *block), BF16),
            pltpu.VMEM((8, 4, *block), BF16),
            pltpu.VMEM((8, 2, block[0] // 2, width), BF16),
            pltpu.VMEM((8, 2, block[0] // 2, width), BF16),
            pltpu.VMEM((8, 2, *block), BF16),
            pltpu.VMEM((8, *block), BF16),
            pltpu.VMEM((8, *block), BF16),
            pltpu.VMEM(block, F32),
            pltpu.VMEM((1, 2, width), F32),
            pltpu.VMEM((1, 2, width), F32),
            pltpu.VMEM((8, 2, width), F32),
            pltpu.VMEM((8, 2, width), F32),
            dma((15,)), dma((5,)), dma((4,)), dma((3, 2)), dma, dma, dma((8,)), dma((2,)), dma((2, 8)), dma((2,)), dma((2, 8)),
            dma((2,)), dma((2, 8)), dma((2,)), dma((2, 8)), dma, dma, dma((4,)), dma((3, 2)),
            dma, dma((8,)), dma((2,)), dma((2, 8, 2)), dma, dma, dma, dma, dma, dma,
        ],
        compiler_params=pltpu.CompilerParams(
            collective_id=0, has_side_effects=True, vmem_limit_bytes=63 * 2**20
        ),
        name="whole_step",
    )(*args)


def write_kernel(both_ref, down_ref, proj_ref, rec_ref, gate_ref, gg_ref, gu_ref, gd_ref, p_ref, r_ref, g_ref):
    fe = gg_ref.shape[1]
    gg_ref[...] = both_ref[:, :fe].astype(F32)
    gu_ref[...] = both_ref[:, fe:].astype(F32)
    gd_ref[...] = down_ref[...].astype(F32)
    p_ref[...] = proj_ref[...]
    r_ref[...] = rec_ref[...]
    g_ref[...] = gate_ref[...]


def write_out(both, down, proj, rec, gate, parts=2):
    model, fe = both.shape[0], both.shape[1] // 2

    def cut(array):
        return pl.BlockSpec((array.shape[0] // parts, array.shape[1]), lambda i: (i, 0))

    outs = (
        jax.ShapeDtypeStruct((model, fe), F32),
        jax.ShapeDtypeStruct((model, fe), F32),
        jax.ShapeDtypeStruct((fe, model), F32),
        jax.ShapeDtypeStruct(proj.shape, proj.dtype),
        jax.ShapeDtypeStruct(rec.shape, rec.dtype),
        jax.ShapeDtypeStruct(gate.shape, gate.dtype),
    )
    ins = (both, down, proj, rec, gate)
    return pl.pallas_call(
        write_kernel,
        grid=(parts,),
        out_shape=outs,
        in_specs=[cut(a) for a in ins],
        out_specs=tuple(cut(a) for a in outs),
        name="write_out",
    )(*ins)


def body(
    n_sp, n_tp, conv_out, gate_in, block_states, decay_param, decay_shift, w_reset, w_input, w_out,
    mixed, d_out, expert_ids, route_weights, w_gate, w_up, w_down,
):
    both, down, proj, rec, gate = whole_step(
        n_sp, n_tp, conv_out, gate_in, block_states, decay_param[None, :], decay_shift[None, :], w_reset, w_input, w_out,
        mixed, d_out, expert_ids.T, route_weights.T, w_gate[0], w_up[0], w_down[0],
    )
    gg, gu, gd, proj, rec, gate = write_out(both, down, proj, rec, gate)
    return gg[None], gu[None], gd[None], proj, rec, gate


def solution(mesh):
    in_specs = (
        P("sp", "tp"), P("sp", "tp"), P("sp", "tp"), P("tp"), P("sp"),
        P("tp", None, None), P("tp", None, None), P("tp", None),
        P("sp", "tp"), P("sp", "tp"), P("sp", None), P("sp", None),
        P("sp", None, "tp"), P("sp", None, "tp"), P("sp", "tp", None),
    )
    out_specs = (
        P("sp", None, "tp"), P("sp", None, "tp"), P("sp", "tp", None),
        P("sp", "tp"), P("sp", "tp"), P("sp", "tp"),
    )
    run = functools.partial(body, mesh.shape["sp"], mesh.shape["tp"])
    return jax.shard_map(run, mesh=mesh, in_specs=in_specs, out_specs=out_specs, check_vma=False)
```
